128 devices in a mesh: sp: 32 (over z, y, core), tp: 4 (over x).
Axes of the slice: x: 4, y: 4, z: 4, core: 2. Of those that a mesh axis runs over, the one named last changes fastest.
Arguments:
- queries: bfloat16 [16384, 1024], P('sp', 'tp'), may hold values from -260 to 260, as said below
- keys: bfloat16 [16384, 512], P('sp', 'tp'), may hold values from -8 to 8, as said below
- values: bfloat16 [16384, 512], P('sp', 'tp'), may hold values from -24 to 24
- doc_ids: int32 [16384], P('sp'), may hold values from 0 to 7, never falling along the last dimension, each value on 1 to 8192 neighbouring positions
- sink_logit: float32 [8], P('tp'), may hold values from 2 to 7
- residual_in: bfloat16 [16384, 2048], P(('sp', 'tp')), may hold values from -6 to 6
- w_out: bfloat16 [1024, 2048], replicated, may hold values from -0.375 to 0.375
- gain_one: float32 [2048], replicated, may hold values from 0.1 to 1.9
- w_gate: bfloat16 [2048, 5632], P('sp', 'tp'), may hold values from -0.125 to 0.125
- w_up: bfloat16 [2048, 5632], P('sp', 'tp'), may hold values from -0.125 to 0.125
- w_down: bfloat16 [5632, 2048], P('tp', 'sp'), may hold values from -0.078125 to 0.078125
- gain_two: float32 [2048], replicated, may hold values from 0.1 to 1.9
Outputs:
- layer_out: bfloat16 [16384, 2048], P(('sp', 'tp'))
The draws below stay inside these ranges and needn't reach their ends.
Inputs may be any that keep to these rules, and one draw needn't show every extreme that they name: Real-valued projected queries. Real-valued projected keys. `doc_ids`: document numbers never fall along the sequence; each document is one run of positions.
All inputs are finite; a program needn't handle non-finite values.
Results may differ from the reference program's by a relative error of at most 0.012.
Values may be sent and summed in bfloat16 or wider, within the bound.
A program may use at most 128 MiB of HBM per device.

```python
import math
import jax
import jax.numpy as jnp
import numpy as np
from jax import lax

D = 2048
QH = 8
HEAD = 128
FF = 5632
HALF = 128
SEQ = 16384
QW = 1024
KVW = 512
FF_DEV = 1408
N_SP = 32
N_TP = 4


def paired_draw(key):
    key = jax.random.fold_in(key, 11)
    first_key, second_key = jax.random.split(key, 2)
    keys_f = jnp.clip(jax.random.normal(first_key, (SEQ, KVW), jnp.float32), -7.5, 7.5)
    queries_f = jnp.clip(jax.random.normal(second_key, (SEQ, QW), jnp.float32), -7.5, 7.5)
    return (queries_f, keys_f)


def draw_queries(key, part):
    return paired_draw(key)[0].astype(jnp.bfloat16)


def draw_keys(key, part):
    return paired_draw(key)[1].astype(jnp.bfloat16)


def levels(rng, shape, cuts, least, high):
    level = 1.0
    for axis_at, parts in cuts:
        steps = jax.random.uniform(jax.random.fold_in(jax.random.fold_in(rng, 6), axis_at), (parts,), jnp.float32, least / len(cuts), high / len(cuts))
        level = level * jnp.repeat(jnp.exp(steps), shape[axis_at] // parts).reshape((-1,) + (1,) * (len(shape) - 1 - axis_at))
    return level


def length_profile(count, total, most, skew):
    weights = [(1 << 20) // math.isqrt(standing ** skew) + 1 for standing in range(2, count + 1)]
    rest, counts = total - most - (count - 1), [1] * (count - 1)
    while rest > 0:
        candidates = [i for i in range(count - 1) if counts[i] < most]
        mass, budget = sum([weights[i] for i in candidates]), rest
        for i in candidates:
            more = min(most - counts[i], max(1, budget * weights[i] // mass), rest)
            counts[i] = counts[i] + more
            rest = rest - more
    return np.array([most] + counts)


def ragged_sizes(key, count, total, most, skew):
    if count == 2:
        one = jax.random.randint(key, (), max(1, total - most), min(most, total - 1) + 1)
        return jnp.stack([one, total - one])
    sizes = jnp.asarray(length_profile(count, total, most, skew), jnp.int32)
    twos = (count - 1) // 2
    donor, receiver = sizes[1:1 + 2 * twos:2], sizes[2:2 + 2 * twos:2]
    margin = jnp.minimum(donor - 1, most - receiver)
    moved = jax.random.randint(jax.random.fold_in(key, 1), (twos,), 0, 1 << 20) % (margin + 1)
    sizes = sizes.at[1:1 + 2 * twos:2].set(donor - moved).at[2:2 + 2 * twos:2].set(receiver + moved)
    return sizes[jax.random.permutation(jax.random.fold_in(key, 2), count)]


def scatter_about(stream_key, shape, spread, limit, cuts=(), kind=jnp.bfloat16):
    array = jax.random.normal(stream_key, shape, jnp.float32) * spread
    if len(cuts) > 0:
        array = levels(stream_key, shape, cuts, -0.22, 0.18) * array
    return jnp.clip(array, min=-limit, max=limit).astype(kind)


def setup_inputs(seed: int = 0) -> dict:
    key_list = jax.random.split(jax.random.key(seed), 13)
    return {
        "queries": draw_queries(jax.random.fold_in(key_list[12], 71), 0),
        "keys": draw_keys(jax.random.fold_in(key_list[12], 71), 0),
        "values": scatter_about(key_list[2], (SEQ, KVW), 4.0, 24.0, ((0, 32), (1, 4))),
        "doc_ids": jnp.searchsorted(jnp.cumsum(ragged_sizes(key_list[3], max(N_SP // 4, 2), SEQ, SEQ // 2, 1)), jnp.arange(SEQ), side="right").astype(jnp.int32),
        "sink_logit": jnp.clip(2.0 + 5.0 * jax.random.uniform(key_list[4], (QH,), jnp.float32) ** levels(key_list[4], (QH,), ((0, 4),), -0.2, 0.2), 2.0, 7.0),
        "residual_in": scatter_about(key_list[5], (SEQ, D), 1.0, 6.0, ((0, 128),)),
        "w_out": scatter_about(key_list[6], (QW, D), (QW // 4) ** -0.5, 0.375),
        "gain_one": jnp.clip(1.0 + 0.18 * jax.random.normal(key_list[7], (D,), jnp.float32), 0.1, 1.9),
        "w_gate": scatter_about(key_list[8], (D, FF), D ** -0.5, 0.125, ((0, 32), (1, 4))),
        "w_up": scatter_about(key_list[9], (D, FF), D ** -0.5, 0.125, ((0, 32), (1, 4))),
        "w_down": scatter_about(key_list[10], (FF, D), FF ** -0.5, 0.078125, ((0, 4), (1, 32))),
        "gain_two": jnp.clip(1.0 + 0.18 * jax.random.normal(key_list[11], (D,), jnp.float32), 0.1, 1.9),
    }


ALPHA = 2.0 ** 0.5
EPS = 1e-05
NEGATIVE = -1e+30

def layer_norm(values_in, gain):
    average = lax.optimization_barrier(jnp.mean(values_in, -1, keepdims=True))
    centred = values_in - average
    variance = lax.optimization_barrier(jnp.mean(centred * centred, -1, keepdims=True))
    return centred * lax.rsqrt(variance + EPS) * gain

def attend(queries, keys, values, doc_ids, sink_logit):
    seq_len = queries.shape[0]
    kv_heads = keys.shape[1] // HEAD
    repeat = queries.shape[1] // keys.shape[1]
    block = math.gcd(512, seq_len)
    span = block + 2 * HALF
    keys_pad = jnp.pad(keys, ((HALF, HALF), (0, 0)))
    values_pad = jnp.pad(values, ((HALF, HALF), (0, 0)))
    docs_pad = jnp.pad(doc_ids, (HALF, HALF), constant_values=-1)
    sinks = sink_logit.reshape(kv_heads, repeat)

    def one_block(index):
        start = index * block
        query_blk = lax.dynamic_slice_in_dim(queries, start, block, 0).reshape(block, kv_heads, repeat, HEAD)
        key_blk = lax.dynamic_slice_in_dim(keys_pad, start, span, 0).reshape(span, kv_heads, HEAD)
        value_blk = lax.dynamic_slice_in_dim(values_pad, start, span, 0).reshape(span, kv_heads, HEAD)
        doc_query = lax.dynamic_slice_in_dim(doc_ids, start, block, 0)
        doc_key = lax.dynamic_slice_in_dim(docs_pad, start, span, 0)
        pos_query = start + jnp.arange(block, dtype=jnp.int32)
        pos_key = start - HALF + jnp.arange(span, dtype=jnp.int32)
        offset = pos_key[None, :] - pos_query[:, None]
        allowed = (jnp.abs(offset) <= HALF) & (doc_key[None, :] == doc_query[:, None])
        allowed = allowed & (pos_key[None, :] >= 0) & (pos_key[None, :] < seq_len)
        scores = jnp.einsum('qgrd,kgd->grqk', query_blk.astype(jnp.float32), key_blk.astype(jnp.float32)) * HEAD ** (-0.5)
        scores = jnp.where(allowed[None, None], scores, NEGATIVE)
        top = jnp.maximum(lax.optimization_barrier(jnp.max(scores, -1)), sinks[:, :, None])
        weights = jnp.exp(scores - top[..., None])
        total = lax.optimization_barrier(jnp.sum(weights, -1)) + jnp.exp(sinks[:, :, None] - top)
        weights = weights.astype(jnp.bfloat16)
        summed = jnp.einsum('grqk,kgd->qgrd', weights.astype(jnp.float32), value_blk.astype(jnp.float32))
        scaled = summed / jnp.transpose(total, (2, 0, 1))[..., None]
        return scaled.reshape(block, kv_heads * repeat * HEAD).astype(jnp.bfloat16)
    blocks = lax.map(one_block, jnp.arange(seq_len // block, dtype=jnp.int32))
    return blocks.reshape(seq_len, -1)

def reference(queries, keys, values, doc_ids, sink_logit, residual_in, w_out, gain_one, w_gate, w_up, w_down, gain_two):
    attended = attend(queries, keys, values, doc_ids, sink_logit)
    mixed = jnp.dot(attended, w_out, preferred_element_type=jnp.float32)
    pre_one = ALPHA * residual_in.astype(jnp.float32) + mixed
    normed = layer_norm(pre_one, gain_one).astype(jnp.bfloat16)
    gate_part = jnp.dot(normed, w_gate, preferred_element_type=jnp.float32)
    up_part = jnp.dot(normed, w_up, preferred_element_type=jnp.float32)
    hidden = (jax.nn.silu(gate_part) * up_part).astype(jnp.bfloat16)

    def partial_down(carry, index):
        hidden_blk = lax.dynamic_slice_in_dim(hidden, index * FF_DEV, FF_DEV, 1)
        weight_blk = lax.dynamic_slice_in_dim(w_down, index * FF_DEV, FF_DEV, 0)
        term = jnp.dot(hidden_blk, weight_blk, preferred_element_type=jnp.float32).astype(jnp.bfloat16)
        term = lax.optimization_barrier(term).astype(jnp.float32)
        return (carry + term, None)
    down, _ = lax.scan(partial_down, jnp.zeros((SEQ, D), jnp.float32), jnp.arange(N_TP, dtype=jnp.int32))
    pre_two = ALPHA * normed.astype(jnp.float32) + down
    return layer_norm(pre_two, gain_two).astype(jnp.bfloat16)
```

```python
import functools

import jax
import jax.numpy as jnp
from jax import lax
from jax.experimental import pallas as pl
from jax.experimental.pallas import tpu as pltpu
from jax.sharding import PartitionSpec as P

HEAD = 128
HALF = 128
CORES = 2
SIDE = 4
CHIPS = SIDE * SIDE
FAR = CHIPS // 2
TP = 4
ALPHA = 2.0**0.5
EPS = 1e-05
NEGATIVE = -1e30
MESH = pl.DeviceIdType.MESH
BF16 = jnp.bfloat16
F32 = jnp.float32
SEGMENTS = ((0, 16),)


def layer_norm(values_in, gain):
    average = jnp.mean(values_in, -1, keepdims=True)
    centred = values_in - average
    variance = jnp.mean(centred * centred, -1, keepdims=True)
    return centred * lax.rsqrt(variance + EPS) * gain


def slot_of(way, distance):
    if distance == 0:
        return 0
    if distance == FAR:
        return CHIPS - 1
    return 2 * distance - 1 + way


def kernel(
    sink_ref,
    q_hbm,
    res_hbm,
    gain_one_hbm,
    gain_two_hbm,
    k_hbm,
    v_hbm,
    doc_hbm,
    w_out_hbm,
    wg_hbm,
    wu_hbm,
    wd_hbm,
    out_ref,
    q_all,
    k_all,
    v_all,
    doc_all,
    gain_one,
    gain_two,
    w_out,
    gate_w,
    up_w,
    down_w,
    att_all,
    res_all,
    pre,
    normed,
    normed_a,
    normed_b,
    gate_acc,
    up_acc,
    hidden,
    parts,
    relay_m,
    relay_p,
    in_m,
    in_p,
    local_sem,
    halo_send,
    halo_recv,
    ring_send,
    ring_recv,
    pair_send,
    pair_recv,
    res_send,
    res_recv,
    att_send,
    att_recv,
    sum_send,
    sum_recv,
):
    sp = lax.axis_index("sp")
    tp = lax.axis_index("tp")
    sp_size = CHIPS * CORES
    core = lax.rem(sp, CORES)
    chip = sp // CORES
    my_y = lax.rem(chip, SIDE)
    my_z = chip // SIDE
    turn = lax.rem(my_y + my_z, SIDE)
    pos = (my_z * SIDE + turn, my_y * SIDE + turn)

    def chip_at(ring, steps):
        p = lax.rem(pos[ring] + (CHIPS + steps), CHIPS)
        a = p // SIDE
        b = lax.rem(lax.rem(p, SIDE) + (SIDE - a), SIDE)
        return a * SIDE + b if ring == 0 else b * SIDE + a

    def chip_of_slot(ring, slot):
        return chip_at(ring, slot // 2 if slot % 2 == 0 else -((slot + 1) // 2))

    rows = q_hbm.shape[0]
    token_rows = res_hbm.shape[0]
    depth = wg_hbm.shape[0]
    units = wg_hbm.shape[1]
    width = res_hbm.shape[1]
    sub_rows = depth // 2
    wide = CORES * depth

    ring_next = [[chip_at(ring, 1) * CORES + core, chip_at(ring, -1) * CORES + core] for ring in range(2)]
    mixed_next = [
        ring_next[0][way] * (1 - core) + ring_next[1][way] * core for way in range(2)
    ]
    partner = (chip * CORES + (1 - core), tp)
    after = (lax.rem(sp + 1, sp_size), tp)
    before = (lax.rem(sp + sp_size - 1, sp_size), tp)
    tp_right = lax.rem(tp + 1, TP)
    tp_left = lax.rem(tp + TP - 1, TP)
    tp_far = lax.rem(tp + 2, TP)
    sides = [(sp, tp_right), (sp, tp_left)]
    from_side = [tp_left, tp_right]

    barrier = pltpu.get_barrier_semaphore()
    greeted = [(ring_next[ring][way], tp) for ring in range(2) for way in range(2)]
    greeted += [partner, after, before] + sides
    for device in greeted:
        pl.semaphore_signal(barrier, inc=1, device_id=device, device_id_type=MESH)

    own_rows = pl.ds(pl.multiple_of(core * depth, depth), depth)
    loads = [
        pltpu.make_async_copy(k_hbm, k_all.at[pl.ds(HALF, rows)], local_sem.at[0]),
        pltpu.make_async_copy(v_hbm, v_all.at[pl.ds(HALF, rows)], local_sem.at[1]),
        pltpu.make_async_copy(doc_hbm, doc_all.at[:, pl.ds(HALF, rows)], local_sem.at[2]),
        pltpu.make_async_copy(q_hbm, q_all, local_sem.at[3]),
    ]
    out_loads = [
        pltpu.make_async_copy(w_out_hbm, w_out, local_sem.at[4]),
        pltpu.make_async_copy(res_hbm, res_all.at[tp], local_sem.at[5]),
        pltpu.make_async_copy(gain_one_hbm, gain_one, local_sem.at[6]),
        pltpu.make_async_copy(gain_two_hbm, gain_two, local_sem.at[7]),
    ]
    own_loads = [
        pltpu.make_async_copy(src, dst.at[own_rows], local_sem.at[8 + i])
        for i, (src, dst) in enumerate(((wg_hbm, gate_w), (wu_hbm, up_w), (wd_hbm, down_w)))
    ]
    for load in loads + out_loads + own_loads:
        load.start()
    pl.semaphore_wait(barrier, len(greeted))

    def remote(src, dst, send, recv, device):
        return pltpu.make_async_remote_copy(
            src_ref=src, dst_ref=dst, send_sem=send, recv_sem=recv, device_id=device, device_id_type=MESH
        )

    sent = []

    def launch(copy):
        copy.start()
        sent.append(copy)

    def arrive(copy):
        copy.wait_recv()

    low, high = (pl.ds(0, HALF), pl.ds(rows - HALF, HALF))
    into_low, into_high = (pl.ds(0, HALF), pl.ds(HALF + rows, HALF))
    halos = []
    for i, (src, dst) in enumerate(((k_hbm, k_all), (v_hbm, v_all))):
        halos.append(
            remote(src.at[high], dst.at[into_low], halo_send.at[i, 0], halo_recv.at[i, 0], after)
        )
        halos.append(
            remote(src.at[low], dst.at[into_high], halo_send.at[i, 1], halo_recv.at[i, 1], before)
        )
    halos.append(
        remote(doc_hbm.at[:, high], doc_all.at[:, into_low], halo_send.at[2, 0], halo_recv.at[2, 0], after)
    )
    halos.append(
        remote(doc_hbm.at[:, low], doc_all.at[:, into_high], halo_send.at[2, 1], halo_recv.at[2, 1], before)
    )
    for halo in halos:
        launch(halo)

    sources = (wg_hbm, wu_hbm, wd_hbm)
    buffers = (gate_w, up_w, down_w)

    def place(piece, way, distance, core_id):
        start = slot_of(way, distance) * wide + core_id * depth + (piece % 2) * sub_rows
        return buffers[piece // 2].at[pl.ds(pl.multiple_of(start, sub_rows), sub_rows)]

    def own(piece):
        return sources[piece // 2].at[pl.ds((piece % 2) * sub_rows, sub_rows)]

    def ring_to(piece, way):
        kind = piece // 2
        return (ring_next[kind][way] if kind < 2 else mixed_next[way], tp)

    def ring_out(way, piece, distance):
        src = own(piece) if distance == 1 else place(piece, way, distance - 1, core)
        return remote(
            src,
            place(piece, way, distance, core),
            ring_send.at[way, piece, distance],
            ring_recv.at[way, piece, distance],
            ring_to(piece, way),
        )

    def ring_in(way, piece, distance):
        dst = place(piece, way, distance, core)
        return remote(
            dst,
            dst,
            ring_send.at[way, piece, distance],
            ring_recv.at[way, piece, distance],
            ring_to(piece, 1 - way),
        )

    def pair_out(way, piece, distance):
        dst = place(piece, way, distance, core)
        src = own(piece) if distance == 0 else dst
        return remote(
            src, dst, pair_send.at[way, piece, distance], pair_recv.at[way, piece, distance], partner
        )

    def pair_in(way, piece, distance):
        dst = place(piece, way, distance, 1 - core)
        return remote(
            dst, dst, pair_send.at[way, piece, distance], pair_recv.at[way, piece, distance], partner
        )

    rounds = []
    for distance in range(1, FAR + 1):
        rounds.append((distance, 0, 1))
        if distance < FAR:
            rounds.append((distance, 1, 0))
    per_phase = len(rounds)

    def pump(index):
        if index < per_phase:
            bases = (0, 2)
        else:
            bases = (4,)
        distance, first, second = rounds[index % per_phase]
        for base in bases:
            for way, sub in ((0, first), (1, second)):
                piece = base + sub
                arrive(ring_in(way, piece, distance))
                if distance + 1 < FAR or (distance + 1 == FAR and sub == way):
                    launch(ring_out(way, piece, distance + 1))
                launch(pair_out(way, piece, distance))
        if index == per_phase - 2:
            launch(ring_out(0, 4, 1))
            launch(ring_out(1, 5, 1))
        if index == per_phase - 1:
            launch(ring_out(0, 5, 1))
            launch(ring_out(1, 4, 1))

    for first, second in ((0, 1), (1, 0)):
        for base in (0, 2):
            launch(ring_out(0, base + first, 1))
            launch(ring_out(1, base + second, 1))

    def res_half(half):
        return pl.ds(half * (token_rows // 2), token_rows // 2)

    def res_own(way, k):
        half = res_half(k if way == 0 else 1 - k)
        return remote(
            res_hbm.at[half], res_all.at[tp, half], res_send.at[way, k], res_recv.at[way, k], sides[way]
        )

    def res_in(way, k):
        half = res_half((k if way == 0 else 1 - k) if k < 2 else way)
        slot = res_all.at[from_side[way] if k < 2 else tp_far, half]
        return remote(slot, slot, res_send.at[way, k], res_recv.at[way, k], sides[1 - way])

    def res_forward(way):
        slot = res_all.at[from_side[way], res_half(way)]
        return remote(slot, slot, res_send.at[way, 2], res_recv.at[way, 2], sides[way])

    for k in range(2):
        for way in range(2):
            launch(res_own(way, k))
    for piece in range(6):
        launch(pair_out(0, piece, 0))

    def block_rows(block):
        return pl.ds(block * HALF, HALF)

    def att_copy(way, block, source, index, device):
        slot = att_all.at[source, block_rows(block)]
        return remote(slot, slot, att_send.at[way, index], att_recv.at[way, index], device)

    for load in loads:
        load.wait()
    for halo in halos:
        arrive(halo)
    span = rows + 2 * HALF
    at = lax.broadcasted_iota(jnp.int32, (1, span), 1) + (sp * rows - HALF)
    inside = jnp.logical_and(at >= 0, at < sp_size * rows)
    doc_keys = jnp.where(inside, doc_all[...], -1)
    reach = 3 * HALF
    repeat = q_hbm.shape[1] // HEAD
    offset = lax.broadcasted_iota(jnp.int32, (HALF, reach), 1) - lax.broadcasted_iota(
        jnp.int32, (HALF, reach), 0
    )
    near = jnp.logical_and(offset >= 0, offset <= 2 * HALF)

    def attend(block):
        doc_row = doc_all[:, (block + 1) * HALF : (block + 2) * HALF]
        doc_query = jnp.broadcast_to(doc_row, (HALF, HALF)).T
        same = jnp.concatenate([doc_query] * 3, 1) == doc_keys[:, block * HALF : block * HALF + reach]
        allowed = jnp.logical_and(near, same)
        key_blk = k_all[block * HALF : block * HALF + reach, :]
        value_blk = v_all[block * HALF : block * HALF + reach, :]
        for h in range(repeat):
            query_blk = q_all[block * HALF : (block + 1) * HALF, h * HEAD : (h + 1) * HEAD]
            scores = lax.dot_general(
                query_blk, key_blk, (((1,), (1,)), ((), ())), preferred_element_type=F32
            ) * HEAD ** (-0.5)
            scores = jnp.where(allowed, scores, NEGATIVE)
            sink = jnp.full((1, 1), sink_ref[h], F32)
            top = jnp.maximum(jnp.max(scores, -1, keepdims=True), sink)
            weights = jnp.exp(scores - top)
            total = jnp.sum(weights, -1, keepdims=True) + jnp.exp(sink - top)
            summed = jnp.dot(weights.astype(BF16), value_blk, preferred_element_type=F32)
            att_all[pl.ds(tp, 1), block * HALF : (block + 1) * HALF, h * HEAD : (h + 1) * HEAD] = (
                summed / total
            ).astype(BF16)[None]
        for way in range(2):
            launch(att_copy(way, block, tp, block, sides[way]))

    def att_forward(block):
        way = block % 2
        arrive(att_copy(way, block, from_side[way], block, sides[1 - way]))
        launch(att_copy(way, block, from_side[way], 4 + block // 2, sides[way]))

    def att_rest(block):
        way = block % 2
        arrive(att_copy(1 - way, block, from_side[1 - way], block, sides[way]))
        arrive(att_copy(way, block, tp_far, 4 + block // 2, sides[1 - way]))

    tile = 512
    strip = 32

    def project(block):
        @pl.loop(0, width // tile)
        def _(t):
            lanes = pl.ds(pl.multiple_of(t * tile, tile), tile)
            mixed = ALPHA * res_all[block, :, lanes].astype(F32)
            for j in range(TP):
                mixed += jnp.dot(
                    att_all[j, block * HALF : (block + 1) * HALF, :],
                    w_out[j * 256 : (j + 1) * 256, lanes],
                    preferred_element_type=F32,
                )
            pre[:, lanes] = mixed

        @pl.loop(0, token_rows // strip)
        def _(t):
            here = pl.ds(pl.multiple_of(t * strip, strip), strip)
            there = pl.ds(pl.multiple_of(block * HALF + t * strip, strip), strip)
            normed[there, :] = layer_norm(pre[here, :], gain_one[...]).astype(BF16)

        part = slice(block * HALF, (block + 1) * HALF)
        for slot in range(CHIPS):
            to = slice(slot * wide, (slot + 1) * wide)
            for ring, buf in ((0, normed_a), (1, normed_b)):
                lanes = pl.ds(pl.multiple_of(chip_of_slot(ring, slot) * wide, wide), wide)
                buf[part, to] = normed[part, lanes]

    def gate_up(lo, hi, lanes):
        deep = slice(lo * wide, hi * wide)
        gate = jnp.dot(normed_a[:, deep], gate_w[deep, lanes], preferred_element_type=F32)
        up = jnp.dot(normed_b[:, deep], up_w[deep, lanes], preferred_element_type=F32)
        if lo > 0:
            gate += gate_acc[:, lanes]
            up += up_acc[:, lanes]
        if hi < CHIPS:
            gate_acc[:, lanes] = gate
            up_acc[:, lanes] = up
        else:
            hidden[:, lanes] = (gate / (1.0 + jnp.exp(-gate)) * up).astype(BF16)

    def gate_up_tiles(lo, hi, first, last):
        @pl.loop(first, last)
        def _(t):
            gate_up(lo, hi, pl.ds(pl.multiple_of(t * 256, 256), 256))

    def gate_up_rest(lo, hi):
        gate_up(lo, hi, slice(units // 256 * 256, units))

    def pair_weights(kind, distance):
        for sub in range(2):
            piece = 2 * kind + sub
            if distance == FAR:
                arrive(pair_in(sub, piece, distance))
            elif distance == 0:
                arrive(pair_in(0, piece, 0))
            else:
                for way in range(2):
                    arrive(pair_in(way, piece, distance))

    def rows_of(j):
        return pl.ds(pl.multiple_of(j * token_rows, token_rows), token_rows)

    def down_chunk(k):
        part = lax.dot_general(
            hidden[...],
            down_w[2 * k * wide : 2 * (k + 1) * wide, :],
            (((1,), (1,)), ((), ())),
            preferred_element_type=F32,
        ).astype(BF16)
        parts[2 * k] = part[:, :wide]
        parts[2 * k + 1] = part[:, wide:]
        a, b = 2 * k, 2 * k + 1
        far = rows_of(tp_far)
        launch(remote(parts.at[a, far], relay_m.at[k], sum_send.at[0, k, 0], sum_recv.at[0, k, 0], sides[0]))
        launch(remote(parts.at[b, far], relay_p.at[k], sum_send.at[1, k, 0], sum_recv.at[1, k, 0], sides[1]))
        launch(
            remote(
                parts.at[b, rows_of(tp_right)], in_m.at[b], sum_send.at[0, k, 1], sum_recv.at[0, k, 1], sides[0]
            )
        )
        launch(
            remote(
                parts.at[a, rows_of(tp_left)], in_p.at[a], sum_send.at[1, k, 1], sum_recv.at[1, k, 1], sides[1]
            )
        )

    def sum_in(way, slot, k, index):
        return remote(slot, slot, sum_send.at[way, k, index], sum_recv.at[way, k, index], sides[1 - way])

    def relay_chunk(k):
        a, b = 2 * k, 2 * k + 1
        for way, slot, held, j, target in (
            (0, a, relay_m, tp_right, in_m),
            (1, b, relay_p, tp_left, in_p),
        ):
            arrive(sum_in(way, held.at[k], k, 0))
            here = rows_of(j)
            parts[slot, here, :] = (
                parts[slot, here, :].astype(F32) + held[k].astype(F32)
            ).astype(BF16)
            launch(
                remote(
                    parts.at[slot, here],
                    target.at[slot],
                    sum_send.at[way, k, 2],
                    sum_recv.at[way, k, 2],
                    sides[way],
                )
            )

    first_lanes = lax.broadcasted_iota(jnp.int32, (token_rows, wide), 1) < depth

    def finish_chunk(k):
        a, b = 2 * k, 2 * k + 1
        arrive(sum_in(0, in_m.at[b], k, 1))
        arrive(sum_in(1, in_p.at[a], k, 1))
        arrive(sum_in(0, in_m.at[a], k, 2))
        arrive(sum_in(1, in_p.at[b], k, 2))
        for slot in (a, b):
            down = (
                parts[slot, rows_of(tp), :].astype(F32)
                + in_m[slot].astype(F32)
                + in_p[slot].astype(F32)
            )
            for ring in range(2):
                lanes = pl.ds(pl.multiple_of(chip_of_slot(ring, slot) * wide, wide), wide)
                mine = first_lanes if ring == 0 else jnp.logical_not(first_lanes)
                pre[:, lanes] += jnp.where(mine, down, 0.0)

    for block in range(4):
        attend(block)
        pump(block)
    for way in range(2):
        arrive(res_in(way, 0))
        launch(res_forward(way))
    pump(4)
    pump(5)
    pump(6)
    for block in range(4):
        att_forward(block)
    pump(7)
    pump(8)
    for load in out_loads:
        load.wait()
    for way in range(2):
        arrive(res_in(way, 1))
        arrive(res_in(way, 2))
    for block in range(4):
        att_rest(block)
        project(block)
        pump(9 + block)
    pre[...] = ALPHA * normed[rows_of(tp), :].astype(F32)
    pump(13)
    pump(14)
    for load in own_loads:
        load.wait()
    for kind in range(2):
        for distance in range(FAR + 1):
            pair_weights(kind, distance)
    gate_up_tiles(0, 16, 0, 2)
    pump(15)
    pump(16)
    gate_up_tiles(0, 16, 2, 4)
    pump(17)
    pump(18)
    gate_up_tiles(0, 16, 4, 5)
    gate_up_rest(0, 16)
    pump(19)
    pair_weights(2, 0)
    index = 20
    for k in range(FAR):
        while index < 2 * per_phase and rounds[index - per_phase][0] <= k + 1:
            pump(index)
            index += 1
        pair_weights(2, k + 1)
        down_chunk(k)
        if k >= 1:
            relay_chunk(k - 1)
        if k >= 3:
            finish_chunk(k - 3)
    relay_chunk(FAR - 1)
    for k in range(FAR - 3, FAR):
        finish_chunk(k)

    @pl.loop(0, token_rows // strip)
    def _(t):
        here = pl.ds(pl.multiple_of(t * strip, strip), strip)
        out_ref[here, :] = layer_norm(pre[here, :], gain_two[...]).astype(BF16)

    for copy in sent:
        copy.wait_send()


def solution(mesh):
    def per_device(
        queries,
        keys,
        values,
        doc_ids,
        sink_logit,
        residual_in,
        w_out,
        gain_one,
        w_gate,
        w_up,
        w_down,
        gain_two,
    ):
        rows = queries.shape[0]
        token_rows, width = residual_in.shape
        units = w_gate.shape[1]
        span = rows + 2 * HALF
        dma = pltpu.SemaphoreType.DMA
        vmem, anywhere = (pl.BlockSpec(memory_space=pltpu.VMEM), pl.BlockSpec(memory_space=pl.ANY))
        return pl.pallas_call(
            kernel,
            out_shape=jax.ShapeDtypeStruct((token_rows, width), BF16),
            in_specs=[pl.BlockSpec(memory_space=pltpu.SMEM)] + [anywhere] * 11,
            out_specs=vmem,
            scratch_shapes=[
                pltpu.VMEM(queries.shape, BF16),
                pltpu.VMEM((span, keys.shape[1]), BF16),
                pltpu.VMEM((span, keys.shape[1]), BF16),
                pltpu.VMEM((1, span), jnp.int32),
                pltpu.VMEM((1, width), F32),
                pltpu.VMEM((1, width), F32),
                pltpu.VMEM(w_out.shape, BF16),
                pltpu.VMEM((width, units), BF16),
                pltpu.VMEM((width, units), BF16),
                pltpu.VMEM((width, units), BF16),
                pltpu.VMEM((TP, rows, queries.shape[1]), BF16),
                pltpu.VMEM((TP, token_rows, width), BF16),
                pltpu.VMEM((token_rows, width), F32),
                pltpu.VMEM((rows, width), BF16),
                pltpu.VMEM((rows, width), BF16),
                pltpu.VMEM((rows, width), BF16),
                pltpu.VMEM((rows, units), F32),
                pltpu.VMEM((rows, units), F32),
                pltpu.VMEM((rows, units), BF16),
                pltpu.VMEM((CHIPS, rows, width // CHIPS), BF16),
                pltpu.VMEM((FAR, token_rows, width // CHIPS), BF16),
                pltpu.VMEM((FAR, token_rows, width // CHIPS), BF16),
                pltpu.VMEM((CHIPS, token_rows, width // CHIPS), BF16),
                pltpu.VMEM((CHIPS, token_rows, width // CHIPS), BF16),
                dma((11,)),
                dma((3, 2)),
                dma((3, 2)),
                dma((2, 6, FAR + 1)),
                dma((2, 6, FAR + 1)),
                dma((2, 6, FAR + 1)),
                dma((2, 6, FAR + 1)),
                dma((2, 3)),
                dma((2, 3)),
                dma((2, 6)),
                dma((2, 6)),
                dma((2, FAR, 3)),
                dma((2, FAR, 3)),
            ],
            compiler_params=pltpu.CompilerParams(
                collective_id=0, has_side_effects=True, vmem_limit_bytes=62 * 2**20
            ),
        )(
            sink_logit,
            queries,
            residual_in,
            gain_one[None, :],
            gain_two[None, :],
            keys,
            values,
            doc_ids[None, :],
            w_out,
            w_gate,
            w_up,
            w_down.T,
        )

    in_specs = (
        P("sp", "tp"),
        P("sp", "tp"),
        P("sp", "tp"),
        P("sp"),
        P("tp"),
        P(("sp", "tp"), None),
        P(),
        P(),
        P("sp", "tp"),
        P("sp", "tp"),
        P("tp", "sp"),
        P(),
    )
    return jax.shard_map(
        per_device, mesh=mesh, in_specs=in_specs, out_specs=P(("sp", "tp"), None), check_vma=False
    )
```

```python
import jax
import jax.numpy as jnp
from jax import lax
from jax.experimental import pallas as pl
from jax.experimental.pallas import tpu as pltpu
from jax.sharding import PartitionSpec as P

HEAD = 128
HALF = 128
CORES = 2
SIDE = 4
CHIPS = SIDE * SIDE
TP = 4
ALPHA = 2.0**0.5
EPS = 1e-05
NEGATIVE = -1e30
MESH = pl.DeviceIdType.MESH
BF16 = jnp.bfloat16
F32 = jnp.float32
OFFSETS = (
    (0, 0),
    (1, 0),
    (0, 1),
    (-1, 0),
    (0, -1),
    (1, 1),
    (-1, -1),
    (1, -1),
    (-1, 1),
    (2, 0),
    (0, 2),
    (2, 1),
    (1, 2),
    (2, -1),
    (-1, 2),
    (2, 2),
)
SLOT = {offset: slot for slot, offset in enumerate(OFFSETS)}
SEGMENTS = ((0, 5), (5, 11), (11, 16))
CHUNKS = ((1, 2), (3, 4), (5, 6), (7, 8), (9, 10), (11, 12), (13, 14), (0, 15))
LAST = 10


def message(number, way):
    s = 2 * way - 1
    return (
        None,
        (0, (0, 0), (s, 0), False),
        (1, (0, 0), (0, s), False),
        (0, (s, 0), (2, 0), True),
        (1, (s, 0), (s, s), False),
        (1, (-s, 0), (-s, s), False),
        (1, (0, s), (0, 2), True),
        (1, (2, 0), (2, s), False),
        (1, (s, s), (s, 2), True),
        (1, (-s, s), (-s, 2), True),
        (1, (2, s), (2, 2), True),
    )[number]


FOLLOW = {1: (3, 4, 5), 2: (6,), 3: (7,), 4: (8,), 5: (9,), 7: (10,)}


def segment_of(slot):
    return [lo <= slot < hi for lo, hi in SEGMENTS].index(True)


def chunk_of(slot):
    return [slot in chunk for chunk in CHUNKS].index(True)


def layer_norm(values_in, gain):
    average = jnp.mean(values_in, -1, keepdims=True)
    centred = values_in - average
    variance = jnp.mean(centred * centred, -1, keepdims=True)
    return centred * lax.rsqrt(variance + EPS) * gain


def kernel(
    sink_ref,
    q_hbm,
    res_hbm,
    gain_one_hbm,
    gain_two_hbm,
    k_hbm,
    v_hbm,
    doc_hbm,
    w_out_hbm,
    wg_hbm,
    wu_hbm,
    wd_hbm,
    out_ref,
    q_all,
    k_all,
    v_all,
    doc_all,
    gains_in,
    gains,
    res_all,
    w_out,
    gate_w,
    up_w,
    down_w,
    att,
    tokens,
    pre,
    normed,
    gate_acc,
    up_acc,
    hidden,
    parts,
    relays,
    arrived,
    local_sem,
    halo_send,
    halo_recv,
    ring_send,
    ring_recv,
    pair_send,
    pair_recv,
    down_recv,
    tok_send,
    tok_recv,
    norm_send,
    norm_recv,
    sum_send,
    relay_recv,
    sum_recv,
):
    sp = lax.axis_index("sp")
    tp = lax.axis_index("tp")
    sp_size = CHIPS * CORES
    core = lax.rem(sp, CORES)
    chip = sp // CORES
    my_y = lax.rem(chip, SIDE)
    my_z = chip // SIDE

    def chip_at(dz, dy):
        z = lax.rem(my_z + (dz + SIDE), SIDE)
        y = lax.rem(my_y + (dy + SIDE), SIDE)
        return z * SIDE + y

    rows = q_hbm.shape[0]
    token_rows = res_hbm.shape[0]
    depth = wg_hbm.shape[0]
    units = wg_hbm.shape[1]
    width = res_hbm.shape[1]
    sub_rows = depth // 2
    wide = CORES * depth
    half_rows = token_rows // 2

    def chip_lanes(slot):
        return pl.ds(pl.multiple_of(chip_at(*OFFSETS[slot]) * wide, wide), wide)

    def slot_lanes(slot):
        return slice(slot * wide, (slot + 1) * wide)

    along_z = [chip_at(1, 0) * CORES + core, chip_at(-1, 0) * CORES + core]
    along_y = [chip_at(0, 1) * CORES + core, chip_at(0, -1) * CORES + core]
    first_axis = [along_z[way] * (1 - core) + along_y[way] * core for way in range(2)]
    second_axis = [along_y[way] * (1 - core) + along_z[way] * core for way in range(2)]
    axes = ((along_z, along_y), (along_y, along_z), (first_axis, second_axis))
    partner = (chip * CORES + (1 - core), tp)
    after = (lax.rem(sp + 1, sp_size), tp)
    before = (lax.rem(sp + sp_size - 1, sp_size), tp)
    tp_right = lax.rem(tp + 1, TP)
    tp_left = lax.rem(tp + TP - 1, TP)
    tp_far = lax.rem(tp + 2, TP)
    sides = [(sp, tp_right), (sp, tp_left)]
    far = (sp, tp_far)

    barrier = pltpu.get_barrier_semaphore()
    greeted = [(axis[way], tp) for axis in (along_z, along_y) for way in range(2)]
    greeted += [partner, after, before, far] + sides
    for device in greeted:
        pl.semaphore_signal(barrier, inc=1, device_id=device, device_id_type=MESH)

    own_rows = pl.ds(pl.multiple_of(core * depth, depth), depth)
    loads = [
        pltpu.make_async_copy(src, dst, local_sem.at[i])
        for i, (src, dst) in enumerate(
            (
                (q_hbm, q_all),
                (k_hbm, k_all.at[pl.ds(HALF, rows)]),
                (v_hbm, v_all.at[pl.ds(HALF, rows)]),
                (doc_hbm, doc_all.at[:, pl.ds(HALF, rows)]),
                (w_out_hbm, w_out),
                (res_hbm, res_all),
                (gain_one_hbm, gains_in.at[pl.ds(0, 1)]),
                (gain_two_hbm, gains_in.at[pl.ds(1, 1)]),
                (wg_hbm, gate_w.at[own_rows]),
                (wu_hbm, up_w.at[own_rows]),
                (wd_hbm, down_w.at[own_rows]),
            )
        )
    ]
    for load in loads:
        load.start()

    def remote(src, dst, send, recv, device):
        return pltpu.make_async_remote_copy(
            src_ref=src, dst_ref=dst, send_sem=send, recv_sem=recv, device_id=device, device_id_type=MESH
        )

    def launch(copy):
        copy.start()

    def arrive(copy):
        copy.wait_recv()

    def wait_bytes(ref, sem):
        remote(ref, ref, sem, sem, partner).wait_recv()

    low, high = (pl.ds(0, HALF), pl.ds(rows - HALF, HALF))
    into_low, into_high = (pl.ds(0, HALF), pl.ds(HALF + rows, HALF))

    def launch_halos():
        for i, (src, dst) in enumerate(((k_hbm, k_all), (v_hbm, v_all))):
            launch(remote(src.at[high], dst.at[into_low], halo_send.at[i], halo_recv.at[i], after))
            launch(remote(src.at[low], dst.at[into_high], halo_send.at[i], halo_recv.at[i], before))
        launch(
            remote(doc_hbm.at[:, high], doc_all.at[:, into_low], halo_send.at[2], halo_recv.at[2], after)
        )
        launch(
            remote(doc_hbm.at[:, low], doc_all.at[:, into_high], halo_send.at[2], halo_recv.at[2], before)
        )

    def halo_refs():
        edge = pl.ds(0, 2 * HALF)
        return (k_all.at[edge], v_all.at[edge], doc_all.at[:, edge])

    def halo_wait():
        for i, ref in enumerate(halo_refs()):
            wait_bytes(ref, halo_recv.at[i])

    sources = (wg_hbm, wu_hbm, wd_hbm)
    buffers = (gate_w, up_w, down_w)

    def slot_for(kind, offset, core_id):
        straight, swapped = SLOT[offset], SLOT[offset[::-1]]
        if kind == 0:
            return straight
        if kind == 1:
            return swapped
        return straight * (1 - core_id) + swapped * core_id

    def place(kind, offset, half, core_id):
        start = slot_for(kind, offset, core_id) * wide + core_id * depth
        if half is None:
            return buffers[kind].at[pl.ds(pl.multiple_of(start, depth), depth)]
        return buffers[kind].at[pl.ds(pl.multiple_of(start + half * sub_rows, sub_rows), sub_rows)]

    def ring(kind, number, way, outgoing):
        axis, src_offset, dst_offset, halved = message(number, way)
        half = way if halved else None
        dst = place(kind, dst_offset, half, core)
        if not outgoing:
            src = dst
        elif src_offset == (0, 0):
            src = sources[kind] if half is None else sources[kind].at[pl.ds(half * sub_rows, sub_rows)]
        else:
            src = place(kind, src_offset, half, core)
        to = (axes[kind][axis][way if outgoing else 1 - way], tp)
        return remote(src, dst, ring_send.at[kind], ring_recv.at[kind, way, number], to)

    def pair(kind, offset, half):
        dst = place(kind, offset, half, core)
        src = sources[kind] if offset == (0, 0) else dst
        slot = SLOT[offset]
        if kind == 2:
            sem = down_recv.at[chunk_of(slot)]
        else:
            sem = pair_recv.at[kind, segment_of(slot)]
        return remote(src, dst, pair_send.at[kind], sem, partner)

    def begin(kinds):
        for number in (1, 2):
            for kind in kinds:
                for way in range(2):
                    launch(ring(kind, number, way, True))

    def tick(number, kinds):
        for kind in kinds:
            for way in range(2):
                arrive(ring(kind, number, way, False))
        for follower in FOLLOW.get(number, ()):
            for kind in kinds:
                for way in range(2):
                    launch(ring(kind, follower, way, True))
        for kind in kinds:
            for way in range(2):
                _, _, offset, halved = message(number, way)
                launch(pair(kind, offset, way if halved else None))

    weights_tick = lambda number: tick(number, (0, 1))
    down_tick = lambda number: tick(number, (2,))

    def segment_wait(segment):
        lo, hi = SEGMENTS[segment]
        for kind in range(2):
            wait_bytes(buffers[kind].at[pl.ds(0, (hi - lo) * depth)], pair_recv.at[kind, segment])

    for load in loads[:4]:
        load.wait()
    span = rows + 2 * HALF
    at = lax.broadcasted_iota(jnp.int32, (1, span), 1) + (sp * rows - HALF)
    inside = jnp.logical_and(at >= 0, at < sp_size * rows)
    reach = 3 * HALF
    repeat = q_hbm.shape[1] // HEAD
    offset_of = lax.broadcasted_iota(jnp.int32, (HALF, reach), 1) - lax.broadcasted_iota(
        jnp.int32, (HALF, reach), 0
    )
    near = jnp.logical_and(offset_of >= 0, offset_of <= 2 * HALF)

    def attend(block):
        here = slice(block * HALF, (block + 1) * HALF)
        there = slice(block * HALF, block * HALF + reach)
        doc_row = doc_all[:, (block + 1) * HALF : (block + 2) * HALF]
        doc_query = jnp.broadcast_to(doc_row, (HALF, HALF)).T
        doc_keys = jnp.where(inside[:, there], doc_all[:, there], -1)
        same = jnp.concatenate([doc_query] * 3, 1) == doc_keys
        allowed = jnp.logical_and(near, same)
        key_blk = k_all[there, :]
        value_blk = v_all[there, :]
        for h in range(repeat):
            lanes = slice(h * HEAD, (h + 1) * HEAD)
            scores = lax.dot_general(
                q_all[here, lanes], key_blk, (((1,), (1,)), ((), ())), preferred_element_type=F32
            ) * HEAD ** (-0.5)
            scores = jnp.where(allowed, scores, NEGATIVE)
            sink = jnp.full((1, 1), sink_ref[h], F32)
            top = jnp.maximum(jnp.max(scores, -1, keepdims=True), sink)
            weights = jnp.exp(scores - top)
            total = jnp.sum(weights, -1, keepdims=True) + jnp.exp(sink - top)
            summed = jnp.dot(weights.astype(BF16), value_blk, preferred_element_type=F32)
            att[here, lanes] = (summed / total).astype(BF16)

    def token_rows_of(j):
        return pl.ds(pl.multiple_of(j * token_rows, token_rows), token_rows)

    def send_tokens():
        for j in (tp_far, tp_right, tp_left):
            launch(
                remote(att.at[token_rows_of(j)], tokens.at[tp], tok_send.at[0], tok_recv.at[0], (sp, j))
            )
        tokens[pl.ds(tp, 1)] = att[token_rows_of(tp), :][None]

    def order_gains():
        for slot in range(CHIPS):
            gains[:, slot_lanes(slot)] = gains_in[:, chip_lanes(slot)]

    def project():
        for first, second in zip(range(0, CHIPS, 2), range(1, CHIPS, 2)):
            picks = (chip_lanes(first), chip_lanes(second))
            mixed = ALPHA * jnp.concatenate([res_all[:, pick] for pick in picks], 1).astype(F32)
            for j in range(TP):
                deep = slice(j * 256, (j + 1) * 256)
                mixed += jnp.dot(
                    tokens[j],
                    jnp.concatenate([w_out[deep, pick] for pick in picks], 1),
                    preferred_element_type=F32,
                )
            pre[:, first * wide : (second + 1) * wide] = mixed

    strip = 32

    def norm_rows(first, last):
        @pl.loop(first // strip, last // strip)
        def _(t):
            here = pl.ds(pl.multiple_of(t * strip, strip), strip)
            normed[here, :] = layer_norm(pre[here, :], gains[0:1, :]).astype(BF16)

    def piece_rows(index):
        return pl.ds(index * half_rows, half_rows)

    ROUTES = ((0, 0, 2), (1, 1, 3), (0, 1, 4), (1, 0, 5), (0, 2, 6), (1, 3, 7))

    def norm_copy(route):
        way, src, dst = ROUTES[route]
        return remote(
            normed.at[piece_rows(src)],
            normed.at[piece_rows(dst)],
            norm_send.at[0],
            norm_recv.at[route],
            sides[way],
        )

    def norm_arrive(route):
        way, _, dst = ROUTES[route]
        slot = normed.at[piece_rows(dst)]
        arrive(remote(slot, slot, norm_send.at[0], norm_recv.at[route], sides[1 - way]))

    def gate_up(top, bottom, lo, hi, lanes):
        deep = slice(lo * wide, hi * wide)
        gate = jnp.dot(normed[top:bottom, deep], gate_w[deep, lanes], preferred_element_type=F32)
        up = jnp.dot(normed[top:bottom, deep], up_w[deep, lanes], preferred_element_type=F32)
        if lo > 0:
            gate += gate_acc[top:bottom, lanes]
            up += up_acc[top:bottom, lanes]
        if hi < CHIPS:
            gate_acc[top:bottom, lanes] = gate
            up_acc[top:bottom, lanes] = up
        else:
            hidden[top:bottom, lanes] = (gate / (1.0 + jnp.exp(-gate)) * up).astype(BF16)

    def gate_up_tiles(top, bottom, lo, hi, first, last):
        @pl.loop(first, last)
        def _(t):
            gate_up(top, bottom, lo, hi, pl.ds(pl.multiple_of(t * 256, 256), 256))

    def gate_up_rest(top, bottom, lo, hi):
        gate_up(top, bottom, lo, hi, slice(units // 256 * 256, units))

    def gate_up_range(top, bottom, lo, hi):
        gate_up_tiles(top, bottom, lo, hi, 0, units // 256)
        gate_up_rest(top, bottom, lo, hi)

    def dest(index):
        return pl.ds(index * token_rows, token_rows)

    OWN, LEFT, RIGHT, FAR = range(4)
    ORDER = (0, 1, 2, 4, 5, 3, 6, 7)

    def down_chunk(k):
        a, b = CHUNKS[k]
        if b == a + 1:
            weights = down_w[a * wide : (b + 1) * wide, :]
        else:
            weights = jnp.concatenate([down_w[s * wide : (s + 1) * wide, :] for s in (a, b)], 0)
        part = lax.dot_general(
            hidden[...], weights, (((1,), (1,)), ((), ())), preferred_element_type=F32
        ).astype(BF16)
        for to, source in enumerate(ORDER):
            for slot, lanes in ((a, slice(0, wide)), (b, slice(wide, 2 * wide))):
                parts[slot, to * half_rows : (to + 1) * half_rows, :] = part[
                    source * half_rows : (source + 1) * half_rows, lanes
                ]
        launch(remote(parts.at[a, dest(FAR)], relays.at[0, k], sum_send.at[0], relay_recv.at[0, k], sides[0]))
        launch(remote(parts.at[b, dest(FAR)], relays.at[1, k], sum_send.at[0], relay_recv.at[1, k], sides[1]))
        launch(remote(parts.at[b, dest(RIGHT)], arrived.at[k, 1], sum_send.at[0], sum_recv.at[k], sides[0]))
        launch(remote(parts.at[a, dest(LEFT)], arrived.at[k, 2], sum_send.at[0], sum_recv.at[k], sides[1]))

    def relay_chunk(k):
        for way, slot, to, index in ((0, CHUNKS[k][0], RIGHT, 0), (1, CHUNKS[k][1], LEFT, 3)):
            held = relays.at[way, k]
            arrive(remote(held, held, sum_send.at[0], relay_recv.at[way, k], sides[1 - way]))
            here = dest(to)
            parts[slot, here, :] = (
                parts[slot, here, :].astype(F32) + relays[way, k].astype(F32)
            ).astype(BF16)
            launch(
                remote(parts.at[slot, here], arrived.at[k, index], sum_send.at[0], sum_recv.at[k], sides[way])
            )

    def finish_chunk(k):
        wait_bytes(arrived.at[k], sum_recv.at[k])
        for slot, left, right in ((CHUNKS[k][0], 0, 2), (CHUNKS[k][1], 1, 3)):
            down = (
                parts[slot, dest(OWN), :].astype(F32)
                + arrived[k, left].astype(F32)
                + arrived[k, right].astype(F32)
            )
            pre[:, slot_lanes(slot)] = ALPHA * normed[0:token_rows, slot_lanes(slot)].astype(F32) + down

    def final_norm():
        @pl.loop(0, token_rows // strip)
        def _(t):
            here = pl.ds(pl.multiple_of(t * strip, strip), strip)
            result = layer_norm(pre[here, :], gains[1:2, :]).astype(BF16)
            for slot in range(CHIPS):
                out_ref[here, chip_lanes(slot)] = result[:, slot_lanes(slot)]

    def sends_wait():
        def gone(ref, sem):
            remote(ref, ref, sem, sem, partner).wait_send()

        for i, ref in enumerate(halo_refs()):
            gone(ref, halo_send.at[i])
        for kind in range(3):
            gone(buffers[kind].at[pl.ds(0, (CHIPS - 1) * depth)], ring_send.at[kind])
            gone(buffers[kind].at[pl.ds(0, CHIPS * depth)], pair_send.at[kind])
        gone(tokens.at[pl.ds(0, TP - 1)], tok_send.at[0])
        gone(normed.at[pl.ds(0, 6 * half_rows)], norm_send.at[0])
        gone(parts.at[pl.ds(0, 12)], sum_send.at[0])

    attend(1)
    attend(2)
    pl.semaphore_wait(barrier, len(greeted))
    launch_halos()
    begin((0, 1))
    for kind in range(3):
        launch(pair(kind, (0, 0), None))
    halo_wait()
    attend(0)
    attend(3)
    send_tokens()
    weights_tick(1)
    for load in loads[4:]:
        load.wait()
    order_gains()
    wait_bytes(tokens.at[pl.ds(0, TP - 1)], tok_recv.at[0])
    project()
    norm_rows(0, half_rows)
    launch(norm_copy(0))
    norm_rows(half_rows, token_rows)
    for route in (1, 2, 3):
        launch(norm_copy(route))
    weights_tick(2)
    weights_tick(3)
    weights_tick(4)
    for route in (0, 1):
        norm_arrive(route)
    for route in (4, 5):
        launch(norm_copy(route))
    weights_tick(5)
    segment_wait(0)
    gate_up_range(0, 256, 0, 5)
    weights_tick(6)
    segment_wait(1)
    gate_up_range(0, 256, 5, 11)
    weights_tick(7)
    begin((2,))
    for route in (2, 3):
        norm_arrive(route)
    gate_up_range(256, 384, 0, 11)
    weights_tick(8)
    weights_tick(9)
    for route in (4, 5):
        norm_arrive(route)
    gate_up_range(384, 512, 0, 11)
    weights_tick(10)
    segment_wait(2)
    gate_up_tiles(0, 512, 11, 16, 0, 3)
    down_tick(1)
    gate_up_tiles(0, 512, 11, 16, 3, 5)
    gate_up_rest(0, 512, 11, 16)
    down_tick(2)
    needs = (2, 2, 4, 5, 6, 9, 9, 10)
    done = 2
    for k in range(len(CHUNKS)):
        while done < needs[k]:
            done += 1
            down_tick(done)
        wait_bytes(down_w.at[pl.ds(0, wide)], down_recv.at[k])
        down_chunk(k)
        if k >= 1:
            relay_chunk(k - 1)
        if k >= 3:
            finish_chunk(k - 3)
    relay_chunk(7)
    for k in (5, 6, 7):
        finish_chunk(k)
    final_norm()
    sends_wait()


def solution(mesh):
    def per_device(
        queries,
        keys,
        values,
        doc_ids,
        sink_logit,
        residual_in,
        w_out,
        gain_one,
        w_gate,
        w_up,
        w_down,
        gain_two,
    ):
        rows = queries.shape[0]
        token_rows, width = residual_in.shape
        units = w_gate.shape[1]
        span = rows + 2 * HALF
        dma = pltpu.SemaphoreType.DMA
        vmem, anywhere = (pl.BlockSpec(memory_space=pltpu.VMEM), pl.BlockSpec(memory_space=pl.ANY))
        return pl.pallas_call(
            kernel,
            out_shape=jax.ShapeDtypeStruct((token_rows, width), BF16),
            in_specs=[pl.BlockSpec(memory_space=pltpu.SMEM)] + [anywhere] * 11,
            out_specs=vmem,
            scratch_shapes=[
                pltpu.VMEM(queries.shape, BF16),
                pltpu.VMEM((span, keys.shape[1]), BF16),
                pltpu.VMEM((span, keys.shape[1]), BF16),
                pltpu.VMEM((1, span), jnp.int32),
                pltpu.VMEM((2, width), F32),
                pltpu.VMEM((2, width), F32),
                pltpu.VMEM((token_rows, width), BF16),
                pltpu.VMEM(w_out.shape, BF16),
                pltpu.VMEM((width, units), BF16),
                pltpu.VMEM((width, units), BF16),
                pltpu.VMEM((width, units), BF16),
                pltpu.VMEM(queries.shape, BF16),
                pltpu.VMEM((TP, token_rows, queries.shape[1]), BF16),
                pltpu.VMEM((token_rows, width), F32),
                pltpu.VMEM((rows, width), BF16),
                pltpu.VMEM((rows, units), F32),
                pltpu.VMEM((rows, units), F32),
                pltpu.VMEM((rows, units), BF16),
                pltpu.VMEM((CHIPS, rows, width // CHIPS), BF16),
                pltpu.VMEM((2, len(CHUNKS), token_rows, width // CHIPS), BF16),
                pltpu.VMEM((len(CHUNKS), 4, token_rows, width // CHIPS), BF16),
                dma((11,)),
                dma((3,)),
                dma((3,)),
                dma((3,)),
                dma((3, 2, LAST + 1)),
                dma((3,)),
                dma((2, len(SEGMENTS))),
                dma((len(CHUNKS),)),
                dma((1,)),
                dma((1,)),
                dma((1,)),
                dma((6,)),
                dma((1,)),
                dma((2, len(CHUNKS))),
                dma((len(CHUNKS),)),
            ],
            compiler_params=pltpu.CompilerParams(
                collective_id=0, has_side_effects=True, vmem_limit_bytes=62 * 2**20
            ),
        )(
            sink_logit,
            queries,
            residual_in,
            gain_one[None, :],
            gain_two[None, :],
            keys,
            values,
            doc_ids[None, :],
            w_out,
            w_gate,
            w_up,
            w_down.T,
        )

    in_specs = (
        P("sp", "tp"),
        P("sp", "tp"),
        P("sp", "tp"),
        P("sp"),
        P("tp"),
        P(("sp", "tp"), None),
        P(),
        P(),
        P("sp", "tp"),
        P("sp", "tp"),
        P("tp", "sp"),
        P(),
    )
    return jax.shard_map(
        per_device, mesh=mesh, in_specs=in_specs, out_specs=P(("sp", "tp"), None), check_vma=False
    )
```

```python
import jax
import jax.numpy as jnp
from jax import lax
from jax.experimental import pallas as pl
from jax.experimental.pallas import tpu as pltpu
from jax.sharding import PartitionSpec as P

HEAD = 128
HALF = 128
CORES = 2
SIDE = 4
CHIPS = SIDE * SIDE
TP = 4
ALPHA = 2.0**0.5
EPS = 1e-05
NEGATIVE = -1e30
MESH = pl.DeviceIdType.MESH
BF16 = jnp.bfloat16
F32 = jnp.float32
OFFSETS = (
    (0, 0),
    (1, 0),
    (0, 1),
    (-1, 0),
    (0, -1),
    (1, 1),
    (-1, -1),
    (1, -1),
    (-1, 1),
    (2, 0),
    (0, 2),
    (2, 1),
    (1, 2),
    (2, -1),
    (-1, 2),
    (2, 2),
)
SLOT = {offset: slot for slot, offset in enumerate(OFFSETS)}
SEGMENTS = ((0, 5), (5, 11), (11, 15), (15, 16))
CHUNKS = ((1, 2), (3, 4), (5, 6), (7, 8), (9, 10), (11, 12), (13, 14), (0, 15))
LAST = 10


def message(number, way):
    s = 2 * way - 1
    return (
        None,
        (0, (0, 0), (s, 0), False),
        (1, (0, 0), (0, s), False),
        (0, (s, 0), (2, 0), True),
        (1, (s, 0), (s, s), False),
        (1, (-s, 0), (-s, s), False),
        (1, (0, s), (0, 2), True),
        (1, (2, 0), (2, s), False),
        (1, (s, s), (s, 2), True),
        (1, (-s, s), (-s, 2), True),
        (1, (2, s), (2, 2), True),
    )[number]


FOLLOW = {1: (3, 4, 5), 2: (6,), 3: (7,), 4: (8,), 5: (9,), 7: (10,)}


def segment_of(slot):
    return [lo <= slot < hi for lo, hi in SEGMENTS].index(True)


def chunk_of(slot):
    return [slot in chunk for chunk in CHUNKS].index(True)


def layer_norm(values_in, gain):
    average = jnp.mean(values_in, -1, keepdims=True)
    centred = values_in - average
    variance = jnp.mean(centred * centred, -1, keepdims=True)
    return centred * lax.rsqrt(variance + EPS) * gain


def kernel(
    sink_ref,
    q_hbm,
    res_hbm,
    gain_one_hbm,
    gain_two_hbm,
    k_hbm,
    v_hbm,
    doc_hbm,
    w_out_hbm,
    wg_hbm,
    wu_hbm,
    wd_hbm,
    out_ref,
    q_all,
    k_all,
    v_all,
    doc_all,
    gains_in,
    gains,
    res_all,
    w_out,
    gate_w,
    up_w,
    down_w,
    att,
    tokens,
    pre,
    normed,
    gate_acc,
    up_acc,
    hidden,
    parts,
    relays,
    arrived,
    local_sem,
    halo_send,
    halo_recv,
    ring_send,
    ring_recv,
    pair_send,
    pair_recv,
    down_recv,
    tok_send,
    tok_recv,
    norm_send,
    norm_recv,
    sum_send,
    relay_recv,
    sum_recv,
):
    sp = lax.axis_index("sp")
    tp = lax.axis_index("tp")
    sp_size = CHIPS * CORES
    core = lax.rem(sp, CORES)
    chip = sp // CORES
    my_y = lax.rem(chip, SIDE)
    my_z = chip // SIDE

    def chip_at(dz, dy):
        z = lax.rem(my_z + (dz + SIDE), SIDE)
        y = lax.rem(my_y + (dy + SIDE), SIDE)
        return z * SIDE + y

    rows = q_hbm.shape[0]
    token_rows = res_hbm.shape[0]
    depth = wg_hbm.shape[0]
    units = wg_hbm.shape[1]
    width = res_hbm.shape[1]
    sub_rows = depth // 2
    wide = CORES * depth
    half_rows = token_rows // 2

    def chip_lanes(slot):
        return pl.ds(pl.multiple_of(chip_at(*OFFSETS[slot]) * wide, wide), wide)

    def slot_lanes(slot):
        return slice(slot * wide, (slot + 1) * wide)

    along_z = [chip_at(1, 0) * CORES + core, chip_at(-1, 0) * CORES + core]
    along_y = [chip_at(0, 1) * CORES + core, chip_at(0, -1) * CORES + core]
    first_axis = [along_z[way] * (1 - core) + along_y[way] * core for way in range(2)]
    second_axis = [along_y[way] * (1 - core) + along_z[way] * core for way in range(2)]
    axes = ((along_z, along_y), (along_y, along_z), (first_axis, second_axis))
    partner = (chip * CORES + (1 - core), tp)
    after = (lax.rem(sp + 1, sp_size), tp)
    before = (lax.rem(sp + sp_size - 1, sp_size), tp)
    tp_right = lax.rem(tp + 1, TP)
    tp_left = lax.rem(tp + TP - 1, TP)
    tp_far = lax.rem(tp + 2, TP)
    sides = [(sp, tp_right), (sp, tp_left)]
    far = (sp, tp_far)

    barrier = pltpu.get_barrier_semaphore()
    greeted = [(axis[way], tp) for axis in (along_z, along_y) for way in range(2)]
    greeted += [partner, after, before, far] + sides
    for device in greeted:
        pl.semaphore_signal(barrier, inc=1, device_id=device, device_id_type=MESH)

    own_rows = pl.ds(pl.multiple_of(core * depth, depth), depth)
    loads = [
        pltpu.make_async_copy(src, dst, local_sem.at[i])
        for i, (src, dst) in enumerate(
            (
                (q_hbm, q_all),
                (k_hbm, k_all.at[pl.ds(HALF, rows)]),
                (v_hbm, v_all.at[pl.ds(HALF, rows)]),
                (doc_hbm, doc_all.at[:, pl.ds(HALF, rows)]),
                (w_out_hbm, w_out),
                (res_hbm, res_all),
                (gain_one_hbm, gains_in.at[pl.ds(0, 1)]),
                (gain_two_hbm, gains_in.at[pl.ds(1, 1)]),
                (wg_hbm, gate_w.at[own_rows]),
                (wu_hbm, up_w.at[own_rows]),
                (wd_hbm, down_w.at[own_rows]),
            )
        )
    ]
    for load in loads:
        load.start()

    def remote(src, dst, send, recv, device):
        return pltpu.make_async_remote_copy(
            src_ref=src, dst_ref=dst, send_sem=send, recv_sem=recv, device_id=device, device_id_type=MESH
        )

    def launch(copy):
        copy.start()

    def arrive(copy):
        copy.wait_recv()

    def wait_bytes(ref, sem):
        remote(ref, ref, sem, sem, partner).wait_recv()

    low, high = (pl.ds(HALF, HALF), pl.ds(rows, HALF))
    into_low, into_high = (pl.ds(0, HALF), pl.ds(HALF + rows, HALF))

    def launch_halos():
        for i, ref in enumerate((k_all, v_all)):
            launch(remote(ref.at[high], ref.at[into_low], halo_send.at[i], halo_recv.at[i], after))
            launch(remote(ref.at[low], ref.at[into_high], halo_send.at[i], halo_recv.at[i], before))
        for src, dst, to in ((high, into_low, after), (low, into_high, before)):
            launch(
                remote(doc_all.at[:, src], doc_all.at[:, dst], halo_send.at[2], halo_recv.at[2], to)
            )

    def halo_refs():
        edge = pl.ds(0, 2 * HALF)
        return (k_all.at[edge], v_all.at[edge], doc_all.at[:, edge])

    def halo_wait():
        for i, ref in enumerate(halo_refs()):
            wait_bytes(ref, halo_recv.at[i])

    buffers = (gate_w, up_w, down_w)

    def slot_for(kind, offset, core_id):
        straight, swapped = SLOT[offset], SLOT[offset[::-1]]
        if kind == 0:
            return straight
        if kind == 1:
            return swapped
        return straight * (1 - core_id) + swapped * core_id

    def place(kind, offset, half, core_id):
        start = slot_for(kind, offset, core_id) * wide + core_id * depth
        if half is None:
            return buffers[kind].at[pl.ds(pl.multiple_of(start, depth), depth)]
        return buffers[kind].at[pl.ds(pl.multiple_of(start + half * sub_rows, sub_rows), sub_rows)]

    def ring(kind, number, way, outgoing):
        axis, src_offset, dst_offset, halved = message(number, way)
        half = way if halved else None
        dst = place(kind, dst_offset, half, core)
        src = place(kind, src_offset, half, core) if outgoing else dst
        to = (axes[kind][axis][way if outgoing else 1 - way], tp)
        return remote(src, dst, ring_send.at[kind], ring_recv.at[kind, way, number], to)

    def pair(kind, offset, half):
        dst = place(kind, offset, half, core)
        slot = SLOT[offset]
        if kind == 2:
            sem = down_recv.at[chunk_of(slot)]
        else:
            sem = pair_recv.at[kind, segment_of(slot)]
        return remote(dst, dst, pair_send.at[kind], sem, partner)

    def begin(kinds):
        for number in (1, 2):
            for kind in kinds:
                for way in range(2):
                    launch(ring(kind, number, way, True))

    def tick(number, kinds):
        for kind in kinds:
            for way in range(2):
                arrive(ring(kind, number, way, False))
        for follower in FOLLOW.get(number, ()):
            for kind in kinds:
                for way in range(2):
                    launch(ring(kind, follower, way, True))
        for kind in kinds:
            for way in range(2):
                _, _, offset, halved = message(number, way)
                launch(pair(kind, offset, way if halved else None))

    weights_tick = lambda number: tick(number, (0, 1))
    down_tick = lambda number: tick(number, (2,))

    def segment_wait(segment):
        lo, hi = SEGMENTS[segment]
        for kind in range(2):
            wait_bytes(buffers[kind].at[pl.ds(0, (hi - lo) * depth)], pair_recv.at[kind, segment])

    span = rows + 2 * HALF
    at = lax.broadcasted_iota(jnp.int32, (1, span), 1) + (sp * rows - HALF)
    inside = jnp.logical_and(at >= 0, at < sp_size * rows)
    reach = 3 * HALF
    repeat = q_hbm.shape[1] // HEAD
    offset_of = lax.broadcasted_iota(jnp.int32, (HALF, reach), 1) - lax.broadcasted_iota(
        jnp.int32, (HALF, reach), 0
    )
    near = jnp.logical_and(offset_of >= 0, offset_of <= 2 * HALF)

    def attend(block):
        here = slice(block * HALF, (block + 1) * HALF)
        there = slice(block * HALF, block * HALF + reach)
        doc_row = doc_all[:, (block + 1) * HALF : (block + 2) * HALF]
        doc_query = jnp.broadcast_to(doc_row, (HALF, HALF)).T
        doc_keys = jnp.where(inside[:, there], doc_all[:, there], -1)
        same = jnp.concatenate([doc_query] * 3, 1) == doc_keys
        allowed = jnp.logical_and(near, same)
        key_blk = k_all[there, :]
        value_blk = v_all[there, :]
        for h in range(repeat):
            lanes = slice(h * HEAD, (h + 1) * HEAD)
            scores = lax.dot_general(
                q_all[here, lanes], key_blk, (((1,), (1,)), ((), ())), preferred_element_type=F32
            ) * HEAD ** (-0.5)
            scores = jnp.where(allowed, scores, NEGATIVE)
            sink = jnp.full((1, 1), sink_ref[h], F32)
            top = jnp.maximum(jnp.max(scores, -1, keepdims=True), sink)
            weights = jnp.exp(scores - top)
            total = jnp.sum(weights, -1, keepdims=True) + jnp.exp(sink - top)
            summed = jnp.dot(weights.astype(BF16), value_blk, preferred_element_type=F32)
            att[here, lanes] = (summed / total).astype(BF16)

    def token_rows_of(j):
        return pl.ds(pl.multiple_of(j * token_rows, token_rows), token_rows)

    def send_tokens():
        for j in (tp_far, tp_right, tp_left):
            launch(
                remote(att.at[token_rows_of(j)], tokens.at[tp], tok_send.at[0], tok_recv.at[0], (sp, j))
            )
        tokens[pl.ds(tp, 1)] = att[token_rows_of(tp), :][None]

    def order_gains():
        for slot in range(CHIPS):
            gains[:, slot_lanes(slot)] = gains_in[:, chip_lanes(slot)]

    def project():
        for first, second in zip(range(0, CHIPS, 2), range(1, CHIPS, 2)):
            picks = (chip_lanes(first), chip_lanes(second))
            mixed = ALPHA * jnp.concatenate([res_all[:, pick] for pick in picks], 1).astype(F32)
            for j in range(TP):
                deep = slice(j * 256, (j + 1) * 256)
                mixed += jnp.dot(
                    tokens[j],
                    jnp.concatenate([w_out[deep, pick] for pick in picks], 1),
                    preferred_element_type=F32,
                )
            pre[:, first * wide : (second + 1) * wide] = mixed

    strip = 32

    def norm_rows(first, last):
        @pl.loop(first // strip, last // strip)
        def _(t):
            here = pl.ds(pl.multiple_of(t * strip, strip), strip)
            normed[here, :] = layer_norm(pre[here, :], gains[0:1, :]).astype(BF16)

    def piece_rows(index):
        return pl.ds(index * half_rows, half_rows)

    ROUTES = ((0, 0, 2), (1, 1, 3), (0, 1, 4), (1, 0, 5), (0, 2, 6), (1, 3, 7))

    def norm_copy(route):
        way, src, dst = ROUTES[route]
        return remote(
            normed.at[piece_rows(src)],
            normed.at[piece_rows(dst)],
            norm_send.at[0],
            norm_recv.at[route],
            sides[way],
        )

    def norm_arrive(route):
        way, _, dst = ROUTES[route]
        slot = normed.at[piece_rows(dst)]
        arrive(remote(slot, slot, norm_send.at[0], norm_recv.at[route], sides[1 - way]))

    def gate_up(top, bottom, lo, hi, lanes):
        deep = slice(lo * wide, hi * wide)
        gate = jnp.dot(normed[top:bottom, deep], gate_w[deep, lanes], preferred_element_type=F32)
        up = jnp.dot(normed[top:bottom, deep], up_w[deep, lanes], preferred_element_type=F32)
        if lo > 0:
            gate += gate_acc[top:bottom, lanes]
            up += up_acc[top:bottom, lanes]
        if hi < CHIPS:
            gate_acc[top:bottom, lanes] = gate
            up_acc[top:bottom, lanes] = up
        else:
            hidden[top:bottom, lanes] = (gate / (1.0 + jnp.exp(-gate)) * up).astype(BF16)

    def gate_up_tiles(top, bottom, lo, hi, first, last):
        @pl.loop(first, last)
        def _(t):
            gate_up(top, bottom, lo, hi, pl.ds(pl.multiple_of(t * 256, 256), 256))

    def gate_up_rest(top, bottom, lo, hi):
        gate_up(top, bottom, lo, hi, slice(units // 256 * 256, units))

    def gate_up_range(top, bottom, lo, hi):
        gate_up_tiles(top, bottom, lo, hi, 0, units // 256)
        gate_up_rest(top, bottom, lo, hi)

    def dest(index):
        return pl.ds(index * token_rows, token_rows)

    OWN, LEFT, RIGHT, FAR = range(4)
    ORDER = (0, 1, 2, 4, 5, 3, 6, 7)

    def down_chunk(k):
        wait_bytes(down_w.at[pl.ds(0, wide)], down_recv.at[k])
        a, b = CHUNKS[k]
        if b == a + 1:
            weights = down_w[a * wide : (b + 1) * wide, :]
        else:
            weights = jnp.concatenate([down_w[s * wide : (s + 1) * wide, :] for s in (a, b)], 0)
        part = lax.dot_general(
            hidden[...], weights, (((1,), (1,)), ((), ())), preferred_element_type=F32
        ).astype(BF16)
        for to, source in enumerate(ORDER):
            for slot, lanes in ((a, slice(0, wide)), (b, slice(wide, 2 * wide))):
                parts[slot, to * half_rows : (to + 1) * half_rows, :] = part[
                    source * half_rows : (source + 1) * half_rows, lanes
                ]
        launch(remote(parts.at[a, dest(FAR)], relays.at[0, k], sum_send.at[0], relay_recv.at[0, k], sides[0]))
        launch(remote(parts.at[b, dest(FAR)], relays.at[1, k], sum_send.at[0], relay_recv.at[1, k], sides[1]))

    def plain_chunk(k):
        a, b = CHUNKS[k]
        launch(remote(parts.at[b, dest(RIGHT)], arrived.at[k, 1], sum_send.at[0], sum_recv.at[k], sides[0]))
        launch(remote(parts.at[a, dest(LEFT)], arrived.at[k, 2], sum_send.at[0], sum_recv.at[k], sides[1]))

    def relay_chunk(k):
        for way, slot, to, index in ((0, CHUNKS[k][0], RIGHT, 0), (1, CHUNKS[k][1], LEFT, 3)):
            held = relays.at[way, k]
            arrive(remote(held, held, sum_send.at[0], relay_recv.at[way, k], sides[1 - way]))
            here = dest(to)
            parts[slot, here, :] = (
                parts[slot, here, :].astype(F32) + relays[way, k].astype(F32)
            ).astype(BF16)
            launch(
                remote(parts.at[slot, here], arrived.at[k, index], sum_send.at[0], sum_recv.at[k], sides[way])
            )

    def finish_chunk(k):
        wait_bytes(arrived.at[k], sum_recv.at[k])
        for slot, left, right in ((CHUNKS[k][0], 0, 2), (CHUNKS[k][1], 1, 3)):
            down = (
                parts[slot, dest(OWN), :].astype(F32)
                + arrived[k, left].astype(F32)
                + arrived[k, right].astype(F32)
            )
            pre[:, slot_lanes(slot)] = ALPHA * normed[0:token_rows, slot_lanes(slot)].astype(F32) + down

    def final_norm():
        @pl.loop(0, token_rows // strip)
        def _(t):
            here = pl.ds(pl.multiple_of(t * strip, strip), strip)
            result = layer_norm(pre[here, :], gains[1:2, :]).astype(BF16)
            for slot in range(CHIPS):
                out_ref[here, chip_lanes(slot)] = result[:, slot_lanes(slot)]

    def sends_wait():
        def gone(ref, sem):
            remote(ref, ref, sem, sem, partner).wait_send()

        for i, ref in enumerate(halo_refs()):
            gone(ref, halo_send.at[i])
        for kind in range(3):
            gone(buffers[kind].at[pl.ds(0, (CHIPS - 1) * depth)], ring_send.at[kind])
            gone(buffers[kind].at[pl.ds(0, CHIPS * depth)], pair_send.at[kind])
        gone(tokens.at[pl.ds(0, TP - 1)], tok_send.at[0])
        gone(normed.at[pl.ds(0, 6 * half_rows)], norm_send.at[0])
        gone(parts.at[pl.ds(0, 12)], sum_send.at[0])

    pl.semaphore_wait(barrier, len(greeted))
    for load in loads[:4]:
        load.wait()
    launch_halos()
    for load in loads[8:]:
        load.wait()
    begin((0, 1))
    for kind in range(3):
        launch(pair(kind, (0, 0), None))
    attend(1)
    attend(2)
    halo_wait()
    attend(0)
    attend(3)
    send_tokens()
    weights_tick(1)
    for load in loads[4:8]:
        load.wait()
    order_gains()
    wait_bytes(tokens.at[pl.ds(0, TP - 1)], tok_recv.at[0])
    project()
    norm_rows(0, half_rows)
    launch(norm_copy(0))
    norm_rows(half_rows, token_rows)
    for route in (1, 2, 3):
        launch(norm_copy(route))
    weights_tick(2)
    weights_tick(3)
    weights_tick(4)
    for route in (0, 1):
        norm_arrive(route)
    for route in (4, 5):
        launch(norm_copy(route))
    weights_tick(5)
    segment_wait(0)
    gate_up_range(0, 256, 0, 5)
    weights_tick(6)
    segment_wait(1)
    gate_up_range(0, 256, 5, 11)
    weights_tick(7)
    begin((2,))
    for route in (2, 3):
        norm_arrive(route)
    gate_up_range(256, 384, 0, 11)
    weights_tick(8)
    weights_tick(9)
    for route in (4, 5):
        norm_arrive(route)
    gate_up_range(384, 512, 0, 11)
    segment_wait(2)
    gate_up_tiles(0, 512, 11, 15, 0, 2)
    weights_tick(10)
    gate_up_tiles(0, 512, 11, 15, 2, 5)
    gate_up_rest(0, 512, 11, 15)
    segment_wait(3)
    gate_up_tiles(0, 512, 15, 16, 0, 2)
    down_tick(1)
    gate_up_tiles(0, 512, 15, 16, 2, 5)
    gate_up_rest(0, 512, 15, 16)
    down_tick(2)
    down_chunk(0)
    plain_chunk(0)
    down_tick(3)
    down_chunk(1)
    plain_chunk(1)
    down_tick(4)
    down_chunk(2)
    plain_chunk(2)
    down_tick(5)
    relay_chunk(0)
    down_chunk(3)
    plain_chunk(3)
    down_tick(6)
    relay_chunk(1)
    down_tick(7)
    down_chunk(4)
    plain_chunk(4)
    relay_chunk(2)
    down_tick(8)
    down_tick(9)
    down_chunk(5)
    plain_chunk(5)
    relay_chunk(3)
    down_chunk(6)
    relay_chunk(4)
    down_tick(10)
    down_chunk(7)
    plain_chunk(6)
    relay_chunk(5)
    plain_chunk(7)
    finish_chunk(0)
    finish_chunk(1)
    finish_chunk(2)
    relay_chunk(6)
    relay_chunk(7)
    finish_chunk(3)
    finish_chunk(4)
    finish_chunk(5)
    finish_chunk(6)
    finish_chunk(7)
    final_norm()
    sends_wait()


def solution(mesh):
    def per_device(
        queries,
        keys,
        values,
        doc_ids,
        sink_logit,
        residual_in,
        w_out,
        gain_one,
        w_gate,
        w_up,
        w_down,
        gain_two,
    ):
        rows = queries.shape[0]
        token_rows, width = residual_in.shape
        units = w_gate.shape[1]
        span = rows + 2 * HALF
        dma = pltpu.SemaphoreType.DMA
        vmem, anywhere = (pl.BlockSpec(memory_space=pltpu.VMEM), pl.BlockSpec(memory_space=pl.ANY))
        return pl.pallas_call(
            kernel,
            out_shape=pltpu.VMEM((token_rows, width), BF16),
            in_specs=[pl.BlockSpec(memory_space=pltpu.SMEM)] + [anywhere] * 11,
            out_specs=vmem,
            scratch_shapes=[
                pltpu.VMEM(queries.shape, BF16),
                pltpu.VMEM((span, keys.shape[1]), BF16),
                pltpu.VMEM((span, keys.shape[1]), BF16),
                pltpu.VMEM((1, span), jnp.int32),
                pltpu.VMEM((2, width), F32),
                pltpu.VMEM((2, width), F32),
                pltpu.VMEM((token_rows, width), BF16),
                pltpu.VMEM(w_out.shape, BF16),
                pltpu.VMEM((width, units), BF16),
                pltpu.VMEM((width, units), BF16),
                pltpu.VMEM((width, units), BF16),
                pltpu.VMEM(queries.shape, BF16),
                pltpu.VMEM((TP, token_rows, queries.shape[1]), BF16),
                pltpu.VMEM((token_rows, width), F32),
                pltpu.VMEM((rows, width), BF16),
                pltpu.VMEM((rows, units), F32),
                pltpu.VMEM((rows, units), F32),
                pltpu.VMEM((rows, units), BF16),
                pltpu.VMEM((CHIPS, rows, width // CHIPS), BF16),
                pltpu.VMEM((2, len(CHUNKS), token_rows, width // CHIPS), BF16),
                pltpu.VMEM((len(CHUNKS), 4, token_rows, width // CHIPS), BF16),
                dma((11,)),
                dma((3,)),
                dma((3,)),
                dma((3,)),
                dma((3, 2, LAST + 1)),
                dma((3,)),
                dma((2, len(SEGMENTS))),
                dma((len(CHUNKS),)),
                dma((1,)),
                dma((1,)),
                dma((1,)),
                dma((6,)),
                dma((1,)),
                dma((2, len(CHUNKS))),
                dma((len(CHUNKS),)),
            ],
            compiler_params=pltpu.CompilerParams(
                collective_id=0, has_side_effects=True, vmem_limit_bytes=62 * 2**20
            ),
        )(
            sink_logit,
            queries,
            residual_in,
            gain_one[None, :],
            gain_two[None, :],
            keys,
            values,
            doc_ids[None, :],
            w_out,
            w_gate,
            w_up,
            w_down.T,
        )

    in_specs = (
        P("sp", "tp"),
        P("sp", "tp"),
        P("sp", "tp"),
        P("sp"),
        P("tp"),
        P(("sp", "tp"), None),
        P(),
        P(),
        P("sp", "tp"),
        P("sp", "tp"),
        P("tp", "sp"),
        P(),
    )
    return jax.shard_map(
        per_device, mesh=mesh, in_specs=in_specs, out_specs=P(("sp", "tp"), None), check_vma=False
    )
```

```python
import jax
import jax.numpy as jnp
from jax import lax
from jax.experimental import pallas as pl
from jax.experimental.pallas import tpu as pltpu
from jax.sharding import PartitionSpec as P

HEAD = 128
HALF = 128
CORES = 2
SIDE = 4
CHIPS = SIDE * SIDE
TP = 4
ALPHA = 2.0**0.5
EPS = 1e-05
NEGATIVE = -1e30
MESH = pl.DeviceIdType.MESH
BF16 = jnp.bfloat16
F32 = jnp.float32
OFFSETS = (
    (0, 0),
    (1, 0),
    (0, 1),
    (-1, 0),
    (0, -1),
    (1, 1),
    (-1, -1),
    (1, -1),
    (-1, 1),
    (2, 0),
    (0, 2),
    (2, 1),
    (1, 2),
    (2, -1),
    (-1, 2),
    (2, 2),
)
SLOT = {offset: slot for slot, offset in enumerate(OFFSETS)}
SEGMENTS = ((0, 4), (4, 10), (10, 16))
CHUNKS = ((1, 3), (2, 4), (5, 6), (7, 8), (9, 10), (11, 13), (12, 14), (0, 15))
LAST = 10


def message(number, way):
    s = 2 * way - 1
    return (
        None,
        (0, (0, 0), (s, 0), False),
        (1, (0, 0), (0, s), False),
        (0, (s, 0), (2, 0), True),
        (1, (s, 0), (s, s), False),
        (1, (-s, 0), (-s, s), False),
        (1, (0, s), (0, 2), True),
        (1, (2, 0), (2, s), False),
        (1, (s, s), (s, 2), True),
        (1, (-s, s), (-s, 2), True),
        (1, (2, s), (2, 2), True),
    )[number]


FOLLOW = {1: (3, 4, 5), 2: (6,), 3: (7,), 4: (8,), 5: (9,), 7: (10,)}


def segment_of(slot):
    return [lo <= slot < hi for lo, hi in SEGMENTS].index(True)


def chunk_of(slot):
    return [slot in chunk for chunk in CHUNKS].index(True)


def layer_norm(values_in, gain):
    average = jnp.mean(values_in, -1, keepdims=True)
    centred = values_in - average
    variance = jnp.mean(centred * centred, -1, keepdims=True)
    return centred * lax.rsqrt(variance + EPS) * gain


def kernel(
    sink_ref,
    q_hbm,
    res_hbm,
    gain_one_hbm,
    gain_two_hbm,
    k_hbm,
    v_hbm,
    doc_hbm,
    w_out_hbm,
    wg_hbm,
    wu_hbm,
    wd_hbm,
    out_ref,
    q_all,
    k_all,
    v_all,
    doc_all,
    gains_in,
    gains,
    res_all,
    w_out,
    gate_w,
    up_w,
    down_w,
    att,
    tokens,
    pre,
    normed,
    gate_acc,
    up_acc,
    hidden,
    parts,
    relays,
    arrived,
    local_sem,
    halo_send,
    halo_recv,
    ring_send,
    ring_recv,
    pair_send,
    pair_recv,
    down_recv,
    tok_send,
    tok_recv,
    norm_send,
    norm_recv,
    sum_send,
    relay_recv,
    sum_recv,
):
    sp = lax.axis_index("sp")
    tp = lax.axis_index("tp")
    sp_size = CHIPS * CORES
    core = lax.rem(sp, CORES)
    chip = sp // CORES
    my_y = lax.rem(chip, SIDE)
    my_z = chip // SIDE

    def chip_at(dz, dy):
        z = lax.rem(my_z + (dz + SIDE), SIDE)
        y = lax.rem(my_y + (dy + SIDE), SIDE)
        return z * SIDE + y

    rows = q_hbm.shape[0]
    token_rows = res_hbm.shape[0]
    depth = wg_hbm.shape[0]
    units = wg_hbm.shape[1]
    width = res_hbm.shape[1]
    sub_rows = depth // 2
    wide = CORES * depth
    half_rows = token_rows // 2

    def chip_lanes(slot):
        return pl.ds(pl.multiple_of(chip_at(*OFFSETS[slot]) * wide, wide), wide)

    def slot_lanes(slot):
        return slice(slot * wide, (slot + 1) * wide)

    along_z = [chip_at(1, 0) * CORES + core, chip_at(-1, 0) * CORES + core]
    along_y = [chip_at(0, 1) * CORES + core, chip_at(0, -1) * CORES + core]
    first_axis = [along_z[way] * (1 - core) + along_y[way] * core for way in range(2)]
    second_axis = [along_y[way] * (1 - core) + along_z[way] * core for way in range(2)]
    axes = ((along_z, along_y), (along_y, along_z), (first_axis, second_axis))
    partner = (chip * CORES + (1 - core), tp)
    after = (lax.rem(sp + 1, sp_size), tp)
    before = (lax.rem(sp + sp_size - 1, sp_size), tp)
    tp_right = lax.rem(tp + 1, TP)
    tp_left = lax.rem(tp + TP - 1, TP)
    tp_far = lax.rem(tp + 2, TP)
    sides = [(sp, tp_right), (sp, tp_left)]
    far = (sp, tp_far)

    barrier = pltpu.get_barrier_semaphore()
    greeted = [(axis[way], tp) for axis in (along_z, along_y) for way in range(2)]
    greeted += [partner, after, before, far] + sides
    for device in greeted:
        pl.semaphore_signal(barrier, inc=1, device_id=device, device_id_type=MESH)

    own_rows = pl.ds(pl.multiple_of(core * depth, depth), depth)
    loads = [
        pltpu.make_async_copy(src, dst, local_sem.at[i])
        for i, (src, dst) in enumerate(
            (
                (q_hbm, q_all),
                (k_hbm, k_all.at[pl.ds(HALF, rows)]),
                (v_hbm, v_all.at[pl.ds(HALF, rows)]),
                (doc_hbm, doc_all.at[:, pl.ds(HALF, rows)]),
                (w_out_hbm, w_out),
                (res_hbm, res_all),
                (gain_one_hbm, gains_in.at[pl.ds(0, 1)]),
                (gain_two_hbm, gains_in.at[pl.ds(1, 1)]),
                (wg_hbm, gate_w.at[own_rows]),
                (wu_hbm, up_w.at[own_rows]),
                (wd_hbm, down_w.at[own_rows]),
            )
        )
    ]
    for load in loads:
        load.start()

    def remote(src, dst, send, recv, device):
        return pltpu.make_async_remote_copy(
            src_ref=src, dst_ref=dst, send_sem=send, recv_sem=recv, device_id=device, device_id_type=MESH
        )

    def launch(copy):
        copy.start()

    def arrive(copy):
        copy.wait_recv()

    def wait_bytes(ref, sem):
        remote(ref, ref, sem, sem, partner).wait_recv()

    low, high = (pl.ds(HALF, HALF), pl.ds(rows, HALF))
    into_low, into_high = (pl.ds(0, HALF), pl.ds(HALF + rows, HALF))

    def launch_halos():
        for i, ref in enumerate((k_all, v_all)):
            launch(remote(ref.at[high], ref.at[into_low], halo_send.at[i], halo_recv.at[i], after))
            launch(remote(ref.at[low], ref.at[into_high], halo_send.at[i], halo_recv.at[i], before))
        for src, dst, to in ((high, into_low, after), (low, into_high, before)):
            launch(
                remote(doc_all.at[:, src], doc_all.at[:, dst], halo_send.at[2], halo_recv.at[2], to)
            )

    def halo_refs():
        edge = pl.ds(0, 2 * HALF)
        return (k_all.at[edge], v_all.at[edge], doc_all.at[:, edge])

    def halo_wait():
        for i, ref in enumerate(halo_refs()):
            wait_bytes(ref, halo_recv.at[i])

    buffers = (gate_w, up_w, down_w)

    def slot_for(kind, offset):
        straight, swapped = SLOT[offset], SLOT[offset[::-1]]
        return swapped if kind == 1 else straight

    def place(kind, offset, half, core_id):
        start = slot_for(kind, offset) * wide + core_id * depth
        if half is None:
            return buffers[kind].at[pl.ds(pl.multiple_of(start, depth), depth)]
        return buffers[kind].at[pl.ds(pl.multiple_of(start + half * sub_rows, sub_rows), sub_rows)]

    def ring(kind, number, way):
        axis, src_offset, dst_offset, halved = message(number, way)
        half = way if halved else None
        dst = place(kind, dst_offset, half, core)
        src = place(kind, src_offset, half, core)
        to = (axes[kind][axis][way], tp)
        return remote(src, dst, ring_send.at[kind], ring_recv.at[kind // 2, number - 1], to)

    def pair(kind, offset, half):
        dst = place(kind, offset, half, core)
        slot = slot_for(kind, offset)
        if kind == 2:
            sem = down_recv.at[chunk_of(slot)]
        else:
            sem = pair_recv.at[segment_of(slot)]
        return remote(dst, dst, pair_send.at[kind], sem, partner)

    def begin(number, kinds):
        for kind in kinds:
            for way in range(2):
                launch(ring(kind, number, way))

    def tick(number, kinds):
        halved = message(number, 0)[3]
        total = 2 * len(kinds) * (sub_rows if halved else depth)
        wait_bytes(buffers[kinds[0]].at[pl.ds(0, total)], ring_recv.at[kinds[0] // 2, number - 1])
        for follower in FOLLOW.get(number, ()):
            for kind in kinds:
                for way in range(2):
                    launch(ring(kind, follower, way))
        for kind in kinds:
            for way in range(2):
                _, _, offset, halved = message(number, way)
                launch(pair(kind, offset, way if halved else None))

    weights_tick = lambda number: tick(number, (0, 1))
    down_tick = lambda number: tick(number, (2,))

    def segment_wait(segment):
        lo, hi = SEGMENTS[segment]
        wait_bytes(gate_w.at[pl.ds(0, 2 * (hi - lo) * depth)], pair_recv.at[segment])

    span = rows + 2 * HALF
    at = lax.broadcasted_iota(jnp.int32, (1, span), 1) + (sp * rows - HALF)
    inside = jnp.logical_and(at >= 0, at < sp_size * rows)
    reach = 3 * HALF
    repeat = q_hbm.shape[1] // HEAD
    offset_of = lax.broadcasted_iota(jnp.int32, (HALF, reach), 1) - lax.broadcasted_iota(
        jnp.int32, (HALF, reach), 0
    )
    near = jnp.logical_and(offset_of >= 0, offset_of <= 2 * HALF)

    def attend(block):
        here = slice(block * HALF, (block + 1) * HALF)
        there = slice(block * HALF, block * HALF + reach)
        doc_row = doc_all[:, (block + 1) * HALF : (block + 2) * HALF]
        doc_query = jnp.broadcast_to(doc_row, (HALF, HALF)).T
        doc_keys = jnp.where(inside[:, there], doc_all[:, there], -1)
        same = jnp.concatenate([doc_query] * 3, 1) == doc_keys
        allowed = jnp.logical_and(near, same)
        key_blk = k_all[there, :]
        value_blk = v_all[there, :]
        for h in range(repeat):
            lanes = slice(h * HEAD, (h + 1) * HEAD)
            scores = lax.dot_general(
                q_all[here, lanes], key_blk, (((1,), (1,)), ((), ())), preferred_element_type=F32
            ) * HEAD ** (-0.5)
            scores = jnp.where(allowed, scores, NEGATIVE)
            sink = jnp.full((1, 1), sink_ref[h], F32)
            top = jnp.maximum(jnp.max(scores, -1, keepdims=True), sink)
            weights = jnp.exp(scores - top)
            total = jnp.sum(weights, -1, keepdims=True) + jnp.exp(sink - top)
            summed = jnp.dot(weights.astype(BF16), value_blk, preferred_element_type=F32)
            att[here, lanes] = (summed / total).astype(BF16)

    def token_rows_of(j):
        return pl.ds(pl.multiple_of(j * token_rows, token_rows), token_rows)

    def send_tokens():
        for j, into in ((tp_far, 3), (tp_right, 1), (tp_left, 2)):
            launch(
                remote(
                    att.at[token_rows_of(j)], tokens.at[into], tok_send.at[0], tok_recv.at[into // 3], (sp, j)
                )
            )
        tokens[0] = att[token_rows_of(tp), :]

    def order_gains():
        for slot in range(CHIPS):
            gains[:, slot_lanes(slot)] = gains_in[:, chip_lanes(slot)]

    def project(held):
        for first, second in zip(range(0, CHIPS, 2), range(1, CHIPS, 2)):
            picks = (chip_lanes(first), chip_lanes(second))
            lanes = slice(first * wide, (second + 1) * wide)
            if held[0] == 0:
                mixed = ALPHA * jnp.concatenate([res_all[:, pick] for pick in picks], 1).astype(F32)
            else:
                mixed = pre[:, lanes]
            for j in held:
                cols = q_hbm.shape[1]
                deep = pl.ds(pl.multiple_of((tp, tp_left, tp_right, tp_far)[j] * cols, cols), cols)
                mixed += jnp.dot(
                    tokens[j],
                    jnp.concatenate([w_out[deep, pick] for pick in picks], 1),
                    preferred_element_type=F32,
                )
            pre[:, lanes] = mixed

    strip = 64

    def norm_rows(first, last):
        @pl.loop(first // strip, last // strip)
        def _(t):
            here = pl.ds(pl.multiple_of(t * strip, strip), strip)
            normed[here, :] = layer_norm(pre[here, :], gains[0:1, :]).astype(BF16)

    def piece_rows(index):
        return pl.ds(index * half_rows, half_rows)

    ROUTES = ((0, 0, 2), (1, 1, 3), (0, 1, 4), (1, 0, 5), (0, 2, 6), (1, 3, 7))

    def norm_copy(route):
        way, src, dst = ROUTES[route]
        return remote(
            normed.at[piece_rows(src)],
            normed.at[piece_rows(dst)],
            norm_send.at[0],
            norm_recv.at[route // 2],
            sides[way],
        )

    def norm_arrive(stage):
        wait_bytes(normed.at[pl.ds(0, 2 * half_rows)], norm_recv.at[stage])

    def gate_up(top, bottom, lo, hi, lanes):
        deep = slice(lo * wide, hi * wide)
        gate = jnp.dot(normed[top:bottom, deep], gate_w[deep, lanes], preferred_element_type=F32)
        up = jnp.dot(normed[top:bottom, deep], up_w[deep, lanes], preferred_element_type=F32)
        if lo > 0:
            gate += gate_acc[top:bottom, lanes]
            up += up_acc[top:bottom, lanes]
        if hi < CHIPS:
            gate_acc[top:bottom, lanes] = gate
            up_acc[top:bottom, lanes] = up
        else:
            hidden[top:bottom, lanes] = (gate / (1.0 + jnp.exp(-gate)) * up).astype(BF16)

    def gate_up_tiles(top, bottom, lo, hi, first, last):
        @pl.loop(first, last)
        def _(t):
            gate_up(top, bottom, lo, hi, pl.ds(pl.multiple_of(t * 256, 256), 256))

    def gate_up_rest(top, bottom, lo, hi):
        gate_up(top, bottom, lo, hi, slice(units // 256 * 256, units))

    def gate_up_range(top, bottom, lo, hi):
        gate_up_tiles(top, bottom, lo, hi, 0, units // 256)
        gate_up_rest(top, bottom, lo, hi)

    def dest(index):
        return pl.ds(index * token_rows, token_rows)

    OWN, LEFT, RIGHT, FAR = range(4)
    ORDER = (0, 1, 2, 4, 5, 3, 6, 7)

    def down_chunk(k):
        wait_bytes(down_w.at[pl.ds(0, wide)], down_recv.at[k])
        a, b = CHUNKS[k]
        if b == a + 1:
            weights = down_w[a * wide : (b + 1) * wide, :]
        else:
            weights = jnp.concatenate([down_w[s * wide : (s + 1) * wide, :] for s in (a, b)], 0)
        part = lax.dot_general(
            hidden[...], weights, (((1,), (1,)), ((), ())), preferred_element_type=F32
        ).astype(BF16)
        for to, source in enumerate(ORDER):
            for slot, lanes in ((a, slice(0, wide)), (b, slice(wide, 2 * wide))):
                parts[slot, to * half_rows : (to + 1) * half_rows, :] = part[
                    source * half_rows : (source + 1) * half_rows, lanes
                ]
        launch(remote(parts.at[a, dest(FAR)], relays.at[k, 0], sum_send.at[0], relay_recv.at[k], sides[0]))
        launch(remote(parts.at[b, dest(FAR)], relays.at[k, 1], sum_send.at[0], relay_recv.at[k], sides[1]))

    def plain_chunk(k):
        a, b = CHUNKS[k]
        launch(remote(parts.at[b, dest(RIGHT)], arrived.at[k, 1], sum_send.at[0], sum_recv.at[k], sides[0]))
        launch(remote(parts.at[a, dest(LEFT)], arrived.at[k, 2], sum_send.at[0], sum_recv.at[k], sides[1]))

    def relay_chunk(k):
        wait_bytes(relays.at[k], relay_recv.at[k])
        for way, slot, to, index in ((0, CHUNKS[k][0], RIGHT, 0), (1, CHUNKS[k][1], LEFT, 3)):
            here = dest(to)
            parts[slot, here, :] = (
                parts[slot, here, :].astype(F32) + relays[k, way].astype(F32)
            ).astype(BF16)
            launch(
                remote(parts.at[slot, here], arrived.at[k, index], sum_send.at[0], sum_recv.at[k], sides[way])
            )

    first_core = lax.broadcasted_iota(jnp.int32, (token_rows, wide), 1) < depth

    def prepare_sum():
        pre[...] = ALPHA * normed[0:token_rows, :].astype(F32)

    def finish_chunk(k):
        wait_bytes(arrived.at[k], sum_recv.at[k])
        for slot, left, right in ((CHUNKS[k][0], 0, 2), (CHUNKS[k][1], 1, 3)):
            down = (
                parts[slot, dest(OWN), :].astype(F32)
                + arrived[k, left].astype(F32)
                + arrived[k, right].astype(F32)
            )
            swapped = SLOT[OFFSETS[slot][::-1]]
            if swapped == slot:
                pre[:, slot_lanes(slot)] += down
            else:
                pre[:, slot_lanes(slot)] += jnp.where(first_core, down, 0.0)
                pre[:, slot_lanes(swapped)] += jnp.where(first_core, 0.0, down)

    def final_norm():
        @pl.loop(0, token_rows // strip)
        def _(t):
            here = pl.ds(pl.multiple_of(t * strip, strip), strip)
            result = layer_norm(pre[here, :], gains[1:2, :]).astype(BF16)
            for slot in range(CHIPS):
                out_ref[here, chip_lanes(slot)] = result[:, slot_lanes(slot)]

    def sends_wait():
        def gone(ref, sem):
            remote(ref, ref, sem, sem, partner).wait_send()

        for i, ref in enumerate(halo_refs()):
            gone(ref, halo_send.at[i])
        for kind in range(3):
            gone(buffers[kind].at[pl.ds(0, (CHIPS - 1) * depth)], ring_send.at[kind])
            gone(buffers[kind].at[pl.ds(0, CHIPS * depth)], pair_send.at[kind])
        gone(tokens.at[pl.ds(0, TP - 1)], tok_send.at[0])
        gone(normed.at[pl.ds(0, 6 * half_rows)], norm_send.at[0])
        gone(parts.at[pl.ds(0, 12)], sum_send.at[0])

    pl.semaphore_wait(barrier, len(greeted))
    for load in loads[:4]:
        load.wait()
    launch_halos()
    for load in loads[8:]:
        load.wait()
    begin(1, (0, 1))
    begin(2, (0, 1))
    for kind in range(3):
        launch(pair(kind, (0, 0), None))
    attend(1)
    attend(2)
    halo_wait()
    attend(0)
    attend(3)
    send_tokens()
    weights_tick(1)
    for load in loads[4:8]:
        load.wait()
    order_gains()
    wait_bytes(tokens.at[pl.ds(0, 2)], tok_recv.at[0])
    project((0, 1, 2))
    wait_bytes(tokens.at[3], tok_recv.at[1])
    project((3,))
    norm_rows(0, half_rows)
    launch(norm_copy(0))
    norm_rows(half_rows, token_rows)
    for route in (1, 2, 3):
        launch(norm_copy(route))
    weights_tick(2)
    weights_tick(3)
    prepare_sum()
    weights_tick(4)
    norm_arrive(0)
    for route in (4, 5):
        launch(norm_copy(route))
    weights_tick(5)
    segment_wait(0)
    gate_up_range(0, 256, 0, 4)
    weights_tick(6)
    segment_wait(1)
    gate_up_range(0, 256, 4, 10)
    weights_tick(7)
    begin(1, (2,))
    norm_arrive(1)
    gate_up_range(256, 384, 0, 10)
    weights_tick(8)
    weights_tick(9)
    norm_arrive(2)
    begin(2, (2,))
    gate_up_tiles(384, 512, 0, 10, 0, 3)
    weights_tick(10)
    gate_up_tiles(384, 512, 0, 10, 3, 5)
    gate_up_rest(384, 512, 0, 10)
    segment_wait(2)
    gate_up_tiles(0, 512, 10, 16, 0, 2)
    down_tick(1)
    gate_up_tiles(0, 512, 10, 16, 2, 5)
    gate_up_rest(0, 512, 10, 16)
    down_tick(2)
    down_chunk(0)
    plain_chunk(0)
    down_chunk(1)
    plain_chunk(1)
    down_tick(3)
    down_tick(4)
    relay_chunk(0)
    down_chunk(2)
    plain_chunk(2)
    down_tick(5)
    down_tick(6)
    relay_chunk(1)
    down_chunk(3)
    plain_chunk(3)
    down_tick(7)
    down_chunk(4)
    plain_chunk(4)
    down_tick(8)
    relay_chunk(2)
    down_tick(9)
    down_chunk(5)
    plain_chunk(5)
    down_tick(10)
    down_chunk(6)
    relay_chunk(3)
    down_chunk(7)
    relay_chunk(4)
    plain_chunk(6)
    relay_chunk(5)
    plain_chunk(7)
    finish_chunk(0)
    finish_chunk(1)
    finish_chunk(2)
    relay_chunk(6)
    relay_chunk(7)
    finish_chunk(3)
    finish_chunk(4)
    finish_chunk(5)
    finish_chunk(6)
    finish_chunk(7)
    final_norm()
    sends_wait()


def solution(mesh):
    def per_device(
        queries,
        keys,
        values,
        doc_ids,
        sink_logit,
        residual_in,
        w_out,
        gain_one,
        w_gate,
        w_up,
        w_down,
        gain_two,
    ):
        rows = queries.shape[0]
        token_rows, width = residual_in.shape
        units = w_gate.shape[1]
        span = rows + 2 * HALF
        dma = pltpu.SemaphoreType.DMA
        vmem, anywhere = (pl.BlockSpec(memory_space=pltpu.VMEM), pl.BlockSpec(memory_space=pl.ANY))
        return pl.pallas_call(
            kernel,
            out_shape=pltpu.VMEM((token_rows, width), BF16),
            in_specs=[pl.BlockSpec(memory_space=pltpu.SMEM)] + [anywhere] * 11,
            out_specs=vmem,
            scratch_shapes=[
                pltpu.VMEM(queries.shape, BF16),
                pltpu.VMEM((span, keys.shape[1]), BF16),
                pltpu.VMEM((span, keys.shape[1]), BF16),
                pltpu.VMEM((1, span), jnp.int32),
                pltpu.VMEM((2, width), F32),
                pltpu.VMEM((2, width), F32),
                pltpu.VMEM((token_rows, width), BF16),
                pltpu.VMEM(w_out.shape, BF16),
                pltpu.VMEM((width, units), BF16),
                pltpu.VMEM((width, units), BF16),
                pltpu.VMEM((width, units), BF16),
                pltpu.VMEM(queries.shape, BF16),
                pltpu.VMEM((TP, token_rows, queries.shape[1]), BF16),
                pltpu.VMEM((token_rows, width), F32),
                pltpu.VMEM((rows, width), BF16),
                pltpu.VMEM((rows, units), F32),
                pltpu.VMEM((rows, units), F32),
                pltpu.VMEM((rows, units), BF16),
                pltpu.VMEM((CHIPS, rows, width // CHIPS), BF16),
                pltpu.VMEM((len(CHUNKS), 2, token_rows, width // CHIPS), BF16),
                pltpu.VMEM((len(CHUNKS), 4, token_rows, width // CHIPS), BF16),
                dma((11,)),
                dma((3,)),
                dma((3,)),
                dma((3,)),
                dma((2, LAST)),
                dma((3,)),
                dma((len(SEGMENTS),)),
                dma((len(CHUNKS),)),
                dma((1,)),
                dma((2,)),
                dma((1,)),
                dma((3,)),
                dma((1,)),
                dma((len(CHUNKS),)),
                dma((len(CHUNKS),)),
            ],
            compiler_params=pltpu.CompilerParams(
                collective_id=0, has_side_effects=True, vmem_limit_bytes=62 * 2**20
            ),
        )(
            sink_logit,
            queries,
            residual_in,
            gain_one[None, :],
            gain_two[None, :],
            keys,
            values,
            doc_ids[None, :],
            w_out,
            w_gate,
            w_up,
            w_down.T,
        )

    in_specs = (
        P("sp", "tp"),
        P("sp", "tp"),
        P("sp", "tp"),
        P("sp"),
        P("tp"),
        P(("sp", "tp"), None),
        P(),
        P(),
        P("sp", "tp"),
        P("sp", "tp"),
        P("tp", "sp"),
        P(),
    )
    return jax.shard_map(
        per_device, mesh=mesh, in_specs=in_specs, out_specs=P(("sp", "tp"), None), check_vma=False
    )
```

```python
import jax
import jax.numpy as jnp
from jax import lax
from jax.experimental import pallas as pl
from jax.experimental.pallas import tpu as pltpu
from jax.sharding import PartitionSpec as P

HEAD = 128
HALF = 128
CORES = 2
SIDE = 4
CHIPS = SIDE * SIDE
TP = 4
ALPHA = 2.0**0.5
EPS = 1e-05
NEGATIVE = -1e30
MESH = pl.DeviceIdType.MESH
BF16 = jnp.bfloat16
F32 = jnp.float32
OFFSETS = (
    (0, 0),
    (1, 0),
    (0, 1),
    (-1, 0),
    (0, -1),
    (1, 1),
    (-1, -1),
    (1, -1),
    (-1, 1),
    (2, 0),
    (0, 2),
    (2, 1),
    (1, 2),
    (2, -1),
    (-1, 2),
    (2, 2),
)
SLOT = {offset: slot for slot, offset in enumerate(OFFSETS)}
SEGMENTS = ((0, 4), (4, 10), (10, 14), (14, 16))
CHUNKS = ((1, 3), (2, 4), (0, 9), (5, 6), (7, 8), (11, 13), (12, 14), (10, 15))
LAST = 10


def message(number, way):
    s = 2 * way - 1
    return (
        None,
        (0, (0, 0), (s, 0), False),
        (1, (0, 0), (0, s), False),
        (0, (s, 0), (2, 0), True),
        (1, (s, 0), (s, s), False),
        (1, (-s, 0), (-s, s), False),
        (1, (0, s), (0, 2), True),
        (1, (2, 0), (2, s), False),
        (1, (s, s), (s, 2), True),
        (1, (-s, s), (-s, 2), True),
        (1, (2, s), (2, 2), True),
    )[number]


FOLLOW = {1: (3, 4, 5), 2: (6,), 3: (7,), 4: (8,), 5: (9,), 7: (10,)}
DOWN_FOLLOW = {1: (3, 4, 5), 3: (7, 6), 4: (8,), 5: (9,), 7: (10,)}


def segment_of(slot):
    return [lo <= slot < hi for lo, hi in SEGMENTS].index(True)


def chunk_of(slot):
    return [slot in chunk for chunk in CHUNKS].index(True)


def layer_norm(values_in, gain):
    average = jnp.mean(values_in, -1, keepdims=True)
    centred = values_in - average
    variance = jnp.mean(centred * centred, -1, keepdims=True)
    return centred * lax.rsqrt(variance + EPS) * gain


def kernel(
    sink_ref,
    q_hbm,
    res_hbm,
    gain_one_hbm,
    gain_two_hbm,
    k_hbm,
    v_hbm,
    doc_hbm,
    w_out_hbm,
    wg_hbm,
    wu_hbm,
    wd_hbm,
    out_ref,
    q_all,
    k_all,
    v_all,
    doc_all,
    gains_in,
    gains,
    res_all,
    w_out,
    gate_w,
    up_w,
    down_w,
    att,
    tokens,
    pre,
    normed,
    gate_acc,
    up_acc,
    hidden,
    parts,
    relays,
    arrived,
    local_sem,
    halo_send,
    halo_recv,
    ring_send,
    ring_recv,
    pair_send,
    pair_recv,
    down_recv,
    tok_send,
    tok_recv,
    norm_send,
    norm_recv,
    sum_send,
    relay_recv,
    sum_recv,
):
    sp = lax.axis_index("sp")
    tp = lax.axis_index("tp")
    sp_size = CHIPS * CORES
    core = lax.rem(sp, CORES)
    chip = sp // CORES
    my_y = lax.rem(chip, SIDE)
    my_z = chip // SIDE

    def chip_at(dz, dy):
        z = lax.rem(my_z + (dz + SIDE), SIDE)
        y = lax.rem(my_y + (dy + SIDE), SIDE)
        return z * SIDE + y

    rows = q_hbm.shape[0]
    token_rows = res_hbm.shape[0]
    depth = wg_hbm.shape[0]
    units = wg_hbm.shape[1]
    width = res_hbm.shape[1]
    sub_rows = depth // 2
    wide = CORES * depth
    half_rows = token_rows // 2

    def chip_lanes(slot):
        return pl.ds(pl.multiple_of(chip_at(*OFFSETS[slot]) * wide, wide), wide)

    def slot_lanes(slot):
        return slice(slot * wide, (slot + 1) * wide)

    along_z = [chip_at(1, 0) * CORES + core, chip_at(-1, 0) * CORES + core]
    along_y = [chip_at(0, 1) * CORES + core, chip_at(0, -1) * CORES + core]
    first_axis = [along_z[way] * (1 - core) + along_y[way] * core for way in range(2)]
    second_axis = [along_y[way] * (1 - core) + along_z[way] * core for way in range(2)]
    axes = ((along_z, along_y), (along_y, along_z), (first_axis, second_axis))
    partner = (chip * CORES + (1 - core), tp)
    after = (lax.rem(sp + 1, sp_size), tp)
    before = (lax.rem(sp + sp_size - 1, sp_size), tp)
    tp_right = lax.rem(tp + 1, TP)
    tp_left = lax.rem(tp + TP - 1, TP)
    tp_far = lax.rem(tp + 2, TP)
    sides = [(sp, tp_right), (sp, tp_left)]
    far = (sp, tp_far)

    barrier = pltpu.get_barrier_semaphore()
    greeted = [(axis[way], tp) for axis in (along_z, along_y) for way in range(2)]
    greeted += [partner, after, before, far] + sides
    for device in greeted:
        pl.semaphore_signal(barrier, inc=1, device_id=device, device_id_type=MESH)

    own_rows = pl.ds(pl.multiple_of(core * depth, depth), depth)
    loads = [
        pltpu.make_async_copy(src, dst, local_sem.at[i])
        for i, (src, dst) in enumerate(
            (
                (q_hbm, q_all),
                (k_hbm, k_all.at[pl.ds(HALF, rows)]),
                (v_hbm, v_all.at[pl.ds(HALF, rows)]),
                (doc_hbm, doc_all.at[:, pl.ds(HALF, rows)]),
                (w_out_hbm, w_out),
                (res_hbm, res_all),
                (gain_one_hbm, gains_in.at[pl.ds(0, 1)]),
                (gain_two_hbm, gains_in.at[pl.ds(1, 1)]),
                (wg_hbm, gate_w.at[own_rows]),
                (wu_hbm, up_w.at[own_rows]),
                (wd_hbm, down_w.at[own_rows]),
            )
        )
    ]
    for load in loads[:4] + loads[8:]:
        load.start()

    def remote(src, dst, send, recv, device):
        return pltpu.make_async_remote_copy(
            src_ref=src, dst_ref=dst, send_sem=send, recv_sem=recv, device_id=device, device_id_type=MESH
        )

    def launch(copy):
        copy.start()

    def arrive(copy):
        copy.wait_recv()

    def wait_bytes(ref, sem):
        remote(ref, ref, sem, sem, partner).wait_recv()

    low, high = (pl.ds(HALF, HALF), pl.ds(rows, HALF))
    into_low, into_high = (pl.ds(0, HALF), pl.ds(HALF + rows, HALF))

    def launch_halos():
        for i, ref in enumerate((k_all, v_all)):
            launch(remote(ref.at[high], ref.at[into_low], halo_send.at[i], halo_recv.at[i], after))
            launch(remote(ref.at[low], ref.at[into_high], halo_send.at[i], halo_recv.at[i], before))
        for src, dst, to in ((high, into_low, after), (low, into_high, before)):
            launch(
                remote(doc_all.at[:, src], doc_all.at[:, dst], halo_send.at[2], halo_recv.at[2], to)
            )

    def halo_refs():
        edge = pl.ds(0, 2 * HALF)
        return (k_all.at[edge], v_all.at[edge], doc_all.at[:, edge])

    def halo_wait():
        for i, ref in enumerate(halo_refs()):
            wait_bytes(ref, halo_recv.at[i])

    buffers = (gate_w, up_w, down_w)

    def slot_for(kind, offset):
        straight, swapped = SLOT[offset], SLOT[offset[::-1]]
        return swapped if kind == 1 else straight

    def place(kind, offset, half, core_id):
        start = slot_for(kind, offset) * wide + core_id * depth
        if half is None:
            return buffers[kind].at[pl.ds(pl.multiple_of(start, depth), depth)]
        return buffers[kind].at[pl.ds(pl.multiple_of(start + half * sub_rows, sub_rows), sub_rows)]

    def ring(kind, number, way):
        axis, src_offset, dst_offset, halved = message(number, way)
        half = way if halved else None
        dst = place(kind, dst_offset, half, core)
        src = place(kind, src_offset, half, core)
        to = (axes[kind][axis][way], tp)
        return remote(src, dst, ring_send.at[kind], ring_recv.at[kind // 2, number - 1], to)

    def pair(kind, offset, half):
        dst = place(kind, offset, half, core)
        slot = slot_for(kind, offset)
        if kind == 2:
            sem = down_recv.at[chunk_of(slot)]
        else:
            sem = pair_recv.at[segment_of(slot)]
        return remote(dst, dst, pair_send.at[kind], sem, partner)

    def begin(number, kinds):
        for kind in kinds:
            for way in range(2):
                launch(ring(kind, number, way))

    def tick(number, kinds):
        halved = message(number, 0)[3]
        total = 2 * len(kinds) * (sub_rows if halved else depth)
        wait_bytes(buffers[kinds[0]].at[pl.ds(0, total)], ring_recv.at[kinds[0] // 2, number - 1])
        for follower in (DOWN_FOLLOW if kinds[0] == 2 else FOLLOW).get(number, ()):
            for kind in kinds:
                for way in range(2):
                    launch(ring(kind, follower, way))
        for kind in kinds:
            for way in range(2):
                _, _, offset, halved = message(number, way)
                launch(pair(kind, offset, way if halved else None))

    weights_tick = lambda number: tick(number, (0, 1))
    down_tick = lambda number: tick(number, (2,))

    def segment_wait(segment):
        lo, hi = SEGMENTS[segment]
        wait_bytes(gate_w.at[pl.ds(0, 2 * (hi - lo) * depth)], pair_recv.at[segment])

    span = rows + 2 * HALF
    at = lax.broadcasted_iota(jnp.int32, (1, span), 1) + (sp * rows - HALF)
    inside = jnp.logical_and(at >= 0, at < sp_size * rows)
    reach = 3 * HALF
    repeat = q_hbm.shape[1] // HEAD
    offset_of = lax.broadcasted_iota(jnp.int32, (HALF, reach), 1) - lax.broadcasted_iota(
        jnp.int32, (HALF, reach), 0
    )
    near = jnp.logical_and(offset_of >= 0, offset_of <= 2 * HALF)

    def attend(block):
        here = slice(block * HALF, (block + 1) * HALF)
        there = slice(block * HALF, block * HALF + reach)
        doc_row = doc_all[:, (block + 1) * HALF : (block + 2) * HALF]
        doc_query = jnp.broadcast_to(doc_row, (HALF, HALF)).T
        doc_keys = jnp.where(inside[:, there], doc_all[:, there], -1)
        same = jnp.concatenate([doc_query] * 3, 1) == doc_keys
        allowed = jnp.logical_and(near, same)
        key_blk = k_all[there, :]
        value_blk = v_all[there, :]
        for h in range(repeat):
            lanes = slice(h * HEAD, (h + 1) * HEAD)
            scores = lax.dot_general(
                q_all[here, lanes], key_blk, (((1,), (1,)), ((), ())), preferred_element_type=F32
            ) * HEAD ** (-0.5)
            scores = jnp.where(allowed, scores, NEGATIVE)
            sink = jnp.full((1, 1), sink_ref[h], F32)
            top = jnp.maximum(jnp.max(scores, -1, keepdims=True), sink)
            weights = jnp.exp(scores - top)
            total = jnp.sum(weights, -1, keepdims=True) + jnp.exp(sink - top)
            summed = jnp.dot(weights.astype(BF16), value_blk, preferred_element_type=F32)
            att[here, lanes] = (summed / total).astype(BF16)

    def token_rows_of(j):
        return pl.ds(pl.multiple_of(j * token_rows, token_rows), token_rows)

    def send_tokens():
        for j, into in ((tp_far, 3), (tp_right, 1), (tp_left, 2)):
            launch(
                remote(
                    att.at[token_rows_of(j)], tokens.at[into], tok_send.at[0], tok_recv.at[into // 3], (sp, j)
                )
            )
        tokens[0] = att[token_rows_of(tp), :]

    def order_gains():
        for slot in range(CHIPS):
            gains[:, slot_lanes(slot)] = gains_in[:, chip_lanes(slot)]

    def project(held):
        for first, second in zip(range(0, CHIPS, 2), range(1, CHIPS, 2)):
            picks = (chip_lanes(first), chip_lanes(second))
            lanes = slice(first * wide, (second + 1) * wide)
            if held[0] == 0:
                mixed = ALPHA * jnp.concatenate([res_all[:, pick] for pick in picks], 1).astype(F32)
            else:
                mixed = pre[:, lanes]
            for j in held:
                cols = q_hbm.shape[1]
                deep = pl.ds(pl.multiple_of((tp, tp_left, tp_right, tp_far)[j] * cols, cols), cols)
                mixed += jnp.dot(
                    tokens[j],
                    jnp.concatenate([w_out[deep, pick] for pick in picks], 1),
                    preferred_element_type=F32,
                )
            pre[:, lanes] = mixed

    strip = 64

    def norm_rows(first, last):
        @pl.loop(first // strip, last // strip)
        def _(t):
            here = pl.ds(pl.multiple_of(t * strip, strip), strip)
            normed[here, :] = layer_norm(pre[here, :], gains[0:1, :]).astype(BF16)

    def piece_rows(index):
        return pl.ds(index * half_rows, half_rows)

    ROUTES = ((0, 0, 2), (1, 1, 3), (0, 1, 4), (1, 0, 5), (0, 2, 6), (1, 3, 7))

    def norm_copy(route):
        way, src, dst = ROUTES[route]
        return remote(
            normed.at[piece_rows(src)],
            normed.at[piece_rows(dst)],
            norm_send.at[0],
            norm_recv.at[route // 2],
            sides[way],
        )

    def norm_arrive(stage):
        wait_bytes(normed.at[pl.ds(0, 2 * half_rows)], norm_recv.at[stage])

    def gate_up(top, bottom, lo, hi, lanes):
        deep = slice(lo * wide, hi * wide)
        gate = jnp.dot(normed[top:bottom, deep], gate_w[deep, lanes], preferred_element_type=F32)
        up = jnp.dot(normed[top:bottom, deep], up_w[deep, lanes], preferred_element_type=F32)
        if lo > 0:
            gate += gate_acc[top:bottom, lanes]
            up += up_acc[top:bottom, lanes]
        if hi < CHIPS:
            gate_acc[top:bottom, lanes] = gate
            up_acc[top:bottom, lanes] = up
        else:
            hidden[top:bottom, lanes] = (gate / (1.0 + jnp.exp(-gate)) * up).astype(BF16)

    def gate_up_range(top, bottom, lo, hi):
        for start in range(0, units, 256):
            gate_up(top, bottom, lo, hi, slice(start, min(start + 256, units)))

    LEFT, RIGHT, OWN, FAR = range(4)
    def down_rows(k, top, bottom, pieces):
        a, b = CHUNKS[k]
        if b == a + 1:
            weights = down_w[a * wide : (b + 1) * wide, :]
        else:
            weights = jnp.concatenate([down_w[s * wide : (s + 1) * wide, :] for s in (a, b)], 0)
        part = lax.dot_general(
            hidden[top:bottom, :], weights, (((1,), (1,)), ((), ())), preferred_element_type=F32
        ).astype(BF16)
        for source, to in enumerate(pieces):
            for side, lanes in ((0, slice(0, wide)), (1, slice(wide, 2 * wide))):
                parts[to // 2, k, side, to % 2 * half_rows : (to % 2 + 1) * half_rows, :] = part[
                    source * half_rows : (source + 1) * half_rows, lanes
                ]

    def down_far(k):
        wait_bytes(down_w.at[pl.ds(0, wide)], down_recv.at[k])
        down_rows(k, 3 * token_rows, 4 * token_rows, (6, 7))
        for way in range(2):
            launch(
                remote(
                    parts.at[FAR, k, way], relays.at[k, way], sum_send.at[0], relay_recv.at[k], sides[way]
                )
            )

    def down_rest(k):
        down_rows(k, 0, 3 * token_rows, (4, 5, 0, 3, 1, 2))

    def plain_chunk(k):
        for way, to, side in ((0, RIGHT, 1), (1, LEFT, 0)):
            launch(
                remote(
                    parts.at[to, k, side], arrived.at[k, to, side], sum_send.at[0], sum_recv.at[k], sides[way]
                )
            )

    def relay_chunk(k, whole):
        wait_bytes(relays.at[k], relay_recv.at[k])
        for way, to in ((0, RIGHT), (1, LEFT)):
            parts[to, k, way] = (parts[to, k, way].astype(F32) + relays[k, way].astype(F32)).astype(BF16)
            piece = (to, k) if whole else (to, k, way)
            into = (k, to) if whole else (k, to, way)
            launch(remote(parts.at[piece], arrived.at[into], sum_send.at[0], sum_recv.at[k], sides[way]))

    first_core = lax.broadcasted_iota(jnp.int32, (token_rows, wide), 1) < depth

    def prepare_sum():
        pre[...] = ALPHA * normed[0:token_rows, :].astype(F32)

    def finish_chunk(k):
        wait_bytes(arrived.at[k], sum_recv.at[k])
        for side, slot in enumerate(CHUNKS[k]):
            down = (
                parts[OWN, k, side].astype(F32)
                + arrived[k, LEFT, side].astype(F32)
                + arrived[k, RIGHT, side].astype(F32)
            )
            swapped = SLOT[OFFSETS[slot][::-1]]
            if swapped == slot:
                pre[:, slot_lanes(slot)] += down
            else:
                pre[:, slot_lanes(slot)] += jnp.where(first_core, down, 0.0)
                pre[:, slot_lanes(swapped)] += jnp.where(first_core, 0.0, down)

    def final_norm():
        @pl.loop(0, token_rows // strip)
        def _(t):
            here = pl.ds(pl.multiple_of(t * strip, strip), strip)
            result = layer_norm(pre[here, :], gains[1:2, :]).astype(BF16)
            for slot in range(CHIPS):
                out_ref[here, chip_lanes(slot)] = result[:, slot_lanes(slot)]

    def sends_wait():
        def gone(ref, sem):
            remote(ref, ref, sem, sem, partner).wait_send()

        for i, ref in enumerate(halo_refs()):
            gone(ref, halo_send.at[i])
        for kind in range(3):
            gone(buffers[kind].at[pl.ds(0, (CHIPS - 1) * depth)], ring_send.at[kind])
            gone(buffers[kind].at[pl.ds(0, CHIPS * depth)], pair_send.at[kind])
        gone(tokens.at[pl.ds(0, TP - 1)], tok_send.at[0])
        gone(normed.at[pl.ds(0, 6 * half_rows)], norm_send.at[0])
        gone(parts.at[pl.ds(0, 3)], sum_send.at[0])

    for load in loads[:4]:
        load.wait()
    attend(1)
    pl.semaphore_wait(barrier, len(greeted))
    launch_halos()
    for load in loads[8:]:
        load.wait()
    begin(1, (0, 1))
    begin(2, (0, 1))
    for kind in range(3):
        launch(pair(kind, (0, 0), None))
    for load in loads[4:8]:
        load.start()
    attend(2)
    halo_wait()
    attend(0)
    attend(3)
    send_tokens()
    weights_tick(1)
    for load in loads[4:8]:
        load.wait()
    order_gains()
    wait_bytes(tokens.at[pl.ds(0, 2)], tok_recv.at[0])
    project((0, 1, 2))
    wait_bytes(tokens.at[3], tok_recv.at[1])
    project((3,))
    norm_rows(0, half_rows)
    launch(norm_copy(0))
    norm_rows(half_rows, token_rows)
    for route in (1, 2, 3):
        launch(norm_copy(route))
    weights_tick(2)
    weights_tick(3)
    prepare_sum()
    weights_tick(4)
    norm_arrive(0)
    for route in (4, 5):
        launch(norm_copy(route))
    weights_tick(5)
    segment_wait(0)
    gate_up_range(0, 256, 0, 4)
    weights_tick(6)
    segment_wait(1)
    gate_up_range(0, 256, 4, 10)
    weights_tick(7)
    begin(1, (2,))
    norm_arrive(1)
    gate_up_range(256, 384, 0, 10)
    weights_tick(8)
    weights_tick(9)
    norm_arrive(2)
    begin(2, (2,))
    gate_up_range(384, 512, 0, 10)
    weights_tick(10)
    segment_wait(2)
    gate_up_range(0, 512, 10, 14)
    down_tick(1)
    segment_wait(3)
    gate_up_range(0, 256, 14, 16)
    down_tick(2)
    gate_up_range(256, 512, 14, 16)
    down_far(0)
    down_far(1)
    down_rest(0)
    plain_chunk(0)
    down_tick(3)
    down_rest(1)
    plain_chunk(1)
    down_tick(4)
    relay_chunk(0, False)
    down_far(2)
    relay_chunk(1, False)
    down_rest(2)
    plain_chunk(2)
    down_tick(5)
    down_far(3)
    down_rest(3)
    plain_chunk(3)
    down_tick(7)
    down_far(4)
    relay_chunk(2, False)
    down_tick(6)
    down_rest(4)
    plain_chunk(4)
    down_tick(8)
    down_far(5)
    relay_chunk(3, False)
    down_tick(9)
    down_rest(5)
    plain_chunk(5)
    down_tick(10)
    down_far(6)
    relay_chunk(4, False)
    down_far(7)
    down_rest(6)
    plain_chunk(6)
    relay_chunk(5, False)
    down_rest(7)
    plain_chunk(7)
    relay_chunk(6, False)
    finish_chunk(0)
    finish_chunk(1)
    finish_chunk(2)
    relay_chunk(7, False)
    finish_chunk(3)
    finish_chunk(4)
    finish_chunk(5)
    finish_chunk(6)
    finish_chunk(7)
    final_norm()
    sends_wait()


def solution(mesh):
    def per_device(
        queries,
        keys,
        values,
        doc_ids,
        sink_logit,
        residual_in,
        w_out,
        gain_one,
        w_gate,
        w_up,
        w_down,
        gain_two,
    ):
        rows = queries.shape[0]
        token_rows, width = residual_in.shape
        units = w_gate.shape[1]
        span = rows + 2 * HALF
        dma = pltpu.SemaphoreType.DMA
        vmem, anywhere = (pl.BlockSpec(memory_space=pltpu.VMEM), pl.BlockSpec(memory_space=pl.ANY))
        return pl.pallas_call(
            kernel,
            out_shape=pltpu.VMEM((token_rows, width), BF16),
            in_specs=[pl.BlockSpec(memory_space=pltpu.SMEM)] + [anywhere] * 11,
            out_specs=vmem,
            scratch_shapes=[
                pltpu.VMEM(queries.shape, BF16),
                pltpu.VMEM((span, keys.shape[1]), BF16),
                pltpu.VMEM((span, keys.shape[1]), BF16),
                pltpu.VMEM((1, span), jnp.int32),
                pltpu.VMEM((2, width), F32),
                pltpu.VMEM((2, width), F32),
                pltpu.VMEM((token_rows, width), BF16),
                pltpu.VMEM(w_out.shape, BF16),
                pltpu.VMEM((width, units), BF16),
                pltpu.VMEM((width, units), BF16),
                pltpu.VMEM((width, units), BF16),
                pltpu.VMEM(queries.shape, BF16),
                pltpu.VMEM((TP, token_rows, queries.shape[1]), BF16),
                pltpu.VMEM((token_rows, width), F32),
                pltpu.VMEM((rows, width), BF16),
                pltpu.VMEM((rows, units), F32),
                pltpu.VMEM((rows, units), F32),
                pltpu.VMEM((rows, units), BF16),
                pltpu.VMEM((4, len(CHUNKS), 2, token_rows, width // CHIPS), BF16),
                pltpu.VMEM((len(CHUNKS), 2, token_rows, width // CHIPS), BF16),
                pltpu.VMEM((len(CHUNKS), 2, 2, token_rows, width // CHIPS), BF16),
                dma((11,)),
                dma((3,)),
                dma((3,)),
                dma((3,)),
                dma((2, LAST)),
                dma((3,)),
                dma((len(SEGMENTS),)),
                dma((len(CHUNKS),)),
                dma((1,)),
                dma((2,)),
                dma((1,)),
                dma((3,)),
                dma((1,)),
                dma((len(CHUNKS),)),
                dma((len(CHUNKS),)),
            ],
            compiler_params=pltpu.CompilerParams(
                collective_id=0, has_side_effects=True, vmem_limit_bytes=62 * 2**20
            ),
        )(
            sink_logit,
            queries,
            residual_in,
            gain_one[None, :],
            gain_two[None, :],
            keys,
            values,
            doc_ids[None, :],
            w_out,
            w_gate,
            w_up,
            w_down.T,
        )

    in_specs = (
        P("sp", "tp"),
        P("sp", "tp"),
        P("sp", "tp"),
        P("sp"),
        P("tp"),
        P(("sp", "tp"), None),
        P(),
        P(),
        P("sp", "tp"),
        P("sp", "tp"),
        P("tp", "sp"),
        P(),
    )
    return jax.shard_map(
        per_device, mesh=mesh, in_specs=in_specs, out_specs=P(("sp", "tp"), None), check_vma=False
    )
```

```python
import jax
import jax.numpy as jnp
from jax import lax
from jax.experimental import pallas as pl
from jax.experimental.pallas import tpu as pltpu
from jax.sharding import PartitionSpec as P

HEAD = 128
HALF = 128
CORES = 2
SIDE = 4
CHIPS = SIDE * SIDE
TP = 4
ALPHA = 2.0**0.5
EPS = 1e-05
NEGATIVE = -1e30
MESH = pl.DeviceIdType.MESH
BF16 = jnp.bfloat16
F32 = jnp.float32
OFFSETS = (
    (0, 0),
    (1, 0),
    (0, 1),
    (-1, 0),
    (0, -1),
    (1, 1),
    (-1, -1),
    (1, -1),
    (-1, 1),
    (2, 0),
    (0, 2),
    (2, 1),
    (1, 2),
    (2, -1),
    (-1, 2),
    (2, 2),
)
SLOT = {offset: slot for slot, offset in enumerate(OFFSETS)}
SEGMENTS = ((0, 4), (4, 10), (10, 14), (14, 16))
CHUNKS = ((1, 3), (2, 4), (0, 9), (5, 6), (7, 8), (11, 13), (12, 14), (10, 15))
LAST = 10


def message(number, way):
    s = 2 * way - 1
    return (
        None,
        (0, (0, 0), (s, 0), False),
        (1, (0, 0), (0, s), False),
        (0, (s, 0), (2, 0), True),
        (1, (s, 0), (s, s), False),
        (1, (-s, 0), (-s, s), False),
        (1, (0, s), (0, 2), True),
        (1, (2, 0), (2, s), False),
        (1, (s, s), (s, 2), True),
        (1, (-s, s), (-s, 2), True),
        (1, (2, s), (2, 2), True),
    )[number]


FOLLOW = {1: (3, 4, 5), 2: (6,), 3: (7,), 4: (8,), 5: (9,), 7: (10,)}
DOWN_FOLLOW = {1: (3, 4, 5), 3: (7, 6), 4: (8,), 5: (9,), 7: (10,)}


def segment_of(slot):
    return [lo <= slot < hi for lo, hi in SEGMENTS].index(True)


def chunk_of(slot):
    return [slot in chunk for chunk in CHUNKS].index(True)


def layer_norm(values_in, gain):
    average = jnp.mean(values_in, -1, keepdims=True)
    centred = values_in - average
    variance = jnp.mean(centred * centred, -1, keepdims=True)
    return centred * lax.rsqrt(variance + EPS) * gain


def kernel(
    sink_ref,
    q_hbm,
    res_hbm,
    gain_one_hbm,
    gain_two_hbm,
    k_hbm,
    v_hbm,
    doc_hbm,
    w_out_hbm,
    wg_hbm,
    wu_hbm,
    wd_hbm,
    out_ref,
    q_all,
    k_all,
    v_all,
    doc_all,
    gains_in,
    gains,
    res_all,
    w_out,
    weights,
    att,
    tokens,
    pre,
    normed,
    gate_acc,
    up_acc,
    hidden,
    parts,
    relays,
    arrived,
    local_sem,
    halo_send,
    halo_recv,
    ring_send,
    ring_recv,
    pair_send,
    pair_recv,
    down_recv,
    tok_send,
    tok_recv,
    norm_send,
    norm_recv,
    sum_send,
    relay_recv,
    sum_recv,
):
    gate_w, up_w, down_w = (weights.at[i] for i in range(3))
    sp = lax.axis_index("sp")
    tp = lax.axis_index("tp")
    sp_size = CHIPS * CORES
    core = lax.rem(sp, CORES)
    chip = sp // CORES
    my_y = lax.rem(chip, SIDE)
    my_z = chip // SIDE

    def chip_at(dz, dy):
        z = lax.rem(my_z + (dz + SIDE), SIDE)
        y = lax.rem(my_y + (dy + SIDE), SIDE)
        return z * SIDE + y

    rows = q_hbm.shape[0]
    token_rows = res_hbm.shape[0]
    depth = wg_hbm.shape[0]
    units = wg_hbm.shape[1]
    width = res_hbm.shape[1]
    sub_rows = depth // 2
    wide = CORES * depth
    half_rows = token_rows // 2

    def chip_lanes(slot):
        return pl.ds(pl.multiple_of(chip_at(*OFFSETS[slot]) * wide, wide), wide)

    def slot_lanes(slot):
        return slice(slot * wide, (slot + 1) * wide)

    along_z = [chip_at(1, 0) * CORES + core, chip_at(-1, 0) * CORES + core]
    along_y = [chip_at(0, 1) * CORES + core, chip_at(0, -1) * CORES + core]
    first_axis = [along_z[way] * (1 - core) + along_y[way] * core for way in range(2)]
    second_axis = [along_y[way] * (1 - core) + along_z[way] * core for way in range(2)]
    axes = ((along_z, along_y), (along_y, along_z), (first_axis, second_axis))
    partner = (chip * CORES + (1 - core), tp)
    after = (lax.rem(sp + 1, sp_size), tp)
    before = (lax.rem(sp + sp_size - 1, sp_size), tp)
    tp_right = lax.rem(tp + 1, TP)
    tp_left = lax.rem(tp + TP - 1, TP)
    tp_far = lax.rem(tp + 2, TP)
    sides = [(sp, tp_right), (sp, tp_left)]
    far = (sp, tp_far)

    barrier = pltpu.get_barrier_semaphore()
    greeted = [(axis[way], tp) for axis in (along_z, along_y) for way in range(2)]
    greeted += [partner, after, before, far] + sides
    for device in greeted:
        pl.semaphore_signal(barrier, inc=1, device_id=device, device_id_type=MESH)

    own_rows = pl.ds(pl.multiple_of(core * depth, depth), depth)
    def load(src, dst, sem):
        pltpu.make_async_copy(src, dst, local_sem.at[sem]).start()

    def loaded(ref, sem):
        pltpu.make_async_copy(ref, ref, local_sem.at[sem]).wait()

    load(k_hbm, k_all.at[pl.ds(HALF, rows)], 0)
    load(v_hbm, v_all.at[pl.ds(HALF, rows)], 0)
    load(q_hbm, q_all, 0)
    load(doc_hbm, doc_all.at[:, pl.ds(HALF, rows)], 1)
    for i, src in enumerate((wg_hbm, wu_hbm, wd_hbm)):
        load(src, weights.at[i, own_rows], 2)

    def remote(src, dst, send, recv, device):
        return pltpu.make_async_remote_copy(
            src_ref=src, dst_ref=dst, send_sem=send, recv_sem=recv, device_id=device, device_id_type=MESH
        )

    def launch(copy):
        copy.start()

    def arrive(copy):
        copy.wait_recv()

    def wait_bytes(ref, sem):
        remote(ref, ref, sem, sem, partner).wait_recv()

    low, high = (pl.ds(HALF, HALF), pl.ds(rows, HALF))
    into_low, into_high = (pl.ds(0, HALF), pl.ds(HALF + rows, HALF))

    def launch_halos():
        for i, ref in enumerate((k_all, v_all)):
            launch(remote(ref.at[high], ref.at[into_low], halo_send.at[0], halo_recv.at[0], after))
            launch(remote(ref.at[low], ref.at[into_high], halo_send.at[0], halo_recv.at[0], before))
        for src, dst, to in ((high, into_low, after), (low, into_high, before)):
            launch(
                remote(doc_all.at[:, src], doc_all.at[:, dst], halo_send.at[1], halo_recv.at[1], to)
            )

    def halo_refs():
        return (k_all.at[pl.ds(0, 4 * HALF)], doc_all.at[:, pl.ds(0, 2 * HALF)])

    def halo_wait():
        for i, ref in enumerate(halo_refs()):
            wait_bytes(ref, halo_recv.at[i])

    buffers = (gate_w, up_w, down_w)

    def slot_for(kind, offset):
        straight, swapped = SLOT[offset], SLOT[offset[::-1]]
        return swapped if kind == 1 else straight

    def place(kind, offset, half, core_id):
        start = slot_for(kind, offset) * wide + core_id * depth
        if half is None:
            return buffers[kind].at[pl.ds(pl.multiple_of(start, depth), depth)]
        return buffers[kind].at[pl.ds(pl.multiple_of(start + half * sub_rows, sub_rows), sub_rows)]

    def ring(kind, number, way):
        axis, src_offset, dst_offset, halved = message(number, way)
        half = way if halved else None
        dst = place(kind, dst_offset, half, core)
        src = place(kind, src_offset, half, core)
        to = (axes[kind][axis][way], tp)
        return remote(src, dst, ring_send.at[0], ring_recv.at[kind // 2, number - 1], to)

    def pair(kind, offset, half):
        dst = place(kind, offset, half, core)
        slot = slot_for(kind, offset)
        if kind == 2:
            sem = down_recv.at[chunk_of(slot)]
        else:
            sem = pair_recv.at[segment_of(slot)]
        return remote(dst, dst, pair_send.at[0], sem, partner)

    def begin(number, kinds):
        for kind in kinds:
            for way in range(2):
                launch(ring(kind, number, way))

    def tick(number, kinds):
        halved = message(number, 0)[3]
        total = 2 * len(kinds) * (sub_rows if halved else depth)
        wait_bytes(buffers[kinds[0]].at[pl.ds(0, total)], ring_recv.at[kinds[0] // 2, number - 1])
        for follower in (DOWN_FOLLOW if kinds[0] == 2 else FOLLOW).get(number, ()):
            for kind in kinds:
                for way in range(2):
                    launch(ring(kind, follower, way))
        for kind in kinds:
            for way in range(2):
                _, _, offset, halved = message(number, way)
                launch(pair(kind, offset, way if halved else None))

    weights_tick = lambda number: tick(number, (0, 1))
    down_tick = lambda number: tick(number, (2,))

    def segment_wait(segment):
        lo, hi = SEGMENTS[segment]
        wait_bytes(gate_w.at[pl.ds(0, 2 * (hi - lo) * depth)], pair_recv.at[segment])

    span = rows + 2 * HALF
    at = lax.broadcasted_iota(jnp.int32, (1, span), 1) + (sp * rows - HALF)
    inside = jnp.logical_and(at >= 0, at < sp_size * rows)
    reach = 3 * HALF
    repeat = q_hbm.shape[1] // HEAD
    offset_of = lax.broadcasted_iota(jnp.int32, (HALF, reach), 1) - lax.broadcasted_iota(
        jnp.int32, (HALF, reach), 0
    )
    near = jnp.logical_and(offset_of >= 0, offset_of <= 2 * HALF)

    def attend(block):
        here = slice(block * HALF, (block + 1) * HALF)
        there = slice(block * HALF, block * HALF + reach)
        doc_row = doc_all[:, (block + 1) * HALF : (block + 2) * HALF]
        doc_query = jnp.broadcast_to(doc_row, (HALF, HALF)).T
        doc_keys = jnp.where(inside[:, there], doc_all[:, there], -1)
        same = jnp.concatenate([doc_query] * 3, 1) == doc_keys
        allowed = jnp.logical_and(near, same)
        key_blk = k_all[there, :]
        value_blk = v_all[there, :]
        for h in range(repeat):
            lanes = slice(h * HEAD, (h + 1) * HEAD)
            scores = lax.dot_general(
                q_all[here, lanes], key_blk, (((1,), (1,)), ((), ())), preferred_element_type=F32
            ) * HEAD ** (-0.5)
            scores = jnp.where(allowed, scores, NEGATIVE)
            sink = jnp.full((1, 1), sink_ref[h], F32)
            top = jnp.maximum(jnp.max(scores, -1, keepdims=True), sink)
            weights = jnp.exp(scores - top)
            total = jnp.sum(weights, -1, keepdims=True) + jnp.exp(sink - top)
            summed = jnp.dot(weights.astype(BF16), value_blk, preferred_element_type=F32)
            att[here, lanes] = (summed / total).astype(BF16)

    def token_rows_of(j):
        return pl.ds(pl.multiple_of(j * token_rows, token_rows), token_rows)

    def send_tokens():
        for j, into in ((tp_far, 3), (tp_right, 1), (tp_left, 2)):
            launch(
                remote(
                    att.at[token_rows_of(j)], tokens.at[into], tok_send.at[0], tok_recv.at[into // 3], (sp, j)
                )
            )
        tokens[0] = att[token_rows_of(tp), :]

    def order_gains():
        for slot in range(CHIPS):
            gains[:, slot_lanes(slot)] = gains_in[:, chip_lanes(slot)]

    def project(held):
        for first, second in zip(range(0, CHIPS, 2), range(1, CHIPS, 2)):
            picks = (chip_lanes(first), chip_lanes(second))
            lanes = slice(first * wide, (second + 1) * wide)
            if held[0] == 0:
                mixed = ALPHA * jnp.concatenate([res_all[:, pick] for pick in picks], 1).astype(F32)
            else:
                mixed = pre[:, lanes]
            for j in held:
                cols = q_hbm.shape[1]
                deep = pl.ds(pl.multiple_of((tp, tp_left, tp_right, tp_far)[j] * cols, cols), cols)
                mixed += jnp.dot(
                    tokens[j],
                    jnp.concatenate([w_out[deep, pick] for pick in picks], 1),
                    preferred_element_type=F32,
                )
            pre[:, lanes] = mixed

    strip = 64

    def norm_rows(first, last):
        @pl.loop(first // strip, last // strip)
        def _(t):
            here = pl.ds(pl.multiple_of(t * strip, strip), strip)
            normed[here, :] = layer_norm(pre[here, :], gains[0:1, :]).astype(BF16)

    def piece_rows(index):
        return pl.ds(index * half_rows, half_rows)

    ROUTES = ((0, 0, 2), (1, 1, 3), (0, 1, 4), (1, 0, 5), (0, 2, 6), (1, 3, 7))

    def norm_copy(route):
        way, src, dst = ROUTES[route]
        return remote(
            normed.at[piece_rows(src)],
            normed.at[piece_rows(dst)],
            norm_send.at[0],
            norm_recv.at[route // 2],
            sides[way],
        )

    def norm_arrive(stage):
        wait_bytes(normed.at[pl.ds(0, 2 * half_rows)], norm_recv.at[stage])

    def gate_up(top, bottom, lo, hi, lanes):
        deep = slice(lo * wide, hi * wide)
        gate = jnp.dot(normed[top:bottom, deep], gate_w[deep, lanes], preferred_element_type=F32)
        up = jnp.dot(normed[top:bottom, deep], up_w[deep, lanes], preferred_element_type=F32)
        if lo > 0:
            gate += gate_acc[top:bottom, lanes]
            up += up_acc[top:bottom, lanes]
        if hi < CHIPS:
            gate_acc[top:bottom, lanes] = gate
            up_acc[top:bottom, lanes] = up
        else:
            hidden[top:bottom, lanes] = (gate / (1.0 + jnp.exp(-gate)) * up).astype(BF16)

    def gate_up_range(top, bottom, lo, hi):
        for start in range(0, units, 256):
            gate_up(top, bottom, lo, hi, slice(start, min(start + 256, units)))

    LEFT, RIGHT, OWN, FAR = range(4)
    def down_rows(k, top, bottom, pieces):
        a, b = CHUNKS[k]
        if b == a + 1:
            weights = down_w[a * wide : (b + 1) * wide, :]
        else:
            weights = jnp.concatenate([down_w[s * wide : (s + 1) * wide, :] for s in (a, b)], 0)
        part = lax.dot_general(
            hidden[top:bottom, :], weights, (((1,), (1,)), ((), ())), preferred_element_type=F32
        ).astype(BF16)
        for source, to in enumerate(pieces):
            for side, lanes in ((0, slice(0, wide)), (1, slice(wide, 2 * wide))):
                parts[to // 2, k, side, to % 2 * half_rows : (to % 2 + 1) * half_rows, :] = part[
                    source * half_rows : (source + 1) * half_rows, lanes
                ]

    def down_far(k):
        wait_bytes(down_w.at[pl.ds(0, wide)], down_recv.at[k])
        down_rows(k, 3 * token_rows, 4 * token_rows, (6, 7))
        for way in range(2):
            launch(
                remote(
                    parts.at[FAR, k, way], relays.at[k, way], sum_send.at[0], relay_recv.at[k], sides[way]
                )
            )

    def down_rest(k):
        down_rows(k, 0, 3 * token_rows, (4, 5, 0, 3, 1, 2))

    def plain_chunk(k):
        for way, to, side in ((0, RIGHT, 1), (1, LEFT, 0)):
            launch(
                remote(
                    parts.at[to, k, side], arrived.at[k, to, side], sum_send.at[0], sum_recv.at[k], sides[way]
                )
            )

    def relay_chunk(k, whole):
        wait_bytes(relays.at[k], relay_recv.at[k])
        for way, to in ((0, RIGHT), (1, LEFT)):
            parts[to, k, way] = (parts[to, k, way].astype(F32) + relays[k, way].astype(F32)).astype(BF16)
            piece = (to, k) if whole else (to, k, way)
            into = (k, to) if whole else (k, to, way)
            launch(remote(parts.at[piece], arrived.at[into], sum_send.at[0], sum_recv.at[k], sides[way]))

    first_core = lax.broadcasted_iota(jnp.int32, (token_rows, wide), 1) < depth

    def prepare_sum():
        pre[...] = ALPHA * normed[0:token_rows, :].astype(F32)

    def finish_chunk(k):
        wait_bytes(arrived.at[k], sum_recv.at[k])
        for side, slot in enumerate(CHUNKS[k]):
            down = (
                parts[OWN, k, side].astype(F32)
                + arrived[k, LEFT, side].astype(F32)
                + arrived[k, RIGHT, side].astype(F32)
            )
            swapped = SLOT[OFFSETS[slot][::-1]]
            if swapped == slot:
                pre[:, slot_lanes(slot)] += down
            else:
                pre[:, slot_lanes(slot)] += jnp.where(first_core, down, 0.0)
                pre[:, slot_lanes(swapped)] += jnp.where(first_core, 0.0, down)

    def final_norm():
        for t in range(token_rows // strip):
            here = pl.ds(t * strip, strip)
            result = layer_norm(pre[here, :], gains[1:2, :]).astype(BF16)
            for slot in range(CHIPS):
                out_ref[here, chip_lanes(slot)] = result[:, slot_lanes(slot)]

    def sends_wait():
        def gone(ref, sem):
            remote(ref, ref, sem, sem, partner).wait_send()

        for i, ref in enumerate(halo_refs()):
            gone(ref, halo_send.at[i])
        gone(weights.at[:, pl.ds(0, (CHIPS - 1) * depth)], ring_send.at[0])
        gone(weights.at[:, pl.ds(0, CHIPS * depth)], pair_send.at[0])
        gone(tokens.at[pl.ds(0, TP - 1)], tok_send.at[0])
        gone(normed.at[pl.ds(0, 6 * half_rows)], norm_send.at[0])
        gone(parts.at[pl.ds(0, 3)], sum_send.at[0])

    loaded(normed.at[pl.ds(0, rows // 4)], 0)
    loaded(doc_all.at[:, pl.ds(HALF, rows)], 1)
    attend(1)
    pl.semaphore_wait(barrier, len(greeted))
    launch_halos()
    loaded(gate_w.at[pl.ds(0, 3 * depth)], 2)
    begin(1, (0, 1))
    begin(2, (0, 1))
    for kind in range(3):
        launch(pair(kind, (0, 0), None))
    load(w_out_hbm, w_out, 3)
    load(res_hbm, res_all, 4)
    for i, src in enumerate((gain_one_hbm, gain_two_hbm)):
        load(src, gains_in.at[pl.ds(i, 1)], 5)
    attend(2)
    halo_wait()
    attend(0)
    attend(3)
    send_tokens()
    weights_tick(1)
    loaded(w_out, 3)
    loaded(res_all, 4)
    loaded(gains_in, 5)
    order_gains()
    wait_bytes(tokens.at[pl.ds(0, 2)], tok_recv.at[0])
    project((0, 1, 2))
    wait_bytes(tokens.at[3], tok_recv.at[1])
    project((3,))
    norm_rows(0, half_rows)
    launch(norm_copy(0))
    norm_rows(half_rows, token_rows)
    for route in (1, 2, 3):
        launch(norm_copy(route))
    weights_tick(2)
    weights_tick(3)
    prepare_sum()
    weights_tick(4)
    norm_arrive(0)
    for route in (4, 5):
        launch(norm_copy(route))
    weights_tick(5)
    segment_wait(0)
    gate_up_range(0, 256, 0, 4)
    weights_tick(6)
    segment_wait(1)
    gate_up_range(0, 256, 4, 10)
    weights_tick(7)
    begin(1, (2,))
    norm_arrive(1)
    gate_up_range(256, 384, 0, 10)
    weights_tick(8)
    weights_tick(9)
    norm_arrive(2)
    begin(2, (2,))
    gate_up_range(384, 512, 0, 10)
    segment_wait(2)
    gate_up_range(0, 128, 10, 14)
    weights_tick(10)
    gate_up_range(128, 512, 10, 14)
    down_tick(1)
    segment_wait(3)
    gate_up_range(0, 256, 14, 16)
    down_tick(2)
    gate_up_range(256, 512, 14, 16)
    down_far(0)
    down_far(1)
    down_rest(0)
    plain_chunk(0)
    down_tick(3)
    down_rest(1)
    plain_chunk(1)
    down_tick(4)
    relay_chunk(0, False)
    down_far(2)
    relay_chunk(1, False)
    down_rest(2)
    plain_chunk(2)
    down_tick(5)
    down_far(3)
    down_rest(3)
    plain_chunk(3)
    down_tick(7)
    down_far(4)
    relay_chunk(2, False)
    down_tick(6)
    down_rest(4)
    plain_chunk(4)
    down_tick(8)
    down_far(5)
    relay_chunk(3, False)
    down_tick(9)
    down_rest(5)
    plain_chunk(5)
    down_tick(10)
    down_far(6)
    relay_chunk(4, False)
    down_far(7)
    down_rest(6)
    plain_chunk(6)
    relay_chunk(5, False)
    down_rest(7)
    plain_chunk(7)
    relay_chunk(6, False)
    finish_chunk(0)
    finish_chunk(1)
    finish_chunk(2)
    relay_chunk(7, False)
    finish_chunk(3)
    finish_chunk(4)
    finish_chunk(5)
    finish_chunk(6)
    finish_chunk(7)
    final_norm()
    sends_wait()


def solution(mesh):
    def per_device(
        queries,
        keys,
        values,
        doc_ids,
        sink_logit,
        residual_in,
        w_out,
        gain_one,
        w_gate,
        w_up,
        w_down,
        gain_two,
    ):
        rows = queries.shape[0]
        token_rows, width = residual_in.shape
        units = w_gate.shape[1]
        span = rows + 2 * HALF
        dma = pltpu.SemaphoreType.DMA
        vmem, anywhere = (pl.BlockSpec(memory_space=pltpu.VMEM), pl.BlockSpec(memory_space=pl.ANY))
        return pl.pallas_call(
            kernel,
            out_shape=pltpu.VMEM((token_rows, width), BF16),
            in_specs=[pl.BlockSpec(memory_space=pltpu.SMEM)] + [anywhere] * 11,
            out_specs=vmem,
            scratch_shapes=[
                pltpu.VMEM(queries.shape, BF16),
                pltpu.VMEM((span, keys.shape[1]), BF16),
                pltpu.VMEM((span, keys.shape[1]), BF16),
                pltpu.VMEM((1, span), jnp.int32),
                pltpu.VMEM((2, width), F32),
                pltpu.VMEM((2, width), F32),
                pltpu.VMEM((token_rows, width), BF16),
                pltpu.VMEM(w_out.shape, BF16),
                pltpu.VMEM((3, width, units), BF16),
                pltpu.VMEM(queries.shape, BF16),
                pltpu.VMEM((TP, token_rows, queries.shape[1]), BF16),
                pltpu.VMEM((token_rows, width), F32),
                pltpu.VMEM((rows, width), BF16),
                pltpu.VMEM((rows, units), F32),
                pltpu.VMEM((rows, units), F32),
                pltpu.VMEM((rows, units), BF16),
                pltpu.VMEM((4, len(CHUNKS), 2, token_rows, width // CHIPS), BF16),
                pltpu.VMEM((len(CHUNKS), 2, token_rows, width // CHIPS), BF16),
                pltpu.VMEM((len(CHUNKS), 2, 2, token_rows, width // CHIPS), BF16),
                dma((6,)),
                dma((2,)),
                dma((2,)),
                dma((1,)),
                dma((2, LAST)),
                dma((1,)),
                dma((len(SEGMENTS),)),
                dma((len(CHUNKS),)),
                dma((1,)),
                dma((2,)),
                dma((1,)),
                dma((3,)),
                dma((1,)),
                dma((len(CHUNKS),)),
                dma((len(CHUNKS),)),
            ],
            compiler_params=pltpu.CompilerParams(
                collective_id=0, has_side_effects=True, vmem_limit_bytes=62 * 2**20
            ),
        )(
            sink_logit,
            queries,
            residual_in,
            gain_one[None, :],
            gain_two[None, :],
            keys,
            values,
            doc_ids[None, :],
            w_out,
            w_gate,
            w_up,
            w_down.T,
        )

    in_specs = (
        P("sp", "tp"),
        P("sp", "tp"),
        P("sp", "tp"),
        P("sp"),
        P("tp"),
        P(("sp", "tp"), None),
        P(),
        P(),
        P("sp", "tp"),
        P("sp", "tp"),
        P("tp", "sp"),
        P(),
    )
    return jax.shard_map(
        per_device, mesh=mesh, in_specs=in_specs, out_specs=P(("sp", "tp"), None), check_vma=False
    )
```

```python
import jax
import jax.numpy as jnp
from jax import lax
from jax.experimental import pallas as pl
from jax.experimental.pallas import tpu as pltpu
from jax.sharding import PartitionSpec as P

HEAD = 128
HALF = 128
CORES = 2
SIDE = 4
CHIPS = SIDE * SIDE
TP = 4
ALPHA = 2.0**0.5
EPS = 1e-05
NEGATIVE = -1e30
MESH = pl.DeviceIdType.MESH
BF16 = jnp.bfloat16
F32 = jnp.float32
OFFSETS = (
    (0, 0),
    (1, 0),
    (0, 1),
    (-1, 0),
    (0, -1),
    (1, 1),
    (-1, -1),
    (1, -1),
    (-1, 1),
    (2, 0),
    (0, 2),
    (2, 1),
    (1, 2),
    (2, -1),
    (-1, 2),
    (2, 2),
)
SLOT = {offset: slot for slot, offset in enumerate(OFFSETS)}
SEGMENTS = ((0, 4), (4, 10), (10, 14), (14, 16))
CHUNKS = ((1, 3), (2, 4), (0, 9), (5, 6), (7, 8), (11, 13), (12, 14), (10, 15))
LAST = 10


def message(number, way):
    s = 2 * way - 1
    return (
        None,
        (0, (0, 0), (s, 0), False),
        (1, (0, 0), (0, s), False),
        (0, (s, 0), (2, 0), True),
        (1, (s, 0), (s, s), False),
        (1, (-s, 0), (-s, s), False),
        (1, (0, s), (0, 2), True),
        (1, (2, 0), (2, s), False),
        (1, (s, s), (s, 2), True),
        (1, (-s, s), (-s, 2), True),
        (1, (2, s), (2, 2), True),
    )[number]


FOLLOW = {1: (3, 4, 5), 2: (6,), 3: (7,), 4: (8,), 5: (9,), 7: (10,)}
DOWN_FOLLOW = {1: (3, 4, 5), 3: (7, 6), 4: (8,), 5: (9,), 7: (10,)}


def segment_of(slot):
    return [lo <= slot < hi for lo, hi in SEGMENTS].index(True)


def chunk_of(slot):
    return [slot in chunk for chunk in CHUNKS].index(True)


def layer_norm(values_in, gain):
    average = jnp.mean(values_in, -1, keepdims=True)
    centred = values_in - average
    variance = jnp.mean(centred * centred, -1, keepdims=True)
    return centred * lax.rsqrt(variance + EPS) * gain


def kernel(
    sink_ref,
    q_hbm,
    res_hbm,
    gain_one_hbm,
    gain_two_hbm,
    k_hbm,
    v_hbm,
    doc_hbm,
    w_out_hbm,
    wg_hbm,
    wu_hbm,
    wd_hbm,
    out_ref,
    q_all,
    k_all,
    v_all,
    doc_all,
    gains_in,
    gains,
    res_all,
    w_out,
    weights,
    att,
    tokens,
    pre,
    normed,
    gate_acc,
    up_acc,
    hidden,
    parts,
    relays,
    arrived,
    local_sem,
    halo_send,
    halo_recv,
    ring_send,
    ring_recv,
    pair_send,
    pair_recv,
    down_recv,
    tok_send,
    tok_recv,
    norm_send,
    norm_recv,
    sum_send,
    relay_recv,
    sum_recv,
):
    gate_w, up_w, down_w = (weights.at[i] for i in range(3))
    sp = lax.axis_index("sp")
    tp = lax.axis_index("tp")
    sp_size = CHIPS * CORES
    core = lax.rem(sp, CORES)
    chip = sp // CORES
    my_y = lax.rem(chip, SIDE)
    my_z = chip // SIDE

    def chip_at(dz, dy):
        z = lax.rem(my_z + (dz + SIDE), SIDE)
        y = lax.rem(my_y + (dy + SIDE), SIDE)
        return z * SIDE + y

    rows = q_hbm.shape[0]
    token_rows = res_hbm.shape[0]
    depth = wg_hbm.shape[0]
    units = wg_hbm.shape[1]
    width = res_hbm.shape[1]
    sub_rows = depth // 2
    wide = CORES * depth
    half_rows = token_rows // 2

    def chip_lanes(slot):
        return pl.ds(pl.multiple_of(chip_at(*OFFSETS[slot]) * wide, wide), wide)

    def slot_lanes(slot):
        return slice(slot * wide, (slot + 1) * wide)

    along_z = [chip_at(1, 0) * CORES + core, chip_at(-1, 0) * CORES + core]
    along_y = [chip_at(0, 1) * CORES + core, chip_at(0, -1) * CORES + core]
    first_axis = [along_z[way] * (1 - core) + along_y[way] * core for way in range(2)]
    second_axis = [along_y[way] * (1 - core) + along_z[way] * core for way in range(2)]
    axes = ((along_z, along_y), (along_y, along_z), (first_axis, second_axis))
    partner = (chip * CORES + (1 - core), tp)
    after = (lax.rem(sp + 1, sp_size), tp)
    before = (lax.rem(sp + sp_size - 1, sp_size), tp)
    tp_right = lax.rem(tp + 1, TP)
    tp_left = lax.rem(tp + TP - 1, TP)
    tp_far = lax.rem(tp + 2, TP)
    sides = [(sp, tp_right), (sp, tp_left)]
    far = (sp, tp_far)

    barrier = pltpu.get_barrier_semaphore()
    greeted = [(axis[way], tp) for axis in (along_z, along_y) for way in range(2)]
    greeted += [partner, after, before, far] + sides
    for device in greeted:
        pl.semaphore_signal(barrier, inc=1, device_id=device, device_id_type=MESH)

    own_rows = pl.ds(pl.multiple_of(core * depth, depth), depth)
    def load(src, dst, sem):
        pltpu.make_async_copy(src, dst, local_sem.at[sem]).start()

    def loaded(ref, sem):
        pltpu.make_async_copy(ref, ref, local_sem.at[sem]).wait()

    load(k_hbm, k_all.at[pl.ds(HALF, rows)], 0)
    load(v_hbm, v_all.at[pl.ds(HALF, rows)], 0)
    load(q_hbm, q_all, 0)
    load(doc_hbm, doc_all.at[:, pl.ds(HALF, rows)], 1)
    for i, src in enumerate((wg_hbm, wu_hbm, wd_hbm)):
        load(src, weights.at[i, own_rows], 2)

    def remote(src, dst, send, recv, device):
        return pltpu.make_async_remote_copy(
            src_ref=src, dst_ref=dst, send_sem=send, recv_sem=recv, device_id=device, device_id_type=MESH
        )

    def launch(copy):
        copy.start()

    def arrive(copy):
        copy.wait_recv()

    def wait_bytes(ref, sem):
        remote(ref, ref, sem, sem, partner).wait_recv()

    low, high = (pl.ds(HALF, HALF), pl.ds(rows, HALF))
    into_low, into_high = (pl.ds(0, HALF), pl.ds(HALF + rows, HALF))

    def launch_halos():
        for i, ref in enumerate((k_all, v_all)):
            launch(remote(ref.at[high], ref.at[into_low], halo_send.at[0], halo_recv.at[0], after))
            launch(remote(ref.at[low], ref.at[into_high], halo_send.at[0], halo_recv.at[0], before))
        for src, dst, to in ((high, into_low, after), (low, into_high, before)):
            launch(
                remote(doc_all.at[:, src], doc_all.at[:, dst], halo_send.at[1], halo_recv.at[1], to)
            )

    def halo_refs():
        return (k_all.at[pl.ds(0, 4 * HALF)], doc_all.at[:, pl.ds(0, 2 * HALF)])

    def halo_wait():
        for i, ref in enumerate(halo_refs()):
            wait_bytes(ref, halo_recv.at[i])

    buffers = (gate_w, up_w, down_w)

    def slot_for(kind, offset):
        straight, swapped = SLOT[offset], SLOT[offset[::-1]]
        return swapped if kind == 1 else straight

    def place(kind, offset, half, core_id):
        start = slot_for(kind, offset) * wide + core_id * depth
        if half is None:
            return buffers[kind].at[pl.ds(pl.multiple_of(start, depth), depth)]
        return buffers[kind].at[pl.ds(pl.multiple_of(start + half * sub_rows, sub_rows), sub_rows)]

    def ring(kind, number, way):
        axis, src_offset, dst_offset, halved = message(number, way)
        half = way if halved else None
        dst = place(kind, dst_offset, half, core)
        src = place(kind, src_offset, half, core)
        to = (axes[kind][axis][way], tp)
        return remote(src, dst, ring_send.at[0], ring_recv.at[kind // 2, number - 1], to)

    def pair(kind, offset, half):
        dst = place(kind, offset, half, core)
        slot = slot_for(kind, offset)
        if kind == 2:
            sem = down_recv.at[chunk_of(slot)]
        else:
            sem = pair_recv.at[segment_of(slot)]
        return remote(dst, dst, pair_send.at[0], sem, partner)

    def begin(number, kinds):
        for kind in kinds:
            for way in range(2):
                launch(ring(kind, number, way))

    def tick(number, kinds):
        halved = message(number, 0)[3]
        total = 2 * len(kinds) * (sub_rows if halved else depth)
        wait_bytes(buffers[kinds[0]].at[pl.ds(0, total)], ring_recv.at[kinds[0] // 2, number - 1])
        for follower in (DOWN_FOLLOW if kinds[0] == 2 else FOLLOW).get(number, ()):
            for kind in kinds:
                for way in range(2):
                    launch(ring(kind, follower, way))
        for kind in kinds:
            for way in range(2):
                _, _, offset, halved = message(number, way)
                launch(pair(kind, offset, way if halved else None))

    weights_tick = lambda number: tick(number, (0, 1))
    down_tick = lambda number: tick(number, (2,))

    def segment_wait(segment):
        lo, hi = SEGMENTS[segment]
        wait_bytes(gate_w.at[pl.ds(0, 2 * (hi - lo) * depth)], pair_recv.at[segment])

    span = rows + 2 * HALF
    at = lax.broadcasted_iota(jnp.int32, (1, span), 1) + (sp * rows - HALF)
    inside = jnp.logical_and(at >= 0, at < sp_size * rows)
    reach = 3 * HALF
    repeat = q_hbm.shape[1] // HEAD
    offset_of = lax.broadcasted_iota(jnp.int32, (HALF, reach), 1) - lax.broadcasted_iota(
        jnp.int32, (HALF, reach), 0
    )
    near = jnp.logical_and(offset_of >= 0, offset_of <= 2 * HALF)

    def attend(block):
        here = slice(block * HALF, (block + 1) * HALF)
        there = slice(block * HALF, block * HALF + reach)
        doc_row = doc_all[:, (block + 1) * HALF : (block + 2) * HALF]
        doc_query = jnp.broadcast_to(doc_row, (HALF, HALF)).T
        doc_keys = jnp.where(inside[:, there], doc_all[:, there], -1)
        same = jnp.concatenate([doc_query] * 3, 1) == doc_keys
        allowed = jnp.logical_and(near, same)
        key_blk = k_all[there, :]
        value_blk = v_all[there, :]
        for h in range(repeat):
            lanes = slice(h * HEAD, (h + 1) * HEAD)
            scores = lax.dot_general(
                q_all[here, lanes], key_blk, (((1,), (1,)), ((), ())), preferred_element_type=F32
            ) * HEAD ** (-0.5)
            scores = jnp.where(allowed, scores, NEGATIVE)
            sink = jnp.full((1, 1), sink_ref[h], F32)
            top = jnp.maximum(jnp.max(scores, -1, keepdims=True), sink)
            weights = jnp.exp(scores - top)
            total = jnp.sum(weights, -1, keepdims=True) + jnp.exp(sink - top)
            summed = jnp.dot(weights.astype(BF16), value_blk, preferred_element_type=F32)
            att[here, lanes] = (summed / total).astype(BF16)

    def token_rows_of(j):
        return pl.ds(pl.multiple_of(j * token_rows, token_rows), token_rows)

    def send_tokens():
        for j, into in ((tp_far, 3), (tp_right, 1), (tp_left, 2)):
            launch(
                remote(
                    att.at[token_rows_of(j)], tokens.at[into], tok_send.at[0], tok_recv.at[into // 3], (sp, j)
                )
            )
        tokens[0] = att[token_rows_of(tp), :]

    def order_gains():
        for slot in range(CHIPS):
            gains[:, slot_lanes(slot)] = gains_in[:, chip_lanes(slot)]

    def project(held):
        for first, second in zip(range(0, CHIPS, 2), range(1, CHIPS, 2)):
            picks = (chip_lanes(first), chip_lanes(second))
            lanes = slice(first * wide, (second + 1) * wide)
            if held[0] == 0:
                mixed = ALPHA * jnp.concatenate([res_all[:, pick] for pick in picks], 1).astype(F32)
            else:
                mixed = pre[:, lanes]
            for j in held:
                cols = q_hbm.shape[1]
                deep = pl.ds(pl.multiple_of((tp, tp_left, tp_right, tp_far)[j] * cols, cols), cols)
                mixed += jnp.dot(
                    tokens[j],
                    jnp.concatenate([w_out[deep, pick] for pick in picks], 1),
                    preferred_element_type=F32,
                )
            pre[:, lanes] = mixed

    strip = 64

    def norm_rows(first, last):
        @pl.loop(first // strip, last // strip)
        def _(t):
            here = pl.ds(pl.multiple_of(t * strip, strip), strip)
            normed[here, :] = layer_norm(pre[here, :], gains[0:1, :]).astype(BF16)

    def piece_rows(index):
        return pl.ds(index * half_rows, half_rows)

    ROUTES = ((0, 0, 2), (1, 1, 3), (0, 1, 4), (1, 0, 5), (0, 2, 6), (1, 3, 7))

    def norm_copy(route):
        way, src, dst = ROUTES[route]
        return remote(
            normed.at[piece_rows(src)],
            normed.at[piece_rows(dst)],
            norm_send.at[0],
            norm_recv.at[route // 2],
            sides[way],
        )

    def norm_arrive(stage):
        wait_bytes(normed.at[pl.ds(0, 2 * half_rows)], norm_recv.at[stage])

    def gate_up(top, bottom, lo, hi, lanes):
        deep = slice(lo * wide, hi * wide)
        gate = jnp.dot(normed[top:bottom, deep], gate_w[deep, lanes], preferred_element_type=F32)
        up = jnp.dot(normed[top:bottom, deep], up_w[deep, lanes], preferred_element_type=F32)
        if lo > 0:
            gate += gate_acc[top:bottom, lanes]
            up += up_acc[top:bottom, lanes]
        if hi < CHIPS:
            gate_acc[top:bottom, lanes] = gate
            up_acc[top:bottom, lanes] = up
        else:
            hidden[top:bottom, lanes] = (gate / (1.0 + jnp.exp(-gate)) * up).astype(BF16)

    def gate_up_range(top, bottom, lo, hi):
        for start in range(0, units, 256):
            gate_up(top, bottom, lo, hi, slice(start, min(start + 256, units)))

    LEFT, RIGHT, OWN, FAR = range(4)
    def down_rows(k, top, bottom, pieces):
        a, b = CHUNKS[k]
        if b == a + 1:
            weights = down_w[a * wide : (b + 1) * wide, :]
        else:
            weights = jnp.concatenate([down_w[s * wide : (s + 1) * wide, :] for s in (a, b)], 0)
        part = lax.dot_general(
            hidden[top:bottom, :], weights, (((1,), (1,)), ((), ())), preferred_element_type=F32
        ).astype(BF16)
        for source, to in enumerate(pieces):
            for side, lanes in ((0, slice(0, wide)), (1, slice(wide, 2 * wide))):
                parts[to // 2, k, side, to % 2 * half_rows : (to % 2 + 1) * half_rows, :] = part[
                    source * half_rows : (source + 1) * half_rows, lanes
                ]

    def down_far(k):
        wait_bytes(down_w.at[pl.ds(0, wide)], down_recv.at[k])
        down_rows(k, 3 * token_rows, 4 * token_rows, (6, 7))
        for way in range(2):
            launch(
                remote(
                    parts.at[FAR, k, way], relays.at[k, way], sum_send.at[0], relay_recv.at[k], sides[way]
                )
            )

    def down_rest(k):
        down_rows(k, 0, 3 * token_rows, (4, 5, 0, 3, 1, 2))

    def plain_chunk(k):
        for way, to, side in ((0, RIGHT, 1), (1, LEFT, 0)):
            launch(
                remote(
                    parts.at[to, k, side], arrived.at[k, to, side], sum_send.at[0], sum_recv.at[k], sides[way]
                )
            )

    def relay_chunk(k, whole):
        wait_bytes(relays.at[k], relay_recv.at[k])
        for way, to in ((0, RIGHT), (1, LEFT)):
            parts[to, k, way] = (parts[to, k, way].astype(F32) + relays[k, way].astype(F32)).astype(BF16)
            piece = (to, k) if whole else (to, k, way)
            into = (k, to) if whole else (k, to, way)
            launch(remote(parts.at[piece], arrived.at[into], sum_send.at[0], sum_recv.at[k], sides[way]))

    first_core = lax.broadcasted_iota(jnp.int32, (token_rows, wide), 1) < depth

    def prepare_sum():
        pre[...] = ALPHA * normed[0:token_rows, :].astype(F32)

    def finish_chunk(k):
        wait_bytes(arrived.at[k], sum_recv.at[k])
        for side, slot in enumerate(CHUNKS[k]):
            down = (
                parts[OWN, k, side].astype(F32)
                + arrived[k, LEFT, side].astype(F32)
                + arrived[k, RIGHT, side].astype(F32)
            )
            swapped = SLOT[OFFSETS[slot][::-1]]
            if swapped == slot:
                pre[:, slot_lanes(slot)] += down
            else:
                pre[:, slot_lanes(slot)] += jnp.where(first_core, down, 0.0)
                pre[:, slot_lanes(swapped)] += jnp.where(first_core, 0.0, down)

    def final_norm():
        for t in range(token_rows // strip):
            here = pl.ds(t * strip, strip)
            result = layer_norm(pre[here, :], gains[1:2, :]).astype(BF16)
            for slot in range(CHIPS):
                out_ref[here, chip_lanes(slot)] = result[:, slot_lanes(slot)]

    def sends_wait():
        def gone(ref, sem):
            remote(ref, ref, sem, sem, partner).wait_send()

        for i, ref in enumerate(halo_refs()):
            gone(ref, halo_send.at[i])
        gone(weights.at[:, pl.ds(0, (CHIPS - 1) * depth)], ring_send.at[0])
        gone(weights.at[:, pl.ds(0, CHIPS * depth)], pair_send.at[0])
        gone(tokens.at[pl.ds(0, TP - 1)], tok_send.at[0])
        gone(normed.at[pl.ds(0, 6 * half_rows)], norm_send.at[0])
        gone(parts.at[pl.ds(0, 3)], sum_send.at[0])

    loaded(normed.at[pl.ds(0, rows // 4)], 0)
    loaded(doc_all.at[:, pl.ds(HALF, rows)], 1)
    attend(1)
    pl.semaphore_wait(barrier, len(greeted))
    launch_halos()
    loaded(gate_w.at[pl.ds(0, 3 * depth)], 2)
    begin(1, (0, 1))
    begin(2, (0, 1))
    for kind in range(3):
        launch(pair(kind, (0, 0), None))
    load(w_out_hbm, w_out, 3)
    load(res_hbm, res_all, 4)
    for i, src in enumerate((gain_one_hbm, gain_two_hbm)):
        load(src, gains_in.at[pl.ds(i, 1)], 5)
    attend(2)
    halo_wait()
    attend(0)
    attend(3)
    send_tokens()
    weights_tick(1)
    loaded(w_out, 3)
    loaded(res_all, 4)
    loaded(gains_in, 5)
    order_gains()
    wait_bytes(tokens.at[pl.ds(0, 2)], tok_recv.at[0])
    project((0, 1, 2))
    wait_bytes(tokens.at[3], tok_recv.at[1])
    project((3,))
    norm_rows(0, half_rows)
    launch(norm_copy(0))
    norm_rows(half_rows, token_rows)
    for route in (1, 2, 3):
        launch(norm_copy(route))
    weights_tick(2)
    weights_tick(3)
    prepare_sum()
    weights_tick(4)
    norm_arrive(0)
    for route in (4, 5):
        launch(norm_copy(route))
    weights_tick(5)
    segment_wait(0)
    gate_up_range(0, 256, 0, 4)
    weights_tick(6)
    segment_wait(1)
    gate_up_range(0, 256, 4, 10)
    weights_tick(7)
    begin(1, (2,))
    norm_arrive(1)
    gate_up_range(256, 384, 0, 10)
    weights_tick(8)
    weights_tick(9)
    norm_arrive(2)
    begin(2, (2,))
    gate_up_range(384, 512, 0, 10)
    segment_wait(2)
    gate_up_range(0, 128, 10, 14)
    weights_tick(10)
    gate_up_range(128, 512, 10, 14)
    down_tick(1)
    segment_wait(3)
    gate_up_range(0, 512, 14, 16)
    down_far(0)
    down_tick(2)
    down_rest(0)
    plain_chunk(0)
    down_far(1)
    down_rest(1)
    plain_chunk(1)
    down_tick(3)
    relay_chunk(0, False)
    down_tick(4)
    down_far(2)
    relay_chunk(1, False)
    down_rest(2)
    plain_chunk(2)
    down_tick(5)
    down_far(3)
    down_rest(3)
    plain_chunk(3)
    down_tick(7)
    down_far(4)
    relay_chunk(2, False)
    down_tick(6)
    down_rest(4)
    plain_chunk(4)
    down_tick(8)
    down_far(5)
    relay_chunk(3, False)
    down_tick(9)
    down_rest(5)
    plain_chunk(5)
    down_tick(10)
    down_far(6)
    relay_chunk(4, False)
    down_far(7)
    down_rest(6)
    plain_chunk(6)
    relay_chunk(5, False)
    down_rest(7)
    plain_chunk(7)
    relay_chunk(6, False)
    finish_chunk(0)
    finish_chunk(1)
    finish_chunk(2)
    relay_chunk(7, False)
    finish_chunk(3)
    finish_chunk(4)
    finish_chunk(5)
    finish_chunk(6)
    finish_chunk(7)
    final_norm()
    sends_wait()


def solution(mesh):
    def per_device(
        queries,
        keys,
        values,
        doc_ids,
        sink_logit,
        residual_in,
        w_out,
        gain_one,
        w_gate,
        w_up,
        w_down,
        gain_two,
    ):
        rows = queries.shape[0]
        token_rows, width = residual_in.shape
        units = w_gate.shape[1]
        span = rows + 2 * HALF
        dma = pltpu.SemaphoreType.DMA
        vmem, anywhere = (pl.BlockSpec(memory_space=pltpu.VMEM), pl.BlockSpec(memory_space=pl.ANY))
        return pl.pallas_call(
            kernel,
            out_shape=pltpu.VMEM((token_rows, width), BF16),
            in_specs=[pl.BlockSpec(memory_space=pltpu.SMEM)] + [anywhere] * 11,
            out_specs=vmem,
            scratch_shapes=[
                pltpu.VMEM(queries.shape, BF16),
                pltpu.VMEM((span, keys.shape[1]), BF16),
                pltpu.VMEM((span, keys.shape[1]), BF16),
                pltpu.VMEM((1, span), jnp.int32),
                pltpu.VMEM((2, width), F32),
                pltpu.VMEM((2, width), F32),
                pltpu.VMEM((token_rows, width), BF16),
                pltpu.VMEM(w_out.shape, BF16),
                pltpu.VMEM((3, width, units), BF16),
                pltpu.VMEM(queries.shape, BF16),
                pltpu.VMEM((TP, token_rows, queries.shape[1]), BF16),
                pltpu.VMEM((token_rows, width), F32),
                pltpu.VMEM((rows, width), BF16),
                pltpu.VMEM((rows, units), F32),
                pltpu.VMEM((rows, units), F32),
                pltpu.VMEM((rows, units), BF16),
                pltpu.VMEM((4, len(CHUNKS), 2, token_rows, width // CHIPS), BF16),
                pltpu.VMEM((len(CHUNKS), 2, token_rows, width // CHIPS), BF16),
                pltpu.VMEM((len(CHUNKS), 2, 2, token_rows, width // CHIPS), BF16),
                dma((6,)),
                dma((2,)),
                dma((2,)),
                dma((1,)),
                dma((2, LAST)),
                dma((1,)),
                dma((len(SEGMENTS),)),
                dma((len(CHUNKS),)),
                dma((1,)),
                dma((2,)),
                dma((1,)),
                dma((3,)),
                dma((1,)),
                dma((len(CHUNKS),)),
                dma((len(CHUNKS),)),
            ],
            compiler_params=pltpu.CompilerParams(
                collective_id=0, has_side_effects=True, vmem_limit_bytes=62 * 2**20
            ),
        )(
            sink_logit,
            queries,
            residual_in,
            gain_one[None, :],
            gain_two[None, :],
            keys,
            values,
            doc_ids[None, :],
            w_out,
            w_gate,
            w_up,
            w_down.T,
        )

    in_specs = (
        P("sp", "tp"),
        P("sp", "tp"),
        P("sp", "tp"),
        P("sp"),
        P("tp"),
        P(("sp", "tp"), None),
        P(),
        P(),
        P("sp", "tp"),
        P("sp", "tp"),
        P("tp", "sp"),
        P(),
    )
    return jax.shard_map(
        per_device, mesh=mesh, in_specs=in_specs, out_specs=P(("sp", "tp"), None), check_vma=False
    )
```

```python
import jax
import jax.numpy as jnp
from jax import lax
from jax.experimental import pallas as pl
from jax.experimental.pallas import tpu as pltpu
from jax.sharding import PartitionSpec as P

HEAD = 128
HALF = 128
CORES = 2
SIDE = 4
CHIPS = SIDE * SIDE
TP = 4
ALPHA = 2.0**0.5
EPS = 1e-05
NEGATIVE = -1e30
MESH = pl.DeviceIdType.MESH
BF16 = jnp.bfloat16
F32 = jnp.float32
OFFSETS = (
    (0, 0),
    (1, 0),
    (0, 1),
    (-1, 0),
    (0, -1),
    (1, 1),
    (-1, -1),
    (1, -1),
    (-1, 1),
    (2, 0),
    (0, 2),
    (2, 1),
    (1, 2),
    (2, -1),
    (-1, 2),
    (2, 2),
)
SLOT = {offset: slot for slot, offset in enumerate(OFFSETS)}
SEGMENTS = ((0, 4), (4, 10), (10, 14), (14, 16))
CHUNKS = ((1, 3), (2, 4), (0, 9), (5, 6), (7, 8), (11, 13), (12, 14), (10, 15))
LAST = 10


def message(number, way):
    s = 2 * way - 1
    return (
        None,
        (0, (0, 0), (s, 0), False),
        (1, (0, 0), (0, s), False),
        (0, (s, 0), (2, 0), True),
        (1, (s, 0), (s, s), False),
        (1, (-s, 0), (-s, s), False),
        (1, (0, s), (0, 2), True),
        (1, (2, 0), (2, s), False),
        (1, (s, s), (s, 2), True),
        (1, (-s, s), (-s, 2), True),
        (1, (2, s), (2, 2), True),
    )[number]


FOLLOW = {1: (3, 4, 5), 2: (6,), 3: (7,), 4: (8,), 5: (9,), 7: (10,)}
DOWN_FOLLOW = {1: (3, 4, 5), 3: (7, 6), 4: (8,), 5: (9,), 7: (10,)}


def segment_of(slot):
    return [lo <= slot < hi for lo, hi in SEGMENTS].index(True)


def chunk_of(slot):
    return [slot in chunk for chunk in CHUNKS].index(True)


def layer_norm(values_in, gain):
    average = jnp.mean(values_in, -1, keepdims=True)
    centred = values_in - average
    variance = jnp.mean(centred * centred, -1, keepdims=True)
    return centred * lax.rsqrt(variance + EPS) * gain


def kernel(
    sink_ref,
    q_hbm,
    res_hbm,
    gain_one_hbm,
    gain_two_hbm,
    k_hbm,
    v_hbm,
    doc_hbm,
    w_out_hbm,
    wg_hbm,
    wu_hbm,
    wd_hbm,
    out_ref,
    q_all,
    k_all,
    v_all,
    doc_all,
    gains_in,
    gains,
    res_all,
    w_out,
    weights,
    att,
    tokens,
    pre,
    normed,
    gate_acc,
    up_acc,
    hidden,
    parts,
    relays,
    arrived,
    local_sem,
    halo_send,
    halo_recv,
    ring_send,
    ring_recv,
    pair_send,
    pair_recv,
    down_recv,
    tok_send,
    tok_recv,
    norm_send,
    norm_recv,
    sum_send,
    relay_recv,
    sum_recv,
):
    gate_w, up_w, down_w = (weights.at[i] for i in range(3))
    sp = lax.axis_index("sp")
    tp = lax.axis_index("tp")
    sp_size = CHIPS * CORES
    core = lax.rem(sp, CORES)
    chip = sp // CORES
    my_y = lax.rem(chip, SIDE)
    my_z = chip // SIDE

    def chip_at(dz, dy):
        z = lax.rem(my_z + (dz + SIDE), SIDE)
        y = lax.rem(my_y + (dy + SIDE), SIDE)
        return z * SIDE + y

    rows = q_hbm.shape[0]
    token_rows = res_hbm.shape[0]
    depth = wg_hbm.shape[0]
    units = wg_hbm.shape[1]
    width = res_hbm.shape[1]
    sub_rows = depth // 2
    wide = CORES * depth
    half_rows = token_rows // 2

    def chip_lanes(slot):
        return pl.ds(pl.multiple_of(chip_at(*OFFSETS[slot]) * wide, wide), wide)

    def slot_lanes(slot):
        return slice(slot * wide, (slot + 1) * wide)

    along_z = [chip_at(1, 0) * CORES + core, chip_at(-1, 0) * CORES + core]
    along_y = [chip_at(0, 1) * CORES + core, chip_at(0, -1) * CORES + core]
    first_axis = [along_z[way] * (1 - core) + along_y[way] * core for way in range(2)]
    second_axis = [along_y[way] * (1 - core) + along_z[way] * core for way in range(2)]
    axes = ((along_z, along_y), (along_y, along_z), (first_axis, second_axis))
    partner = (chip * CORES + (1 - core), tp)
    after = (lax.rem(sp + 1, sp_size), tp)
    before = (lax.rem(sp + sp_size - 1, sp_size), tp)
    tp_right = lax.rem(tp + 1, TP)
    tp_left = lax.rem(tp + TP - 1, TP)
    tp_far = lax.rem(tp + 2, TP)
    sides = [(sp, tp_right), (sp, tp_left)]
    far = (sp, tp_far)

    barrier = pltpu.get_barrier_semaphore()
    greeted = [(axis[way], tp) for axis in (along_z, along_y) for way in range(2)]
    greeted += [partner, after, before, far] + sides
    for device in greeted:
        pl.semaphore_signal(barrier, inc=1, device_id=device, device_id_type=MESH)

    own_rows = pl.ds(pl.multiple_of(core * depth, depth), depth)
    def load(src, dst, sem):
        pltpu.make_async_copy(src, dst, local_sem.at[sem]).start()

    def loaded(ref, sem):
        pltpu.make_async_copy(ref, ref, local_sem.at[sem]).wait()

    load(k_hbm, k_all.at[pl.ds(HALF, rows)], 0)
    load(v_hbm, v_all.at[pl.ds(HALF, rows)], 0)
    load(q_hbm, q_all, 0)
    load(doc_hbm, doc_all.at[:, pl.ds(HALF, rows)], 1)
    for i, src in enumerate((wg_hbm, wu_hbm, wd_hbm)):
        load(src, weights.at[i, own_rows], 2)

    def remote(src, dst, send, recv, device):
        return pltpu.make_async_remote_copy(
            src_ref=src, dst_ref=dst, send_sem=send, recv_sem=recv, device_id=device, device_id_type=MESH
        )

    def launch(copy):
        copy.start()

    def arrive(copy):
        copy.wait_recv()

    def wait_bytes(ref, sem):
        remote(ref, ref, sem, sem, partner).wait_recv()

    low, high = (pl.ds(HALF, HALF), pl.ds(rows, HALF))
    into_low, into_high = (pl.ds(0, HALF), pl.ds(HALF + rows, HALF))

    def launch_halos():
        for i, ref in enumerate((k_all, v_all)):
            launch(remote(ref.at[high], ref.at[into_low], halo_send.at[0], halo_recv.at[0], after))
            launch(remote(ref.at[low], ref.at[into_high], halo_send.at[0], halo_recv.at[0], before))
        for src, dst, to in ((high, into_low, after), (low, into_high, before)):
            launch(
                remote(doc_all.at[:, src], doc_all.at[:, dst], halo_send.at[1], halo_recv.at[1], to)
            )

    def halo_refs():
        return (k_all.at[pl.ds(0, 4 * HALF)], doc_all.at[:, pl.ds(0, 2 * HALF)])

    def halo_wait():
        for i, ref in enumerate(halo_refs()):
            wait_bytes(ref, halo_recv.at[i])

    buffers = (gate_w, up_w, down_w)

    def slot_for(kind, offset):
        straight, swapped = SLOT[offset], SLOT[offset[::-1]]
        return swapped if kind == 1 else straight

    def place(kind, offset, half, core_id):
        start = slot_for(kind, offset) * wide + core_id * depth
        if half is None:
            return buffers[kind].at[pl.ds(pl.multiple_of(start, depth), depth)]
        return buffers[kind].at[pl.ds(pl.multiple_of(start + half * sub_rows, sub_rows), sub_rows)]

    def ring(kind, number, way):
        axis, src_offset, dst_offset, halved = message(number, way)
        half = way if halved else None
        dst = place(kind, dst_offset, half, core)
        src = place(kind, src_offset, half, core)
        to = (axes[kind][axis][way], tp)
        return remote(src, dst, ring_send.at[0], ring_recv.at[kind // 2, number - 1], to)

    def pair(kind, offset, half):
        dst = place(kind, offset, half, core)
        slot = slot_for(kind, offset)
        if kind == 2:
            sem = down_recv.at[chunk_of(slot)]
        else:
            sem = pair_recv.at[segment_of(slot)]
        return remote(dst, dst, pair_send.at[0], sem, partner)

    def begin(number, kinds):
        for kind in kinds:
            for way in range(2):
                launch(ring(kind, number, way))

    def tick(number, kinds):
        halved = message(number, 0)[3]
        total = 2 * len(kinds) * (sub_rows if halved else depth)
        wait_bytes(buffers[kinds[0]].at[pl.ds(0, total)], ring_recv.at[kinds[0] // 2, number - 1])
        for follower in (DOWN_FOLLOW if kinds[0] == 2 else FOLLOW).get(number, ()):
            for kind in kinds:
                for way in range(2):
                    launch(ring(kind, follower, way))
        for kind in kinds:
            for way in range(2):
                _, _, offset, halved = message(number, way)
                launch(pair(kind, offset, way if halved else None))

    weights_tick = lambda number: tick(number, (0, 1))
    down_tick = lambda number: tick(number, (2,))

    def segment_wait(segment):
        lo, hi = SEGMENTS[segment]
        wait_bytes(gate_w.at[pl.ds(0, 2 * (hi - lo) * depth)], pair_recv.at[segment])

    span = rows + 2 * HALF
    at = lax.broadcasted_iota(jnp.int32, (1, span), 1) + (sp * rows - HALF)
    inside = jnp.logical_and(at >= 0, at < sp_size * rows)
    reach = 3 * HALF
    repeat = q_hbm.shape[1] // HEAD
    offset_of = lax.broadcasted_iota(jnp.int32, (HALF, reach), 1) - lax.broadcasted_iota(
        jnp.int32, (HALF, reach), 0
    )
    near = jnp.logical_and(offset_of >= 0, offset_of <= 2 * HALF)

    def attend(block):
        here = slice(block * HALF, (block + 1) * HALF)
        there = slice(block * HALF, block * HALF + reach)
        doc_row = doc_all[:, (block + 1) * HALF : (block + 2) * HALF]
        doc_query = jnp.broadcast_to(doc_row, (HALF, HALF)).T
        doc_keys = jnp.where(inside[:, there], doc_all[:, there], -1)
        same = jnp.concatenate([doc_query] * 3, 1) == doc_keys
        allowed = jnp.logical_and(near, same)
        key_blk = k_all[there, :]
        value_blk = v_all[there, :]
        for h in range(repeat):
            lanes = slice(h * HEAD, (h + 1) * HEAD)
            scores = lax.dot_general(
                q_all[here, lanes], key_blk, (((1,), (1,)), ((), ())), preferred_element_type=F32
            ) * HEAD ** (-0.5)
            scores = jnp.where(allowed, scores, NEGATIVE)
            sink = jnp.full((1, 1), sink_ref[h], F32)
            top = jnp.maximum(jnp.max(scores, -1, keepdims=True), sink)
            weights = jnp.exp(scores - top)
            total = jnp.sum(weights, -1, keepdims=True) + jnp.exp(sink - top)
            summed = jnp.dot(weights.astype(BF16), value_blk, preferred_element_type=F32)
            att[here, lanes] = (summed / total).astype(BF16)

    def token_rows_of(j):
        return pl.ds(pl.multiple_of(j * token_rows, token_rows), token_rows)

    def send_tokens():
        for j, into in ((tp_far, 3), (tp_right, 1), (tp_left, 2)):
            launch(
                remote(
                    att.at[token_rows_of(j)], tokens.at[into], tok_send.at[0], tok_recv.at[into // 3], (sp, j)
                )
            )
        tokens[0] = att[token_rows_of(tp), :]

    def order_gains():
        for slot in range(CHIPS):
            gains[:, slot_lanes(slot)] = gains_in[:, chip_lanes(slot)]

    def project(held):
        for first, second in zip(range(0, CHIPS, 2), range(1, CHIPS, 2)):
            picks = (chip_lanes(first), chip_lanes(second))
            lanes = slice(first * wide, (second + 1) * wide)
            if held[0] == 0:
                mixed = ALPHA * jnp.concatenate([res_all[:, pick] for pick in picks], 1).astype(F32)
            else:
                mixed = pre[:, lanes]
            for j in held:
                cols = q_hbm.shape[1]
                deep = pl.ds(pl.multiple_of((tp, tp_left, tp_right, tp_far)[j] * cols, cols), cols)
                mixed += jnp.dot(
                    tokens[j],
                    jnp.concatenate([w_out[deep, pick] for pick in picks], 1),
                    preferred_element_type=F32,
                )
            pre[:, lanes] = mixed

    strip = 64

    def norm_rows(first, last):
        @pl.loop(first // strip, last // strip)
        def _(t):
            here = pl.ds(pl.multiple_of(t * strip, strip), strip)
            normed[here, :] = layer_norm(pre[here, :], gains[0:1, :]).astype(BF16)

    def piece_rows(index):
        return pl.ds(index * half_rows, half_rows)

    ROUTES = ((0, 0, 2), (1, 1, 3), (0, 1, 4), (1, 0, 5), (0, 2, 6), (1, 3, 7))

    def norm_copy(route):
        way, src, dst = ROUTES[route]
        return remote(
            normed.at[piece_rows(src)],
            normed.at[piece_rows(dst)],
            norm_send.at[0],
            norm_recv.at[route // 2],
            sides[way],
        )

    def norm_arrive(stage):
        wait_bytes(normed.at[pl.ds(0, 2 * half_rows)], norm_recv.at[stage])

    def gate_up(top, bottom, lo, hi, lanes):
        deep = slice(lo * wide, hi * wide)
        gate = jnp.dot(normed[top:bottom, deep], gate_w[deep, lanes], preferred_element_type=F32)
        up = jnp.dot(normed[top:bottom, deep], up_w[deep, lanes], preferred_element_type=F32)
        if lo > 0:
            gate += gate_acc[top:bottom, lanes]
            up += up_acc[top:bottom, lanes]
        if hi < CHIPS:
            gate_acc[top:bottom, lanes] = gate
            up_acc[top:bottom, lanes] = up
        else:
            hidden[top:bottom, lanes] = (gate / (1.0 + jnp.exp(-gate)) * up).astype(BF16)

    def gate_up_range(top, bottom, lo, hi):
        for start in range(0, units, 256):
            gate_up(top, bottom, lo, hi, slice(start, min(start + 256, units)))

    LEFT, RIGHT, OWN, FAR = range(4)
    def down_rows(k, top, bottom, pieces):
        a, b = CHUNKS[k]
        if b == a + 1:
            weights = down_w[a * wide : (b + 1) * wide, :]
        else:
            weights = jnp.concatenate([down_w[s * wide : (s + 1) * wide, :] for s in (a, b)], 0)
        part = lax.dot_general(
            hidden[top:bottom, :], weights, (((1,), (1,)), ((), ())), preferred_element_type=F32
        ).astype(BF16)
        for source, to in enumerate(pieces):
            for side, lanes in ((0, slice(0, wide)), (1, slice(wide, 2 * wide))):
                parts[to // 2, k, side, to % 2 * half_rows : (to % 2 + 1) * half_rows, :] = part[
                    source * half_rows : (source + 1) * half_rows, lanes
                ]

    def down_far(k):
        wait_bytes(down_w.at[pl.ds(0, wide)], down_recv.at[k])
        down_rows(k, 3 * token_rows, 4 * token_rows, (6, 7))
        for way in range(2):
            launch(
                remote(
                    parts.at[FAR, k, way], relays.at[k, way], sum_send.at[0], relay_recv.at[k], sides[way]
                )
            )

    def down_rest(k):
        down_rows(k, 0, 3 * token_rows, (4, 5, 0, 3, 1, 2))

    def plain_chunk(k):
        for way, to, side in ((0, RIGHT, 1), (1, LEFT, 0)):
            launch(
                remote(
                    parts.at[to, k, side], arrived.at[k, to, side], sum_send.at[0], sum_recv.at[k], sides[way]
                )
            )

    def relay_chunk(k, whole):
        wait_bytes(relays.at[k], relay_recv.at[k])
        for way, to in ((0, RIGHT), (1, LEFT)):
            parts[to, k, way] = (parts[to, k, way].astype(F32) + relays[k, way].astype(F32)).astype(BF16)
            piece = (to, k) if whole else (to, k, way)
            into = (k, to) if whole else (k, to, way)
            launch(remote(parts.at[piece], arrived.at[into], sum_send.at[0], sum_recv.at[k], sides[way]))

    first_core = lax.broadcasted_iota(jnp.int32, (token_rows, wide), 1) < depth

    def prepare_sum():
        pre[...] = ALPHA * normed[0:token_rows, :].astype(F32)

    def finish_chunk(k):
        wait_bytes(arrived.at[k], sum_recv.at[k])
        for side, slot in enumerate(CHUNKS[k]):
            down = (
                parts[OWN, k, side].astype(F32)
                + arrived[k, LEFT, side].astype(F32)
                + arrived[k, RIGHT, side].astype(F32)
            )
            swapped = SLOT[OFFSETS[slot][::-1]]
            if swapped == slot:
                pre[:, slot_lanes(slot)] += down
            else:
                pre[:, slot_lanes(slot)] += jnp.where(first_core, down, 0.0)
                pre[:, slot_lanes(swapped)] += jnp.where(first_core, 0.0, down)

    def final_norm():
        for t in range(token_rows // strip):
            here = pl.ds(t * strip, strip)
            result = layer_norm(pre[here, :], gains[1:2, :]).astype(BF16)
            for slot in range(CHIPS):
                out_ref[here, chip_lanes(slot)] = result[:, slot_lanes(slot)]

    def sends_wait():
        def gone(ref, sem):
            remote(ref, ref, sem, sem, partner).wait_send()

        for i, ref in enumerate(halo_refs()):
            gone(ref, halo_send.at[i])
        gone(weights.at[:, pl.ds(0, (CHIPS - 1) * depth)], ring_send.at[0])
        gone(weights.at[:, pl.ds(0, CHIPS * depth)], pair_send.at[0])
        gone(tokens.at[pl.ds(0, TP - 1)], tok_send.at[0])
        gone(normed.at[pl.ds(0, 6 * half_rows)], norm_send.at[0])
        gone(parts.at[pl.ds(0, 3)], sum_send.at[0])

    loaded(normed.at[pl.ds(0, rows // 4)], 0)
    loaded(doc_all.at[:, pl.ds(HALF, rows)], 1)
    attend(1)
    pl.semaphore_wait(barrier, len(greeted))
    launch_halos()
    loaded(gate_w.at[pl.ds(0, 3 * depth)], 2)
    begin(1, (0, 1))
    begin(2, (0, 1))
    for kind in range(3):
        launch(pair(kind, (0, 0), None))
    load(w_out_hbm, w_out, 3)
    load(res_hbm, res_all, 4)
    for i, src in enumerate((gain_one_hbm, gain_two_hbm)):
        load(src, gains_in.at[pl.ds(i, 1)], 5)
    attend(2)
    halo_wait()
    attend(0)
    attend(3)
    send_tokens()
    weights_tick(1)
    loaded(w_out, 3)
    loaded(res_all, 4)
    loaded(gains_in, 5)
    order_gains()
    wait_bytes(tokens.at[pl.ds(0, 2)], tok_recv.at[0])
    project((0, 1, 2))
    wait_bytes(tokens.at[3], tok_recv.at[1])
    project((3,))
    norm_rows(0, half_rows)
    launch(norm_copy(0))
    norm_rows(half_rows, token_rows)
    for route in (1, 2, 3):
        launch(norm_copy(route))
    weights_tick(2)
    weights_tick(3)
    prepare_sum()
    weights_tick(4)
    norm_arrive(0)
    for route in (4, 5):
        launch(norm_copy(route))
    weights_tick(5)
    segment_wait(0)
    gate_up_range(0, 256, 0, 4)
    weights_tick(6)
    segment_wait(1)
    gate_up_range(0, 256, 4, 10)
    weights_tick(7)
    begin(1, (2,))
    norm_arrive(1)
    gate_up_range(256, 384, 0, 10)
    weights_tick(8)
    weights_tick(9)
    norm_arrive(2)
    begin(2, (2,))
    gate_up_range(384, 512, 0, 10)
    segment_wait(2)
    gate_up_range(0, 128, 10, 14)
    weights_tick(10)
    gate_up_range(128, 512, 10, 14)
    down_tick(1)
    segment_wait(3)
    gate_up_range(0, 512, 14, 16)
    down_far(0)
    down_tick(2)
    down_rest(0)
    plain_chunk(0)
    down_far(1)
    down_rest(1)
    plain_chunk(1)
    down_tick(3)
    down_tick(4)
    relay_chunk(0, False)
    down_far(2)
    down_tick(5)
    relay_chunk(1, False)
    down_rest(2)
    plain_chunk(2)
    down_far(3)
    down_rest(3)
    plain_chunk(3)
    down_tick(7)
    down_far(4)
    relay_chunk(2, False)
    down_tick(6)
    down_rest(4)
    plain_chunk(4)
    down_tick(8)
    down_far(5)
    relay_chunk(3, False)
    down_tick(9)
    down_rest(5)
    plain_chunk(5)
    down_tick(10)
    down_far(6)
    relay_chunk(4, False)
    down_far(7)
    down_rest(6)
    plain_chunk(6)
    relay_chunk(5, False)
    down_rest(7)
    plain_chunk(7)
    relay_chunk(6, False)
    finish_chunk(0)
    finish_chunk(1)
    finish_chunk(2)
    relay_chunk(7, False)
    finish_chunk(3)
    finish_chunk(4)
    finish_chunk(5)
    finish_chunk(6)
    finish_chunk(7)
    final_norm()
    sends_wait()


def solution(mesh):
    def per_device(
        queries,
        keys,
        values,
        doc_ids,
        sink_logit,
        residual_in,
        w_out,
        gain_one,
        w_gate,
        w_up,
        w_down,
        gain_two,
    ):
        rows = queries.shape[0]
        token_rows, width = residual_in.shape
        units = w_gate.shape[1]
        span = rows + 2 * HALF
        dma = pltpu.SemaphoreType.DMA
        vmem, anywhere = (pl.BlockSpec(memory_space=pltpu.VMEM), pl.BlockSpec(memory_space=pl.ANY))
        return pl.pallas_call(
            kernel,
            out_shape=pltpu.VMEM((token_rows, width), BF16),
            in_specs=[pl.BlockSpec(memory_space=pltpu.SMEM)] + [anywhere] * 11,
            out_specs=vmem,
            scratch_shapes=[
                pltpu.VMEM(queries.shape, BF16),
                pltpu.VMEM((span, keys.shape[1]), BF16),
                pltpu.VMEM((span, keys.shape[1]), BF16),
                pltpu.VMEM((1, span), jnp.int32),
                pltpu.VMEM((2, width), F32),
                pltpu.VMEM((2, width), F32),
                pltpu.VMEM((token_rows, width), BF16),
                pltpu.VMEM(w_out.shape, BF16),
                pltpu.VMEM((3, width, units), BF16),
                pltpu.VMEM(queries.shape, BF16),
                pltpu.VMEM((TP, token_rows, queries.shape[1]), BF16),
                pltpu.VMEM((token_rows, width), F32),
                pltpu.VMEM((rows, width), BF16),
                pltpu.VMEM((rows, units), F32),
                pltpu.VMEM((rows, units), F32),
                pltpu.VMEM((rows, units), BF16),
                pltpu.VMEM((4, len(CHUNKS), 2, token_rows, width // CHIPS), BF16),
                pltpu.VMEM((len(CHUNKS), 2, token_rows, width // CHIPS), BF16),
                pltpu.VMEM((len(CHUNKS), 2, 2, token_rows, width // CHIPS), BF16),
                dma((6,)),
                dma((2,)),
                dma((2,)),
                dma((1,)),
                dma((2, LAST)),
                dma((1,)),
                dma((len(SEGMENTS),)),
                dma((len(CHUNKS),)),
                dma((1,)),
                dma((2,)),
                dma((1,)),
                dma((3,)),
                dma((1,)),
                dma((len(CHUNKS),)),
                dma((len(CHUNKS),)),
            ],
            compiler_params=pltpu.CompilerParams(
                collective_id=0, has_side_effects=True, vmem_limit_bytes=62 * 2**20
            ),
        )(
            sink_logit,
            queries,
            residual_in,
            gain_one[None, :],
            gain_two[None, :],
            keys,
            values,
            doc_ids[None, :],
            w_out,
            w_gate,
            w_up,
            w_down.T,
        )

    in_specs = (
        P("sp", "tp"),
        P("sp", "tp"),
        P("sp", "tp"),
        P("sp"),
        P("tp"),
        P(("sp", "tp"), None),
        P(),
        P(),
        P("sp", "tp"),
        P("sp", "tp"),
        P("tp", "sp"),
        P(),
    )
    return jax.shard_map(
        per_device, mesh=mesh, in_specs=in_specs, out_specs=P(("sp", "tp"), None), check_vma=False
    )
```
